512 devices in a mesh: ep: 128 (over z, y, core), tp: 4 (over x).
Axes of the slice: x: 4, y: 8, z: 8, core: 2. Of those that a mesh axis runs over, the one named last changes fastest.
Arguments:
- tokens: bfloat16 [16384, 2048], P('ep'), may hold values from -24 to 24
- cotangent: bfloat16 [16384, 2048], P('ep'), may hold values from -6 to 6
- routing: int32 [16384, 2], P('ep'), may hold values from 0 to 127, all different within a row; in each aligned block of 128 rows (0 to 127, 128 to 255, ...) at most 4 rows name the same one
- router_weight: bfloat16 [2048, 128], replicated, may hold values from -0.125 to 0.125
- gate_weight: bfloat16 [128, 2048, 512], P('ep', None, 'tp'), may hold values from -0.125 to 0.125
- up_weight: bfloat16 [128, 2048, 512], P('ep', None, 'tp'), may hold values from -0.125 to 0.125
- down_weight: bfloat16 [128, 512, 2048], P('ep', 'tp'), may hold values from -0.25 to 0.25
Outputs:
- grad_tokens: bfloat16 [16384, 2048], P('ep', 'tp')
- grad_gating: float32 [16384, 2], P('ep')
- grad_router: float32 [2048, 128], P('ep')
- grad_gate_weight: bfloat16 [128, 2048, 512], P('ep', None, 'tp')
- grad_up_weight: bfloat16 [128, 2048, 512], P('ep', None, 'tp')
- grad_down_weight: bfloat16 [128, 512, 2048], P('ep', 'tp')
- in_norms: float32 [128, 2, 2048], P('ep')
- down_norms: float32 [128, 512], P('ep', 'tp')
- router_norms: float32 [2048], P('ep')
The draws below stay inside these ranges and needn't reach their ends.
Inputs may be any that keep to these rules, and one draw needn't show every extreme that they name: `routing`: each row names 2 different experts. Among the rows of one index of ep no expert is named by more than 4 rows, a bound that some block reaches in some of them.
All inputs are finite; a program needn't handle non-finite values.
Results may differ from the reference program's by a relative error of at most 0.014.
Values may be sent and summed in bfloat16 or wider, within the bound.
No kernel may reach another device: no remote copies, remote signals or barrier semaphores. Data moves between devices by JAX's collectives and lax.ppermute only.
A program may use at most 64 MiB of HBM per device.

```python
import math
import jax
import jax.numpy as jnp
import numpy as np
from jax import lax

D = 2048
F = 512
TOP = 2
TOK_DEV = 128
EXPERTS = 128
TOKENS = 16384
CAP = 4
N_EP = 128
N_TP = 4


def raised(values, rng, source, target, shards_of, factor):
    owner, partner = [(jnp.arange(values.shape[dim]) // (values.shape[dim] // shards_of)).reshape([-1 if axis == dim else 1 for axis in range(values.ndim)]) for dim in (source, target)]
    chosen = jax.random.permutation(rng, shards_of)[partner]
    strong = (owner == chosen) | (owner == (partner + shards_of // 2) % shards_of)
    return jnp.where(strong, factor * values, values)


def level_of(stream_key, shape, pieces, smallest, largest):
    def one(dim, shards_of):
        heights = jax.random.uniform(jax.random.fold_in(jax.random.fold_in(stream_key, 6), dim), (shards_of,), jnp.float32, smallest / len(pieces), largest / len(pieces))
        return jnp.repeat(jnp.exp(heights), shape[dim] // shards_of).reshape((-1,) + (1,) * (len(shape) - dim - 1))

    level = one(*pieces[0])
    for cut in pieces[1:]:
        level = level * one(*cut)
    return level


def routed_block(stream_key, own, number, rows, number_of, top, bound, slope):
    ranking = jax.random.permutation(stream_key, number_of)
    packed, usual = shares(number_of, rows * top, bound, slope, True), shares(number_of, rows * top, bound, slope, False)
    places = jnp.arange(number_of)

    def named(sizes, turn):
        used = int((sizes > 0).sum())
        fixed = max(1, used // 4)
        shifted = fixed + (places - fixed + turn * (used - fixed)) % max(1, number_of - fixed)
        return jnp.zeros((number_of,), jnp.int32).at[ranking[jnp.where(places < fixed, places, shifted)]].set(jnp.asarray(sizes, jnp.int32))

    sizes = jnp.where(number % 4 == 0, named(packed, number // 4), named(usual, number - number // 4 - 1))
    mixed = jax.random.permutation(jax.random.fold_in(own, 3), number_of)
    donor, receiver = mixed[0:number_of // 2 * 2:2], mixed[1:number_of // 2 * 2:2]
    room = jnp.minimum(sizes[donor] - 1, bound - sizes[receiver]) // 2
    room = jnp.where((donor == ranking[0]) | (receiver == ranking[0]) | (sizes[receiver] == 0), 0, jnp.maximum(room, 0))
    shifted = jax.random.randint(jax.random.fold_in(own, 4), (number_of // 2,), 0, 1 << 20) % (room + 1)
    sizes = sizes.at[donor].add(-shifted).at[receiver].add(shifted)
    members = jnp.searchsorted(jnp.cumsum(sizes), jnp.arange(rows * top), side="right").astype(jnp.int32)
    listing = members.reshape(top, rows).T
    listing = listing[jax.random.permutation(jax.random.fold_in(own, 1), rows)]
    turn = jax.random.randint(jax.random.fold_in(own, 2), (rows, 1), 0, top)
    return jnp.take_along_axis(listing, (jnp.arange(top)[None, :] + turn) % top, axis=1)


def shares(count, total, limit, slope, full):
    portions = [(1 << 20) // math.isqrt(rank ** slope) + 1 for rank in range(1, count + 1)]
    largest = limit if full else min(limit, max(-(-total // count), total * portions[0] // sum(portions)))
    least = 1 if total - largest >= count - 1 else 0
    counts, surplus = [largest] + [least] * (count - 1), total - largest - least * (count - 1)
    while surplus > 0:
        movable = [i for i in range(1, count) if counts[i] < largest] or [i for i in range(1, count) if counts[i] < limit]
        whole, budget = sum([portions[i] for i in movable]), surplus
        for i in movable:
            addition = min(limit - counts[i], max(1, budget * portions[i] // whole), surplus)
            counts[i] = counts[i] + addition
            surplus = surplus - addition
    return np.array(counts)


def centred(stream_key, extent, scale, bound, cuts=(), held_as=jnp.bfloat16):
    values = scale * jax.random.normal(stream_key, extent, jnp.float32)
    if cuts:
        values = values * level_of(stream_key, extent, cuts, -0.22, 0.18)
    return jnp.clip(values, -bound, bound).astype(held_as)


def gaussian_with(own_key, extent, scale, reach, split, heavy, held_as=jnp.bfloat16):
    drawn = scale * jax.random.normal(own_key, extent, jnp.float32)
    if split:
        drawn = drawn * level_of(own_key, extent, split, -0.22, 0.18)
    return jnp.clip(raised(drawn, jax.random.fold_in(own_key, 3), *heavy), -reach, reach).astype(held_as)


def setup_inputs(seed: int = 0) -> dict:
    arg_keys = jax.random.split(jax.random.key(seed), 8)
    tokens = gaussian_with(arg_keys[0], (TOKENS, D), 1.0, 24.0, ((0, 128),), (0, 1, 128, 5.5))
    cotangent = centred(arg_keys[1], (TOKENS, D), 1.0, 6.0, ((0, 128),))
    routing_keys = jax.random.split(jax.random.fold_in(arg_keys[2], 1), TOKENS // TOK_DEV)
    routing_turns = jax.random.permutation(jax.random.fold_in(arg_keys[2], 3), TOKENS // TOK_DEV)
    routing = jax.vmap(lambda own, number: routed_block(jax.random.fold_in(arg_keys[2], 2), own, number, TOK_DEV, EXPERTS, TOP, CAP, 2))(routing_keys, routing_turns).reshape((TOKENS, TOP))
    router_weight = centred(arg_keys[3], (D, EXPERTS), D ** -0.5, 0.125)
    gate_weight = centred(arg_keys[4], (EXPERTS, D, F), D ** -0.5, 0.125, ((0, 128), (2, 4)))
    up_weight = centred(arg_keys[5], (EXPERTS, D, F), D ** -0.5, 0.125, ((0, 128), (2, 4)))
    down_weight = centred(arg_keys[6], (EXPERTS, F, D), F ** -0.5, 0.25, ((0, 128), (1, 4)))
    return {"tokens": tokens, "cotangent": cotangent, "routing": routing, "router_weight": router_weight, "gate_weight": gate_weight, "up_weight": up_weight, "down_weight": down_weight}


def silu_parts(pre_gate):
    sigmoid_gate = jax.nn.sigmoid(pre_gate)
    return pre_gate * sigmoid_gate, sigmoid_gate * (1.0 + pre_gate * (1.0 - sigmoid_gate))


def block_layout(block_routing):
    flat_expert = block_routing.reshape(-1)
    one_hot = (flat_expert[:, None] == jnp.arange(EXPERTS, dtype=jnp.int32)[None, :]).astype(jnp.int32)
    earlier = jnp.cumsum(one_hot, axis=0) - one_hot
    within = jnp.sum(earlier * one_hot, axis=1)
    position = (flat_expert * CAP + within).astype(jnp.int32)
    vacant = jnp.full((EXPERTS * CAP,), -1, jnp.int32)
    return vacant.at[position].set(jnp.arange(TOK_DEV * TOP, dtype=jnp.int32))


def reference(tokens, cotangent, routing, router_weight, gate_weight, up_weight, down_weight):
    local_layout = jax.vmap(block_layout)(routing.reshape(N_EP, TOK_DEV, TOP))
    offsets = (jnp.arange(N_EP, dtype=jnp.int32) * (TOK_DEV * TOP))[:, None]
    global_layout = jnp.where(local_layout >= 0, local_layout + offsets, TOKENS * TOP).astype(jnp.int32)
    expert_layout = global_layout.reshape(N_EP, EXPERTS, CAP).transpose(1, 0, 2).reshape(EXPERTS, N_EP * CAP)

    logits = jnp.dot(tokens, router_weight, preferred_element_type=jnp.float32)
    scores = jax.nn.sigmoid(jnp.take_along_axis(logits, routing, axis=1))
    score_sum = jnp.sum(scores, axis=1, keepdims=True)
    gating = scores / score_sum
    flat_gating = jnp.concatenate([gating.reshape(-1), jnp.zeros((1,), jnp.float32)])
    padded_tokens = jnp.concatenate([tokens, jnp.zeros((1, D), jnp.bfloat16)], axis=0)
    padded_cotangent = jnp.concatenate([cotangent, jnp.zeros((1, D), jnp.bfloat16)], axis=0)
    hidden_block = F // N_TP
    arrived = N_EP * CAP

    def one_expert(carried, inputs):
        token_terms, gating_grads = carried
        slot_layout, weight_gate, weight_up, weight_down = inputs
        source_rows = slot_layout // TOP
        rows_in = padded_tokens[source_rows]
        cot_rows = padded_cotangent[source_rows]
        slot_gating = flat_gating[slot_layout][:, None]
        pre_gate = jnp.dot(rows_in, weight_gate, preferred_element_type=jnp.float32)
        pre_up = jnp.dot(rows_in, weight_up, preferred_element_type=jnp.float32)
        activated, silu_slope = silu_parts(pre_gate)
        hidden = (activated * pre_up).astype(jnp.bfloat16)
        back_raw = lax.dot_general(cot_rows, weight_down, (((1,), (1,)), ((), ())),
                                   preferred_element_type=jnp.float32)
        hidden_wide = hidden.astype(jnp.float32)
        gate_grad = jnp.sum(hidden_wide * back_raw, axis=1)
        scaled_back = slot_gating * back_raw
        grad_pre_gate = (scaled_back * pre_up * silu_slope).astype(jnp.bfloat16)
        grad_pre_up = (scaled_back * activated).astype(jnp.bfloat16)
        scaled_hidden = (slot_gating * hidden_wide).astype(jnp.bfloat16)
        gate_sum = jnp.dot(rows_in.T, grad_pre_gate, preferred_element_type=jnp.float32)
        up_sum = jnp.dot(rows_in.T, grad_pre_up, preferred_element_type=jnp.float32)
        down_sum = jnp.dot(scaled_hidden.T, cot_rows, preferred_element_type=jnp.float32)
        norms_in = jnp.stack([jnp.sum(gate_sum * gate_sum, axis=1), jnp.sum(up_sum * up_sum, axis=1)])
        norms_down = jnp.sum(down_sum * down_sum, axis=1)
        pieces_gate = grad_pre_gate.reshape(arrived, N_TP, hidden_block).astype(jnp.float32)
        pieces_up = grad_pre_up.reshape(arrived, N_TP, hidden_block).astype(jnp.float32)
        blocks_gate = weight_gate.reshape(D, N_TP, hidden_block).astype(jnp.float32)
        blocks_up = weight_up.reshape(D, N_TP, hidden_block).astype(jnp.float32)
        partial_value = (jnp.einsum("rpf,dpf->prd", pieces_gate, blocks_gate)
                   + jnp.einsum("rpf,dpf->prd", pieces_up, blocks_up))
        rounded = lax.optimization_barrier(partial_value.astype(jnp.bfloat16))
        token_term = jnp.sum(rounded.astype(jnp.float32), axis=0).astype(jnp.bfloat16)
        token_terms = token_terms.at[slot_layout].set(token_term)
        gating_grads = gating_grads.at[slot_layout].set(gate_grad)
        return (token_terms, gating_grads), (gate_sum.astype(jnp.bfloat16), up_sum.astype(jnp.bfloat16),
                                             down_sum.astype(jnp.bfloat16), norms_in, norms_down)

    start_terms = jnp.zeros((TOKENS * TOP + 1, D), jnp.bfloat16)
    start_grads = jnp.zeros((TOKENS * TOP + 1,), jnp.float32)
    (token_terms, gating_grads), stacked = lax.scan(
        one_expert, (start_terms, start_grads), (expert_layout, gate_weight, up_weight, down_weight))
    grad_gate_weight, grad_up_weight, grad_down_weight, in_norms, down_norms = stacked

    summed_terms = jnp.sum(token_terms[:TOKENS * TOP].reshape(TOKENS, TOP, D).astype(jnp.float32), axis=1)
    grad_gating = gating_grads[:TOKENS * TOP].reshape(TOKENS, TOP)
    weighted = jnp.sum(gating * grad_gating, axis=1, keepdims=True)
    grad_scores = (grad_gating - weighted) / score_sum
    grad_chosen = grad_scores * scores * (1.0 - scores)
    token_index = jnp.arange(TOKENS, dtype=jnp.int32)[:, None]
    grad_logits = jnp.zeros((TOKENS, EXPERTS), jnp.float32).at[token_index, routing].add(grad_chosen)
    grad_logits = grad_logits.astype(jnp.bfloat16)
    router_term = lax.dot_general(grad_logits, router_weight, (((1,), (1,)), ((), ())),
                                  preferred_element_type=jnp.float32)
    grad_tokens = (summed_terms + router_term).astype(jnp.bfloat16)
    grad_router = jnp.dot(tokens.T, grad_logits, preferred_element_type=jnp.float32)
    router_norms = jnp.sum(grad_router * grad_router, axis=1)
    return (grad_tokens, grad_gating, grad_router, grad_gate_weight, grad_up_weight, grad_down_weight,
            in_norms, down_norms, router_norms)
```

```python
import functools

import jax
import jax.numpy as jnp
from jax import lax
from jax.experimental import pallas as pl
from jax.experimental.pallas import tpu as pltpu
from jax.sharding import Mesh
from jax.sharding import PartitionSpec as P

EP = ("ep_0", "ep_1", "ep_3", "ep_2")
NEAR = ("ep_3", "ep_2")
ALL = EP + ("tp",)
F32 = jnp.float32
BF16 = jnp.bfloat16


TOK = 128
D = 2048
EXPERTS = 128
CAP = 4
TP = 4
DQ = D // TP
F = 512
FQ = F // TP
ROWS = EXPERTS * CAP
SENT = EXPERTS * 8


def dot(a, b, ca=1, cb=0):
    return lax.dot_general(a, b, (((ca,), (cb,)), ((), ())), preferred_element_type=F32)


def iota(shape, dim):
    return lax.broadcasted_iota(jnp.int32, shape, dim)


def pieces(x):
    hi = x.astype(BF16).astype(F32)
    rest = x - hi
    mid = rest.astype(BF16).astype(F32)
    return hi, mid, rest - mid


def aligned(x, n):
    return pl.multiple_of(x * n, n)


def to_rows(half):
    slot = iota((128, 256), 0)
    row = iota((128, 256), 1)
    return ((row // 8 == slot // 4) & (row % 8 == slot % 4 + 4 * half)).astype(BF16)


def whole(shape):
    return pl.BlockSpec(shape, lambda g, p: (0,) * len(shape))


def call(kernel, name, scalars, ins, in_specs, outs, out_specs=None):
    return pl.pallas_call(
        kernel,
        name=name,
        grid_spec=pltpu.PrefetchScalarGridSpec(
            num_scalar_prefetch=1,
            grid=(1,),
            in_specs=in_specs,
            out_specs=out_specs or tuple(whole(o.shape) for o in outs),
        ),
        out_shape=tuple(outs),
    )(scalars, *ins)


def sds(shape, dtype):
    return jax.ShapeDtypeStruct(shape, dtype)


def dispatch_kernel(sc, tok, tok_q, cot_q, routing, router, send, match0, match1, stats):
    experts = iota((EXPERTS, TOK), 0)
    picked = [(experts == routing[k : k + 1, :]) for k in range(2)]
    both = (picked[0] | picked[1]).astype(F32)
    logits = dot(router[...], tok[...], 0, 1)
    s = [
        jax.nn.sigmoid(jnp.sum(jnp.where(m, logits, 0.0), axis=0, keepdims=True)) for m in picked
    ]
    total = s[0] + s[1]
    g = [v / total for v in s]
    slope = [v * (1.0 - v) / total for v in s]
    before = (iota((TOK, TOK), 0) < iota((TOK, TOK), 1)).astype(BF16)
    within = dot(both.astype(BF16), before)
    repeat = (iota((SENT, EXPERTS), 0) // 8 == iota((SENT, EXPERTS), 1)).astype(BF16)
    sub = (iota((SENT, TOK), 0) % 8).astype(F32)
    slot = jnp.where(sub < 4.0, sub, sub - 4.0)
    line = iota((128, TOK), 0)
    found = []
    info = None
    for k, out in ((0, match0), (1, match1)):
        place = jnp.where(picked[k], within, -1.0).astype(BF16)
        one = jnp.where(dot(repeat, place) == slot, 1.0, 0.0)
        out[...] = one.astype(BF16)
        found.append(one)
        own = slope[k] * g[1 - k]
        other = slope[1 - k] * g[k]
        columns = [*pieces(g[k]), *pieces(own), *pieces(other), routing[1 - k : 2 - k, :].astype(F32)]
        table = jnp.zeros((128, TOK), F32)
        for c, v in enumerate(columns):
            table = jnp.where(line == c, v, table)
        part = dot(one.astype(BF16), table.astype(BF16), 1, 1)
        info = part if info is None else info + part
    any_one = found[0] + found[1]
    first = jnp.where(sub < 4.0, any_one, 0.0).astype(BF16)
    second = jnp.where(sub < 4.0, 0.0, any_one).astype(BF16)
    send[:, 0:DQ] = (dot(first, tok_q[...]) + dot(second, cot_q[...])).astype(BF16)
    send[:, DQ : DQ + 128] = info.astype(BF16)
    stats[...] = jnp.concatenate(
        [s[0], s[1], total, g[0], g[1], total, total, total], axis=0
    )


def pack_kernel(sc, gate, up, down, *outs):
    p = sc[0]
    for d, out in enumerate(outs, 1):
        q = (p + d) % TP
        out[0:DQ, :] = gate[pl.ds(aligned(q, DQ), DQ), :]
        out[DQ : 2 * DQ, :] = up[pl.ds(aligned(q, DQ), DQ), :]
        for c in range(4):
            out[2 * DQ + 128 * c : 2 * DQ + 128 * (c + 1), :] = down[
                :, pl.ds(aligned(q * 4 + c, 128), 128)
            ]


def hidden_kernel(sc, got, gate, up, down, w1, w2, w3, tok_c, cot_c, info_c, part, gate_f, up_f, down_f):
    p = sc[0]
    here = aligned(p, FQ)
    gate_f[:, pl.ds(here, FQ)] = gate[...]
    up_f[:, pl.ds(here, FQ)] = up[...]
    down_f[pl.ds(here, FQ), :] = down[...]
    for d, w in ((1, w1), (2, w2), (3, w3)):
        f = aligned((p + TP - d) % TP, FQ)
        gate_f[:, pl.ds(f, FQ)] = w[0:DQ, :]
        up_f[:, pl.ds(f, FQ)] = w[DQ : 2 * DQ, :]
        for c in range(4):
            down_f[pl.ds(f, FQ), 128 * c : 128 * (c + 1)] = w[
                2 * DQ + 128 * c : 2 * DQ + 128 * (c + 1), :
            ]
    sel_t = to_rows(0)
    sel_c = to_rows(1)
    for q in range(TP):
        block = got[256 * q : 256 * (q + 1), :]
        mine = dot(sel_t, block).astype(BF16)
        cots = dot(sel_c, block[:, 0:DQ]).astype(BF16)
        toks = mine[:, 0:DQ]
        rows = slice(128 * q, 128 * (q + 1))
        tok_c[rows, :] = toks
        cot_c[rows, :] = cots
        info_c[rows, :] = mine[:, DQ:]
        part[q, :, 0:F] = dot(toks, gate_f[...]).astype(BF16)
        part[q, :, F : 2 * F] = dot(toks, up_f[...]).astype(BF16)
        part[q, :, 2 * F :] = dot(cots, down_f[...], 1, 1).astype(BF16)


def grads_kernel(sc, part, info, out):
    total = part[0].astype(F32)
    for q in range(1, TP):
        total = total + part[q].astype(F32)
    pre_gate = total[:, 0:F]
    pre_up = total[:, F : 2 * F]
    back = total[:, 2 * F :]
    about = info[...].astype(F32)
    gating = about[:, 0:1] + about[:, 1:2] + about[:, 2:3]
    sig = jax.nn.sigmoid(pre_gate)
    activated = pre_gate * sig
    slope = sig * (1.0 + pre_gate * (1.0 - sig))
    hidden = (activated * pre_up).astype(BF16).astype(F32)
    gg = jnp.sum(hidden * back, axis=1, keepdims=True)
    scaled = gating * back
    lane = iota((128, 128), 1)
    tail = jnp.zeros((128, 128), F32)
    for c, v in enumerate(pieces(gg)):
        tail = jnp.where(lane == c, v, tail)
    values = (scaled * pre_up * slope, scaled * activated, gating * hidden)
    for q in range(TP):
        for c, v in enumerate(values):
            out[q, :, F * c : F * (c + 1)] = v.astype(BF16)
        out[q, :, 3 * F :] = tail.astype(BF16)


def row_sums(x):
    n, width = x.shape
    acc = x[:, 0:128]
    for c in range(1, width // 128):
        acc = acc + x[:, 128 * c : 128 * (c + 1)]
    return jnp.concatenate(
        [jnp.sum(acc[128 * c : 128 * (c + 1), :].T, axis=0, keepdims=True) for c in range(n // 128)],
        axis=0,
    )


def back_kernel(sc, grads, tok_c, cot_c, info_c, gate_f, up_f, send, *outs):
    p = sc[0]
    own_expert = sc[1]
    g_gate = grads[:, 0:F]
    g_up = grads[:, F : 2 * F]
    toks = tok_c[...]
    cots = cot_c[...]
    back = (dot(g_gate, gate_f[...], 1, 1) + dot(g_up, up_f[...], 1, 1)).astype(BF16)
    tail = grads[:, 3 * F :]
    wide = tail.astype(F32)
    gg = wide[:, 0:1] + wide[:, 1:2] + wide[:, 2:3]
    about = info_c[...].astype(F32)
    own = (about[:, 3:4] + about[:, 4:5] + about[:, 5:6]) * gg
    other = (about[:, 6:7] + about[:, 7:8] + about[:, 8:9]) * gg
    other_expert = about[:, 9:10].astype(jnp.int32)
    lane = iota((ROWS, EXPERTS), 1)
    mix = jnp.where(lane == own_expert, own, 0.0) - jnp.where(lane == other_expert, other, 0.0)
    mix_hi = mix.astype(BF16)
    mix_lo = (mix - mix_hi.astype(F32)).astype(BF16)
    router = (dot(toks, mix_hi, 0, 0) + dot(toks, mix_lo, 0, 0)).astype(BF16)
    sel_t = to_rows(0)
    sel_c = to_rows(1)
    half = DQ // 2
    for q in range(TP):
        rows = slice(128 * q, 128 * (q + 1))
        dest = slice(256 * q, 256 * (q + 1))
        send[dest, 0:half] = (
            dot(sel_t, back[rows, 0:half], 0, 0) + dot(sel_c, back[rows, half:], 0, 0)
        ).astype(BF16)
        send[dest, half : half + 128] = (
            dot(sel_t, router[rows, :], 0, 0) + dot(sel_c, tail[rows, :], 0, 0)
        ).astype(BF16)
    acc_gate = jnp.zeros((DQ, FQ), F32)
    acc_up = jnp.zeros((DQ, FQ), F32)
    for d, out in enumerate(outs):
        f = (p + d) % TP
        gate_sum = dot(toks, grads[:, pl.ds(aligned(f, FQ), FQ)], 0, 0)
        up_sum = dot(toks, grads[:, pl.ds(aligned(f + TP, FQ), FQ)], 0, 0)
        down_sum = dot(grads[:, pl.ds(aligned(f + 2 * TP, FQ), FQ)], cots, 0, 0)
        acc_gate = acc_gate + gate_sum * gate_sum
        acc_up = acc_up + up_sum * up_sum
        out[0:DQ, :] = gate_sum.astype(BF16)
        out[DQ : 2 * DQ, :] = up_sum.astype(BF16)
        for c in range(4):
            out[2 * DQ + 128 * c : 2 * DQ + 128 * (c + 1), :] = down_sum[
                :, 128 * c : 128 * (c + 1)
            ].astype(BF16)
        hi, mid, lo = pieces(row_sums(down_sum * down_sum))
        line = iota((8, 128), 0)
        last = jnp.where(line == 0, hi, jnp.where(line == 1, mid, jnp.where(line == 2, lo, 0.0)))
        out[3 * DQ + 24 : 3 * DQ + 32, :] = last.astype(BF16)
    both = jnp.concatenate([row_sums(acc_gate), row_sums(acc_up)], axis=0)
    norms = jnp.concatenate(pieces(both), axis=0).astype(BF16)
    for out in outs:
        out[3 * DQ : 3 * DQ + 24, :] = norms


def router_kernel(sc, got, out):
    pick = (iota((8, SENT), 0) == iota((8, SENT), 1) % 8).astype(BF16)
    out[...] = dot(pick, got[...])[0:4, :]


def home_kernel(sc, got, match0, match1, stats, routing, router, grad_tokens, grad_gating):
    sub = iota((SENT, TOK), 0) % 8
    m0 = match0[...].astype(F32)
    m1 = match1[...].astype(F32)
    both = m0 + m1
    first = jnp.where(sub < 4, both, 0.0).astype(BF16)
    second = jnp.where(sub < 4, 0.0, both).astype(BF16)
    half = DQ // 2
    tail = got[:, half : half + 128]
    at = [jnp.where(sub < 4, 0.0, m).astype(BF16) for m in (m0, m1)]
    rows = []
    cols = []
    for m in at:
        r = dot(tail, m, 0, 0)
        rows.append(r[0:1, :] + r[1:2, :] + r[2:3, :])
        c = dot(m, tail, 0, 0)
        cols.append(c[:, 0:1] + c[:, 1:2] + c[:, 2:3])
    grad_gating[...] = jnp.where(iota((TOK, 2), 1) == 0, cols[0], cols[1])
    st = stats[...]
    total = st[2:3, :]
    weighted = st[3:4, :] * rows[0] + st[4:5, :] * rows[1]
    experts = iota((EXPERTS, TOK), 0)
    logits = jnp.zeros((EXPERTS, TOK), F32)
    for k in range(2):
        s = st[k : k + 1, :]
        chosen = (rows[k] - weighted) / total * s * (1.0 - s)
        logits = jnp.where(experts == routing[k : k + 1, :], chosen, logits)
    logits = logits.astype(BF16)
    term = dot(logits, router[...], 0, 1)
    grad_tokens[:, 0:half] = (dot(first, got[:, 0:half], 0, 0) + term[:, 0:half]).astype(BF16)
    grad_tokens[:, half:] = (dot(second, got[:, 0:half], 0, 0) + term[:, half:]).astype(BF16)


def weights_kernel(sc, own, x1, x2, x3, gate, up, down, in_norms, down_norms):
    p = sc[0]
    total = None
    for d, x in enumerate((own, x1, x2, x3)):
        q = (p + TP - d) % TP
        gate[pl.ds(aligned(q, DQ), DQ), :] = x[0:DQ, :]
        up[pl.ds(aligned(q, DQ), DQ), :] = x[DQ : 2 * DQ, :]
        for c in range(4):
            down[:, pl.ds(aligned(q * 4 + c, 128), 128)] = x[
                2 * DQ + 128 * c : 2 * DQ + 128 * (c + 1), :
            ]
        tail = x[3 * DQ : 3 * DQ + 32, :].astype(F32)
        norms = tail[0:8, :] + tail[8:16, :] + tail[16:24, :]
        for c in range(4):
            at = pl.ds(aligned(q * 4 + c, 128), 128)
            in_norms[0:1, at] = norms[c : c + 1, :]
            in_norms[1:2, at] = norms[4 + c : 5 + c, :]
        part = tail[24:25, :] + tail[25:26, :] + tail[26:27, :]
        total = part if total is None else total + part
    down_norms[...] = total


def shards(tokens, cotangent, routing, router_weight, gate_weight, up_weight, down_weight):
    tp_index = lax.axis_index("tp")
    ep_index = lax.axis_index(EP)
    sc = jnp.stack([tp_index, ep_index]).astype(jnp.int32)
    routing_t = routing.T
    gate_w = gate_weight[0]
    up_w = up_weight[0]
    down_w = down_weight[0]
    feature_block = pl.BlockSpec((TOK, DQ), lambda g, p: (0, p[0]))
    row_block = pl.BlockSpec((DQ, 128), lambda g, p: (p[0], 0))

    send, match0, match1, stats = call(
        dispatch_kernel,
        "dispatch",
        sc,
        (tokens, tokens, cotangent, routing_t, router_weight),
        (whole((TOK, D)), feature_block, feature_block, whole((2, TOK)), whole((D, EXPERTS))),
        (
            sds((SENT, DQ + 128), BF16),
            sds((SENT, TOK), BF16),
            sds((SENT, TOK), BF16),
            sds((8, TOK), F32),
        ),
    )
    got = lax.all_to_all(send.reshape(EXPERTS, 8, DQ + 128), EP, 0, 0, tiled=True)

    def shift(d):
        return [(a, (a + d) % TP) for a in range(TP)]

    packed = call(
        pack_kernel,
        "pack",
        sc,
        (gate_w, up_w, down_w),
        (whole((D, FQ)), whole((D, FQ)), whole((FQ, D))),
        (sds((3 * DQ, FQ), BF16),) * 3,
    )
    w = [lax.ppermute(x, "tp", shift(d)) for d, x in enumerate(packed, 1)]

    tok_c, cot_c, info_c, part, gate_f, up_f, down_f = call(
        hidden_kernel,
        "hidden",
        sc,
        (got.reshape(SENT, DQ + 128), gate_w, up_w, down_w, *w),
        (
            whole((SENT, DQ + 128)),
            row_block,
            row_block,
            pl.BlockSpec((FQ, DQ), lambda g, p: (0, p[0])),
            *(whole((3 * DQ, FQ)),) * 3,
        ),
        (
            sds((ROWS, DQ), BF16),
            sds((ROWS, DQ), BF16),
            sds((ROWS, 128), BF16),
            sds((TP, 128, 3 * F), BF16),
            sds((DQ, F), BF16),
            sds((DQ, F), BF16),
            sds((F, DQ), BF16),
        ),
    )
    parts = lax.all_to_all(part, "tp", 0, 0, tiled=True)
    (grads,) = call(
        grads_kernel,
        "grads",
        sc,
        (parts, info_c),
        (whole((TP, 128, 3 * F)), pl.BlockSpec((128, 128), lambda g, p: (p[0], 0))),
        (sds((TP, 128, 3 * F + 128), BF16),),
    )
    all_grads = lax.all_to_all(grads, "tp", 0, 0, tiled=True).reshape(ROWS, 3 * F + 128)
    send_back, *blocks = call(
        back_kernel,
        "back",
        sc,
        (all_grads, tok_c, cot_c, info_c, gate_f, up_f),
        (
            whole((ROWS, 3 * F + 128)),
            whole((ROWS, DQ)),
            whole((ROWS, DQ)),
            whole((ROWS, 128)),
            whole((DQ, F)),
            whole((DQ, F)),
        ),
        (sds((SENT, DQ // 2 + 128), BF16),) + (sds((3 * DQ + 32, 128), BF16),) * 4,
    )
    home = lax.all_to_all(
        send_back.reshape(EXPERTS, 8, DQ // 2 + 128), EP, 0, 0, tiled=True
    ).reshape(SENT, DQ // 2 + 128)
    x = [lax.ppermute(b, "tp", shift(d)) for d, b in enumerate(blocks[1:], 1)]
    grad_gate, grad_up, grad_down, in_norms, down_norms = call(
        weights_kernel,
        "weights",
        sc,
        (blocks[0], *x),
        (whole((3 * DQ + 32, 128)),) * 4,
        (
            sds((D, FQ), BF16),
            sds((D, FQ), BF16),
            sds((FQ, D), BF16),
            sds((2, D), F32),
            sds((1, FQ), F32),
        ),
    )
    (own_rows,) = call(
        router_kernel,
        "router",
        sc,
        (home,),
        (pl.BlockSpec((SENT, 128), lambda g, p: (0, 2)),),
        (sds((4, EXPERTS), F32),),
    )
    near = lax.all_gather(own_rows, NEAR, axis=0, tiled=True)
    moves = [
        (i * TP + p, (32 * p + i // 4) * TP + i % 4) for i in range(EXPERTS) for p in range(TP)
    ]
    grad_router = lax.ppermute(near, ALL, moves)
    grad_tokens, grad_gating = call(
        home_kernel,
        "home",
        sc,
        (home, match0, match1, stats, routing_t, router_weight),
        (
            whole((SENT, DQ // 2 + 128)),
            whole((SENT, TOK)),
            whole((SENT, TOK)),
            whole((8, TOK)),
            whole((2, TOK)),
            row_block,
        ),
        (sds((TOK, DQ), BF16), sds((TOK, 2), F32)),
    )
    router_norms = jnp.sum(grad_router * grad_router, axis=1)
    return (
        grad_tokens,
        grad_gating,
        grad_router,
        grad_gate[None],
        grad_up[None],
        grad_down[None],
        in_norms[None],
        down_norms,
        router_norms,
    )


def solution(mesh):
    split = Mesh(mesh.devices.reshape(8, 4, 2, 2, TP), ("ep_0", "ep_1", "ep_3", "ep_2", "tp"))
    in_specs = (
        P(EP, None),
        P(EP, None),
        P(EP, None),
        P(),
        P(EP, None, "tp"),
        P(EP, None, "tp"),
        P(EP, "tp", None),
    )
    out_specs = (
        P(EP, "tp"),
        P(EP, None),
        P(EP, None),
        P(EP, None, "tp"),
        P(EP, None, "tp"),
        P(EP, "tp", None),
        P(EP, None, None),
        P(EP, "tp"),
        P(EP),
    )
    return jax.shard_map(
        shards, mesh=split, in_specs=in_specs, out_specs=out_specs, check_vma=False
    )
```

```python
import functools

import jax
import jax.numpy as jnp
from jax import lax
from jax.experimental import pallas as pl
from jax.experimental.pallas import tpu as pltpu
from jax.sharding import Mesh
from jax.sharding import PartitionSpec as P

EP = ("ep_0", "ep_1", "ep_3", "ep_2")
NEAR = ("ep_3", "ep_2")
ALL = EP + ("tp",)
F32 = jnp.float32
BF16 = jnp.bfloat16


TOK = 128
D = 2048
EXPERTS = 128
CAP = 4
TP = 4
DQ = D // TP
F = 512
FQ = F // TP
ROWS = EXPERTS * CAP
SENT = EXPERTS * 8


def dot(a, b, ca=1, cb=0):
    return lax.dot_general(a, b, (((ca,), (cb,)), ((), ())), preferred_element_type=F32)


def iota(shape, dim):
    return lax.broadcasted_iota(jnp.int32, shape, dim)


def pieces(x):
    hi = x.astype(BF16).astype(F32)
    rest = x - hi
    mid = rest.astype(BF16).astype(F32)
    return hi, mid, rest - mid


def aligned(x, n):
    return pl.multiple_of(x * n, n)


def to_rows(half):
    slot = iota((128, 256), 0)
    row = iota((128, 256), 1)
    return ((row // 8 == slot // 4) & (row % 8 == slot % 4 + 4 * half)).astype(BF16)


ON_CHIP = pl.BlockSpec(memory_space=pltpu.VMEM)


def call(kernel, name, scalars, ins, outs, scratch=()):
    arrays = []
    specs = []
    for x in ins:
        if isinstance(x, tuple):
            arrays.append(x[0])
            specs.append(x[1])
        else:
            arrays.append(pltpu.with_memory_space_constraint(x, pltpu.VMEM))
            specs.append(ON_CHIP)
    return pl.pallas_call(
        kernel,
        name=name,
        grid_spec=pltpu.PrefetchScalarGridSpec(
            num_scalar_prefetch=1,
            grid=(1,),
            in_specs=tuple(specs),
            out_specs=(ON_CHIP,) * len(outs),
            scratch_shapes=scratch,
        ),
        out_shape=tuple(outs),
        compiler_params=pltpu.CompilerParams(vmem_limit_bytes=32 << 20),
    )(scalars, *arrays)


def whole(x):
    return (x, pl.BlockSpec(x.shape, lambda g, p: (0,) * x.ndim))


def sds(shape, dtype):
    return jax.ShapeDtypeStruct(shape, dtype)


def hbm(shape, dtype):
    return pltpu.HBM(shape, dtype)


def vmem(shape, dtype):
    return pltpu.VMEM(shape, dtype)


def dispatch_kernel(sc, tok, tok_q, cot_q, routing, router, send, match0, match1, stats):
    experts = iota((EXPERTS, TOK), 0)
    picked = [(experts == routing[k : k + 1, :]) for k in range(2)]
    both = (picked[0] | picked[1]).astype(F32)
    logits = dot(router[...], tok[...], 0, 1)
    s = [
        jax.nn.sigmoid(jnp.sum(jnp.where(m, logits, 0.0), axis=0, keepdims=True)) for m in picked
    ]
    total = s[0] + s[1]
    g = [v / total for v in s]
    slope = [v * (1.0 - v) / total for v in s]
    before = (iota((TOK, TOK), 0) < iota((TOK, TOK), 1)).astype(BF16)
    within = dot(both.astype(BF16), before)
    repeat = (iota((SENT, EXPERTS), 0) // 8 == iota((SENT, EXPERTS), 1)).astype(BF16)
    sub = (iota((SENT, TOK), 0) % 8).astype(F32)
    slot = jnp.where(sub < 4.0, sub, sub - 4.0)
    line = iota((128, TOK), 0)
    found = []
    info = None
    for k, out in ((0, match0), (1, match1)):
        place = jnp.where(picked[k], within, -1.0).astype(BF16)
        one = jnp.where(dot(repeat, place) == slot, 1.0, 0.0)
        out[...] = one.astype(BF16)
        found.append(one)
        own = slope[k] * g[1 - k]
        other = slope[1 - k] * g[k]
        columns = [*pieces(g[k]), *pieces(own), *pieces(other), routing[1 - k : 2 - k, :].astype(F32)]
        table = jnp.zeros((128, TOK), F32)
        for c, v in enumerate(columns):
            table = jnp.where(line == c, v, table)
        part = dot(one.astype(BF16), table.astype(BF16), 1, 1)
        info = part if info is None else info + part
    any_one = found[0] + found[1]
    first = jnp.where(sub < 4.0, any_one, 0.0).astype(BF16)
    second = jnp.where(sub < 4.0, 0.0, any_one).astype(BF16)
    send[:, 0:DQ] = (dot(first, tok_q[...]) + dot(second, cot_q[...])).astype(BF16)
    send[:, DQ : DQ + 128] = info.astype(BF16)
    stats[...] = jnp.concatenate(
        [s[0], s[1], total, g[0], g[1], total, total, total], axis=0
    )


def pack_kernel(sc, gate, up, down, *outs):
    p = sc[0]
    for d, out in enumerate(outs, 1):
        q = (p + d) % TP
        out[0:DQ, :] = gate[pl.ds(aligned(q, DQ), DQ), :]
        out[DQ : 2 * DQ, :] = up[pl.ds(aligned(q, DQ), DQ), :]
        for c in range(4):
            out[2 * DQ + 128 * c : 2 * DQ + 128 * (c + 1), :] = down[
                :, pl.ds(aligned(q * 4 + c, 128), 128)
            ]


def hidden_kernel(sc, got, gate, up, down, w1, w2, w3, tok_c, cot_c, info_c, part, gate_f, up_f, down_f):
    p = sc[0]
    here = aligned(p, FQ)
    gate_f[:, pl.ds(here, FQ)] = gate[...]
    up_f[:, pl.ds(here, FQ)] = up[...]
    down_f[pl.ds(here, FQ), :] = down[...]
    for d, w in ((1, w1), (2, w2), (3, w3)):
        f = aligned((p + TP - d) % TP, FQ)
        gate_f[:, pl.ds(f, FQ)] = w[0:DQ, :]
        up_f[:, pl.ds(f, FQ)] = w[DQ : 2 * DQ, :]
        for c in range(4):
            down_f[pl.ds(f, FQ), 128 * c : 128 * (c + 1)] = w[
                2 * DQ + 128 * c : 2 * DQ + 128 * (c + 1), :
            ]
    sel_t = to_rows(0)
    sel_c = to_rows(1)
    for q in range(TP):
        block = got[256 * q : 256 * (q + 1), :]
        mine = dot(sel_t, block).astype(BF16)
        cots = dot(sel_c, block[:, 0:DQ]).astype(BF16)
        toks = mine[:, 0:DQ]
        rows = slice(128 * q, 128 * (q + 1))
        tok_c[rows, :] = toks
        cot_c[rows, :] = cots
        info_c[rows, :] = mine[:, DQ:]
        part[q, :, 0:F] = dot(toks, gate_f[...]).astype(BF16)
        part[q, :, F : 2 * F] = dot(toks, up_f[...]).astype(BF16)
        part[q, :, 2 * F :] = dot(cots, down_f[...], 1, 1).astype(BF16)


def grads_kernel(sc, part, info, out):
    here = aligned(sc[0], 128)
    total = part[0].astype(F32)
    for q in range(1, TP):
        total = total + part[q].astype(F32)
    pre_gate = total[:, 0:F]
    pre_up = total[:, F : 2 * F]
    back = total[:, 2 * F :]
    about = info[pl.ds(here, 128), :].astype(F32)
    gating = about[:, 0:1] + about[:, 1:2] + about[:, 2:3]
    sig = jax.nn.sigmoid(pre_gate)
    activated = pre_gate * sig
    slope = sig * (1.0 + pre_gate * (1.0 - sig))
    hidden = (activated * pre_up).astype(BF16).astype(F32)
    gg = jnp.sum(hidden * back, axis=1, keepdims=True)
    scaled = gating * back
    lane = iota((128, 128), 1)
    tail = jnp.zeros((128, 128), F32)
    for c, v in enumerate(pieces(gg)):
        tail = jnp.where(lane == c, v, tail)
    values = (scaled * pre_up * slope, scaled * activated, gating * hidden)
    for q in range(TP):
        for c, v in enumerate(values):
            out[q, :, F * c : F * (c + 1)] = v.astype(BF16)
        out[q, :, 3 * F :] = tail.astype(BF16)


def row_sums(x):
    n, width = x.shape
    acc = x[:, 0:128]
    for c in range(1, width // 128):
        acc = acc + x[:, 128 * c : 128 * (c + 1)]
    return jnp.concatenate(
        [jnp.sum(acc[128 * c : 128 * (c + 1), :].T, axis=0, keepdims=True) for c in range(n // 128)],
        axis=0,
    )


def back_kernel(sc, grads, tok_c, info_c, gate_f, up_f, send):
    own_expert = sc[1]
    back = (dot(grads[:, 0:F], gate_f[...], 1, 1) + dot(grads[:, F : 2 * F], up_f[...], 1, 1)).astype(BF16)
    tail = grads[:, 3 * F :]
    wide = tail.astype(F32)
    gg = wide[:, 0:1] + wide[:, 1:2] + wide[:, 2:3]
    about = info_c[...].astype(F32)
    own = (about[:, 3:4] + about[:, 4:5] + about[:, 5:6]) * gg
    other = (about[:, 6:7] + about[:, 7:8] + about[:, 8:9]) * gg
    other_expert = about[:, 9:10].astype(jnp.int32)
    lane = iota((ROWS, EXPERTS), 1)
    mix = jnp.where(lane == own_expert, own, 0.0) - jnp.where(lane == other_expert, other, 0.0)
    mix_hi = mix.astype(BF16)
    mix_lo = (mix - mix_hi.astype(F32)).astype(BF16)
    router = dot(tok_c[...], jnp.concatenate([mix_hi, mix_lo], axis=1), 0, 0)
    router = (router[:, 0:EXPERTS] + router[:, EXPERTS:]).astype(BF16)
    sel_t = to_rows(0)
    sel_c = to_rows(1)
    half = DQ // 2
    for q in range(TP):
        rows = slice(128 * q, 128 * (q + 1))
        first = jnp.concatenate([back[rows, 0:half], router[rows, :]], axis=1)
        second = jnp.concatenate([back[rows, half:], tail[rows, :]], axis=1)
        send[256 * q : 256 * (q + 1), :] = (dot(sel_t, first, 0, 0) + dot(sel_c, second, 0, 0)).astype(BF16)


def sums_kernel(sc, grads, tok_c, cot_c, *outs):
    p = sc[0]
    toks = tok_c[...].T
    cots = cot_c[...]
    acc_gate = jnp.zeros((DQ, FQ), F32)
    acc_up = jnp.zeros((DQ, FQ), F32)
    for d, out in enumerate(outs):
        f = (p + d) % TP
        gate_sum = dot(toks, grads[:, pl.ds(aligned(f, FQ), FQ)])
        up_sum = dot(toks, grads[:, pl.ds(aligned(f + TP, FQ), FQ)])
        down_sum = dot(grads[:, pl.ds(aligned(f + 2 * TP, FQ), FQ)], cots, 0, 0)
        acc_gate = acc_gate + gate_sum * gate_sum
        acc_up = acc_up + up_sum * up_sum
        out[0:DQ, :] = gate_sum.astype(BF16)
        out[DQ : 2 * DQ, :] = up_sum.astype(BF16)
        for c in range(4):
            out[2 * DQ + 128 * c : 2 * DQ + 128 * (c + 1), :] = down_sum[
                :, 128 * c : 128 * (c + 1)
            ].astype(BF16)
        hi, mid, lo = pieces(row_sums(down_sum * down_sum))
        line = iota((8, 128), 0)
        last = jnp.where(line == 0, hi, jnp.where(line == 1, mid, jnp.where(line == 2, lo, 0.0)))
        out[3 * DQ + 24 : 3 * DQ + 32, :] = last.astype(BF16)
    both = jnp.concatenate([row_sums(acc_gate), row_sums(acc_up)], axis=0)
    norms = jnp.concatenate(pieces(both), axis=0).astype(BF16)
    for out in outs:
        out[3 * DQ : 3 * DQ + 24, :] = norms


def router_kernel(sc, got, out):
    half = DQ // 2
    pick = (iota((8, SENT), 0) == iota((8, SENT), 1) % 8).astype(BF16)
    out[...] = dot(pick, got[:, half : half + 128])[0:4, :]


def home_kernel(sc, got, match0, match1, stats, routing, router, grad_tokens, grad_gating):
    sub = iota((SENT, TOK), 0) % 8
    m0 = match0[...].astype(F32)
    m1 = match1[...].astype(F32)
    both = m0 + m1
    first = jnp.where(sub < 4, both, 0.0).astype(BF16)
    second = jnp.where(sub < 4, 0.0, both).astype(BF16)
    half = DQ // 2
    tail = got[:, half : half + 128]
    at = [jnp.where(sub < 4, 0.0, m).astype(BF16) for m in (m0, m1)]
    rows = []
    for m in at:
        r = dot(tail, m, 0, 0)
        rows.append(r[0:1, :] + r[1:2, :] + r[2:3, :])
    grad_gating[...] = jnp.concatenate(rows, axis=0)
    st = stats[...]
    total = st[2:3, :]
    weighted = st[3:4, :] * rows[0] + st[4:5, :] * rows[1]
    experts = iota((EXPERTS, TOK), 0)
    logits = jnp.zeros((EXPERTS, TOK), F32)
    for k in range(2):
        s = st[k : k + 1, :]
        chosen = (rows[k] - weighted) / total * s * (1.0 - s)
        logits = jnp.where(experts == routing[k : k + 1, :], chosen, logits)
    logits = logits.astype(BF16)
    term = dot(logits, router[...], 0, 1)
    grad_tokens[:, 0:half] = (dot(first, got[:, 0:half], 0, 0) + term[:, 0:half]).astype(BF16)
    grad_tokens[:, half:] = (dot(second, got[:, 0:half], 0, 0) + term[:, half:]).astype(BF16)


def weights_kernel(sc, own, x1, x2, x3, gate, up, down, in_norms, down_norms):
    p = sc[0]
    total = None
    for d, x in enumerate((own, x1, x2, x3)):
        q = (p + TP - d) % TP
        gate[pl.ds(aligned(q, DQ), DQ), :] = x[0:DQ, :]
        up[pl.ds(aligned(q, DQ), DQ), :] = x[DQ : 2 * DQ, :]
        for c in range(4):
            down[:, pl.ds(aligned(q * 4 + c, 128), 128)] = x[
                2 * DQ + 128 * c : 2 * DQ + 128 * (c + 1), :
            ]
        tail = x[3 * DQ : 3 * DQ + 32, :].astype(F32)
        norms = tail[0:8, :] + tail[8:16, :] + tail[16:24, :]
        for c in range(4):
            at = pl.ds(aligned(q * 4 + c, 128), 128)
            in_norms[0:1, at] = norms[c : c + 1, :]
            in_norms[1:2, at] = norms[4 + c : 5 + c, :]
        part = tail[24:25, :] + tail[25:26, :] + tail[26:27, :]
        total = part if total is None else total + part
    down_norms[...] = total


def shards(tokens, cotangent, routing, router_weight, gate_weight, up_weight, down_weight):
    tp_index = lax.axis_index("tp")
    ep_index = lax.axis_index(EP)
    sc = jnp.stack([tp_index, ep_index]).astype(jnp.int32)
    routing_t = routing.T
    gate_w = gate_weight[0]
    up_w = up_weight[0]
    down_w = down_weight[0]
    feature_block = pl.BlockSpec((TOK, DQ), lambda g, p: (0, p[0]))
    row_block = pl.BlockSpec((DQ, 128), lambda g, p: (p[0], 0))

    send, match0, match1, stats = call(
        dispatch_kernel,
        "dispatch",
        sc,
        (
            whole(tokens),
            (tokens, feature_block),
            (cotangent, feature_block),
            whole(routing_t),
            whole(router_weight),
        ),
        (
            hbm((SENT, DQ + 128), BF16),
            hbm((SENT, TOK), BF16),
            hbm((SENT, TOK), BF16),
            hbm((8, TOK), F32),
        ),
    )
    got = lax.all_to_all(send.reshape(EXPERTS, 8, DQ + 128), EP, 0, 0, tiled=True)

    def shift(d):
        return [(a, (a + d) % TP) for a in range(TP)]

    packed = call(
        pack_kernel,
        "pack",
        sc,
        (whole(gate_w), whole(up_w), whole(down_w)),
        (vmem((3 * DQ, FQ), BF16),) * 3,
    )
    w = [lax.ppermute(x, "tp", shift(d)) for d, x in enumerate(packed, 1)]

    tok_c, cot_c, info_c, part, gate_f, up_f = call(
        hidden_kernel,
        "hidden",
        sc,
        (
            got.reshape(SENT, DQ + 128),
            (gate_w, row_block),
            (up_w, row_block),
            (down_w, pl.BlockSpec((FQ, DQ), lambda g, p: (0, p[0]))),
            *(whole(pltpu.with_memory_space_constraint(x, pltpu.HBM)) for x in w),
        ),
        (
            hbm((ROWS, DQ), BF16),
            hbm((ROWS, DQ), BF16),
            hbm((ROWS, 128), BF16),
            vmem((TP, 128, 3 * F), BF16),
            hbm((DQ, F), BF16),
            hbm((DQ, F), BF16),
        ),
        (pltpu.VMEM((F, DQ), BF16),),
    )
    parts = lax.all_to_all(part, "tp", 0, 0, tiled=True)
    (grads,) = call(
        grads_kernel, "grads", sc, (parts, whole(info_c)), (vmem((TP, 128, 3 * F + 128), BF16),)
    )
    all_grads = lax.all_to_all(grads, "tp", 0, 0, tiled=True).reshape(ROWS, 3 * F + 128)
    (send_back,) = call(
        back_kernel,
        "back",
        sc,
        (all_grads, whole(tok_c), whole(info_c), whole(gate_f), whole(up_f)),
        (hbm((SENT, DQ // 2 + 128), BF16),),
    )
    home = lax.all_to_all(
        send_back.reshape(EXPERTS, 8, DQ // 2 + 128), EP, 0, 0, tiled=True
    ).reshape(SENT, DQ // 2 + 128)
    blocks = call(
        sums_kernel,
        "sums",
        sc,
        (whole(all_grads), whole(tok_c), whole(cot_c)),
        (hbm((3 * DQ + 32, 128), BF16),) + (vmem((3 * DQ + 32, 128), BF16),) * 3,
    )
    x = [lax.ppermute(b, "tp", shift(d)) for d, b in enumerate(blocks[1:], 1)]
    grad_gate, grad_up, grad_down, in_norms, down_norms = call(
        weights_kernel,
        "weights",
        sc,
        tuple(map(whole, (blocks[0], *x))),
        (
            sds((D, FQ), BF16),
            sds((D, FQ), BF16),
            sds((FQ, D), BF16),
            sds((2, D), F32),
            sds((1, FQ), F32),
        ),
    )
    (own_rows,) = call(router_kernel, "router", sc, (home,), (vmem((4, EXPERTS), F32),))
    near = lax.all_gather(own_rows, NEAR, axis=0, tiled=True)
    moves = [
        (i * TP + p, (32 * p + i // 4) * TP + i % 4) for i in range(EXPERTS) for p in range(TP)
    ]
    grad_router = lax.ppermute(near, ALL, moves)
    grad_tokens, grad_gating = call(
        home_kernel,
        "home",
        sc,
        (home, whole(match0), whole(match1), whole(stats), whole(routing_t), (router_weight, row_block)),
        (sds((TOK, DQ), BF16), sds((2, TOK), F32)),
    )
    router_norms = jnp.sum(grad_router * grad_router, axis=1)
    return (
        grad_tokens,
        grad_gating.T,
        grad_router,
        grad_gate[None],
        grad_up[None],
        grad_down[None],
        in_norms[None],
        down_norms,
        router_norms,
    )


def solution(mesh):
    split = Mesh(mesh.devices.reshape(8, 4, 2, 2, TP), ("ep_0", "ep_1", "ep_3", "ep_2", "tp"))
    in_specs = (
        P(EP, None),
        P(EP, None),
        P(EP, None),
        P(),
        P(EP, None, "tp"),
        P(EP, None, "tp"),
        P(EP, "tp", None),
    )
    out_specs = (
        P(EP, "tp"),
        P(EP, None),
        P(EP, None),
        P(EP, None, "tp"),
        P(EP, None, "tp"),
        P(EP, "tp", None),
        P(EP, None, None),
        P(EP, "tp"),
        P(EP),
    )
    return jax.shard_map(
        shards, mesh=split, in_specs=in_specs, out_specs=out_specs, check_vma=False
    )
```

```python
import functools

import jax
import jax.numpy as jnp
from jax import lax
from jax.experimental import pallas as pl
from jax.experimental.pallas import tpu as pltpu
from jax.sharding import Mesh
from jax.sharding import PartitionSpec as P

EP = ("ep_0", "ep_1", "ep_3", "ep_2")
NEAR = ("ep_3", "ep_2")
ALL = EP + ("tp",)
F32 = jnp.float32
BF16 = jnp.bfloat16


TOK = 128
D = 2048
EXPERTS = 128
CAP = 4
TP = 4
DQ = D // TP
F = 512
FQ = F // TP
ROWS = EXPERTS * CAP
SENT = EXPERTS * 8


def dot(a, b, ca=1, cb=0):
    return lax.dot_general(a, b, (((ca,), (cb,)), ((), ())), preferred_element_type=F32)


def iota(shape, dim):
    return lax.broadcasted_iota(jnp.int32, shape, dim)


def pieces(x):
    hi = x.astype(BF16).astype(F32)
    rest = x - hi
    mid = rest.astype(BF16).astype(F32)
    return hi, mid, rest - mid


def aligned(x, n):
    return pl.multiple_of(x * n, n)


def to_rows(half):
    slot = iota((128, 256), 0)
    row = iota((128, 256), 1)
    return ((row // 8 == slot // 4) & (row % 8 == slot % 4 + 4 * half)).astype(BF16)


ON_CHIP = pl.BlockSpec(memory_space=pltpu.VMEM)


def call(kernel, name, scalars, ins, outs, scratch=()):
    arrays = []
    specs = []
    for x in ins:
        if isinstance(x, tuple):
            arrays.append(x[0])
            specs.append(x[1])
        else:
            arrays.append(pltpu.with_memory_space_constraint(x, pltpu.VMEM))
            specs.append(ON_CHIP)
    return pl.pallas_call(
        kernel,
        name=name,
        grid_spec=pltpu.PrefetchScalarGridSpec(
            num_scalar_prefetch=1,
            grid=(1,),
            in_specs=tuple(specs),
            out_specs=(ON_CHIP,) * len(outs),
            scratch_shapes=scratch,
        ),
        out_shape=tuple(outs),
        compiler_params=pltpu.CompilerParams(vmem_limit_bytes=32 << 20),
    )(scalars, *arrays)


def whole(x):
    return (x, pl.BlockSpec(x.shape, lambda g, p: (0,) * x.ndim))


def sds(shape, dtype):
    return jax.ShapeDtypeStruct(shape, dtype)


def hbm(shape, dtype):
    return pltpu.HBM(shape, dtype)


def vmem(shape, dtype):
    return pltpu.VMEM(shape, dtype)


def expand():
    repeat = (iota((SENT, EXPERTS), 0) // 8 == iota((SENT, EXPERTS), 1)).astype(BF16)
    sub = (iota((SENT, TOK), 0) % 8).astype(F32)
    return repeat, sub, jnp.where(sub < 4.0, sub, sub - 4.0)


def dispatch_kernel(sc, tok, cot_q, routing, router, send, place0, place1, stats):
    own_part = pl.ds(aligned(sc[0], DQ), DQ)
    experts = iota((EXPERTS, TOK), 0)
    picked = [(experts == routing[k : k + 1, :]) for k in range(2)]
    both = (picked[0] | picked[1]).astype(F32)
    logits = dot(router[...], tok[...], 0, 1)
    s = [
        jax.nn.sigmoid(jnp.sum(jnp.where(m, logits, 0.0), axis=0, keepdims=True)) for m in picked
    ]
    total = s[0] + s[1]
    g = [v / total for v in s]
    slope = [v * (1.0 - v) / total for v in s]
    before = (iota((TOK, TOK), 0) < iota((TOK, TOK), 1)).astype(BF16)
    within = dot(both.astype(BF16), before)
    repeat, sub, slot = expand()
    line = iota((128, TOK), 0)
    found = []
    info = None
    for k, out in ((0, place0), (1, place1)):
        place = jnp.where(picked[k], within, -1.0).astype(BF16)
        out[...] = place
        one = jnp.where(dot(repeat, place) == slot, 1.0, 0.0)
        found.append(one)
        own = slope[k] * g[1 - k]
        other = slope[1 - k] * g[k]
        columns = [*pieces(g[k]), *pieces(own), *pieces(other), routing[1 - k : 2 - k, :].astype(F32)]
        table = jnp.zeros((128, TOK), F32)
        for c, v in enumerate(columns):
            table = jnp.where(line == c, v, table)
        part = dot(one.astype(BF16), table.astype(BF16), 1, 1)
        info = part if info is None else info + part
    any_one = found[0] + found[1]
    first = jnp.where(sub < 4.0, any_one, 0.0).astype(BF16)
    second = jnp.where(sub < 4.0, 0.0, any_one).astype(BF16)
    send[:, 0:DQ] = (dot(first, tok[:, own_part]) + dot(second, cot_q[...])).astype(BF16)
    send[:, DQ : DQ + 128] = info.astype(BF16)
    stats[...] = jnp.concatenate(
        [s[0], s[1], total, g[0], g[1], total, total, total], axis=0
    )


def pack_kernel(sc, gate, up, down, *outs):
    p = sc[0]
    for d, out in enumerate(outs, 1):
        q = (p + d) % TP
        out[0:DQ, :] = gate[pl.ds(aligned(q, DQ), DQ), :]
        out[DQ : 2 * DQ, :] = up[pl.ds(aligned(q, DQ), DQ), :]
        for c in range(4):
            out[2 * DQ + 128 * c : 2 * DQ + 128 * (c + 1), :] = down[
                :, pl.ds(aligned(q * 4 + c, 128), 128)
            ]


def assemble_kernel(sc, gate, up, down, w1, w2, w3, gate_f, up_f, down_f):
    p = sc[0]
    here = aligned(p, FQ)
    gate_f[:, pl.ds(here, FQ)] = gate[...]
    up_f[:, pl.ds(here, FQ)] = up[...]
    down_f[pl.ds(here, FQ), :] = down[...]
    for d, w in ((1, w1), (2, w2), (3, w3)):
        f = aligned((p + TP - d) % TP, FQ)
        gate_f[:, pl.ds(f, FQ)] = w[0:DQ, :]
        up_f[:, pl.ds(f, FQ)] = w[DQ : 2 * DQ, :]
        for c in range(4):
            down_f[pl.ds(f, FQ), 128 * c : 128 * (c + 1)] = w[
                2 * DQ + 128 * c : 2 * DQ + 128 * (c + 1), :
            ]


def hidden_kernel(d, sc, got, gate_f, up_f, down_f, tok_c, cot_c, info_c, part):
    q = (sc[0] + d) % TP
    block = got[pl.ds(aligned(q, 256), 256), :]
    mine = dot(to_rows(0), block).astype(BF16)
    cots = dot(to_rows(1), block[:, 0:DQ]).astype(BF16)
    toks = mine[:, 0:DQ]
    tok_c[...] = toks
    cot_c[...] = cots
    info_c[...] = mine[:, DQ:]
    part[:, 0:F] = dot(toks, gate_f[...]).astype(BF16)
    part[:, F : 2 * F] = dot(toks, up_f[...]).astype(BF16)
    part[:, 2 * F :] = dot(cots, down_f[...], 1, 1).astype(BF16)


def grads_kernel(sc, own, part1, part2, part3, info, main, side):
    total = own[...].astype(F32)
    for part in (part1, part2, part3):
        total = total + part[...].astype(F32)
    pre_gate = total[:, 0:F]
    pre_up = total[:, F : 2 * F]
    back = total[:, 2 * F :]
    about = info[...].astype(F32)
    gating = about[:, 0:1] + about[:, 1:2] + about[:, 2:3]
    sig = jax.nn.sigmoid(pre_gate)
    activated = pre_gate * sig
    slope = sig * (1.0 + pre_gate * (1.0 - sig))
    hidden = (activated * pre_up).astype(BF16).astype(F32)
    gg = jnp.sum(hidden * back, axis=1, keepdims=True)
    scaled = gating * back
    lane = iota((128, 128), 1)
    tail = jnp.zeros((128, 128), F32)
    for c, v in enumerate(pieces(gg)):
        tail = jnp.where(lane == c, v, tail)
    main[:, 0:F] = (scaled * pre_up * slope).astype(BF16)
    main[:, F : 2 * F] = (scaled * activated).astype(BF16)
    main[:, 2 * F :] = tail.astype(BF16)
    side[...] = (gating * hidden).astype(BF16)


def row_sums(x):
    n, width = x.shape
    acc = x[:, 0:128]
    for c in range(1, width // 128):
        acc = acc + x[:, 128 * c : 128 * (c + 1)]
    return jnp.concatenate(
        [jnp.sum(acc[128 * c : 128 * (c + 1), :].T, axis=0, keepdims=True) for c in range(n // 128)],
        axis=0,
    )


def back_kernel(sc, *refs):
    grads, tok_c, info_c = refs[0:4], refs[4:8], refs[8:12]
    gate_f, up_f, send = refs[12:]
    own_expert = sc[1]
    lane = iota((128, EXPERTS), 1)
    half = DQ // 2
    backs = []
    mixes = []
    for d in range(TP):
        g = grads[d]
        backs.append((dot(g[:, 0:F], gate_f[...], 1, 1) + dot(g[:, F : 2 * F], up_f[...], 1, 1)).astype(BF16))
        wide = g[:, 2 * F :].astype(F32)
        gg = wide[:, 0:1] + wide[:, 1:2] + wide[:, 2:3]
        about = info_c[d][...].astype(F32)
        own = (about[:, 3:4] + about[:, 4:5] + about[:, 5:6]) * gg
        other = (about[:, 6:7] + about[:, 7:8] + about[:, 8:9]) * gg
        other_expert = about[:, 9:10].astype(jnp.int32)
        mix = jnp.where(lane == own_expert, own, 0.0) - jnp.where(lane == other_expert, other, 0.0)
        mix_hi = mix.astype(BF16)
        mix_lo = (mix - mix_hi.astype(F32)).astype(BF16)
        mixes.append(jnp.concatenate([mix_hi, mix_lo], axis=1))
    toks = jnp.concatenate([t[...] for t in tok_c], axis=0)
    router = dot(toks, jnp.concatenate(mixes, axis=0), 0, 0)
    router = (router[:, 0:EXPERTS] + router[:, EXPERTS:]).astype(BF16)
    sel_t = to_rows(0)
    sel_c = to_rows(1)
    for q in range(TP):
        dest = slice(256 * q, 256 * (q + 1))
        send[dest, half : half + 128] = dot(sel_t, router[128 * q : 128 * (q + 1), :], 0, 0).astype(BF16)
    for d in range(TP):
        dest = pl.ds(aligned((sc[0] + d) % TP, 256), 256)
        tail = grads[d][:, 2 * F :]
        send[dest, 0:half] = (
            dot(sel_t, backs[d][:, 0:half], 0, 0) + dot(sel_c, backs[d][:, half:], 0, 0)
        ).astype(BF16)
        send[dest, half : half + 128] = (
            send[dest, half : half + 128].astype(F32) + dot(sel_c, tail, 0, 0)
        ).astype(BF16)


def sums_kernel(sc, *refs):
    p = sc[0]
    main, side, tok_c, cot_c = refs[0:4], refs[4:8], refs[8:12], refs[12:16]
    outs = refs[16:]
    toks = jnp.concatenate([t[...] for t in tok_c], axis=0).T
    cots = jnp.concatenate([t[...] for t in cot_c], axis=0)
    acc_gate = jnp.zeros((DQ, FQ), F32)
    acc_up = jnp.zeros((DQ, FQ), F32)
    for d, out in enumerate(outs):
        f = (p + d) % TP
        at_gate = pl.ds(aligned(f, FQ), FQ)
        at_up = pl.ds(aligned(f + TP, FQ), FQ)
        gate_sum = dot(toks, jnp.concatenate([g[:, at_gate] for g in main], axis=0))
        up_sum = dot(toks, jnp.concatenate([g[:, at_up] for g in main], axis=0))
        down_sum = dot(jnp.concatenate([g[:, at_gate] for g in side], axis=0), cots, 0, 0)
        acc_gate = acc_gate + gate_sum * gate_sum
        acc_up = acc_up + up_sum * up_sum
        out[0:DQ, :] = gate_sum.astype(BF16)
        out[DQ : 2 * DQ, :] = up_sum.astype(BF16)
        for c in range(4):
            out[2 * DQ + 128 * c : 2 * DQ + 128 * (c + 1), :] = down_sum[
                :, 128 * c : 128 * (c + 1)
            ].astype(BF16)
        hi, mid, lo = pieces(row_sums(down_sum * down_sum))
        line = iota((8, 128), 0)
        last = jnp.where(line == 0, hi, jnp.where(line == 1, mid, jnp.where(line == 2, lo, 0.0)))
        out[3 * DQ + 24 : 3 * DQ + 32, :] = last.astype(BF16)
    both = jnp.concatenate([row_sums(acc_gate), row_sums(acc_up)], axis=0)
    norms = jnp.concatenate(pieces(both), axis=0).astype(BF16)
    for out in outs:
        out[3 * DQ : 3 * DQ + 24, :] = norms


def router_kernel(sc, got, out):
    half = DQ // 2
    pick = (iota((8, SENT), 0) == iota((8, SENT), 1) % 8).astype(BF16)
    out[...] = dot(pick, got[:, half : half + 128])[0:4, :]


def home_kernel(sc, got, place0, place1, stats, routing, router, grad_tokens, grad_gating):
    repeat, sub, slot = expand()
    m0, m1 = (jnp.where(dot(repeat, x[...]) == slot, 1.0, 0.0) for x in (place0, place1))
    both = m0 + m1
    first = jnp.where(sub < 4.0, both, 0.0).astype(BF16)
    second = jnp.where(sub < 4.0, 0.0, both).astype(BF16)
    half = DQ // 2
    tail = got[:, half : half + 128]
    at = [jnp.where(sub < 4.0, 0.0, m).astype(BF16) for m in (m0, m1)]
    rows = []
    for m in at:
        r = dot(tail, m, 0, 0)
        rows.append(r[0:1, :] + r[1:2, :] + r[2:3, :])
    grad_gating[...] = jnp.concatenate(rows, axis=0)
    st = stats[...]
    total = st[2:3, :]
    weighted = st[3:4, :] * rows[0] + st[4:5, :] * rows[1]
    experts = iota((EXPERTS, TOK), 0)
    logits = jnp.zeros((EXPERTS, TOK), F32)
    for k in range(2):
        s = st[k : k + 1, :]
        chosen = (rows[k] - weighted) / total * s * (1.0 - s)
        logits = jnp.where(experts == routing[k : k + 1, :], chosen, logits)
    logits = logits.astype(BF16)
    term = dot(logits, router[...], 0, 1)
    grad_tokens[:, 0:half] = (dot(first, got[:, 0:half], 0, 0) + term[:, 0:half]).astype(BF16)
    grad_tokens[:, half:] = (dot(second, got[:, 0:half], 0, 0) + term[:, half:]).astype(BF16)


def finish_kernel(sc, got, grad_router, norms):
    x = got[...]
    grad_router[...] = x
    ones = jnp.ones((8, EXPERTS), F32)
    sums = lax.dot_general(
        ones,
        x * x,
        (((1,), (1,)), ((), ())),
        precision=lax.Precision.HIGHEST,
        preferred_element_type=F32,
    )
    norms[...] = sums[0:1, :]


def weights_kernel(sc, own, x1, x2, x3, gate, up, down, in_norms, down_norms):
    p = sc[0]
    total = None
    for d, x in enumerate((own, x1, x2, x3)):
        q = (p + TP - d) % TP
        gate[pl.ds(aligned(q, DQ), DQ), :] = x[0:DQ, :]
        up[pl.ds(aligned(q, DQ), DQ), :] = x[DQ : 2 * DQ, :]
        for c in range(4):
            down[:, pl.ds(aligned(q * 4 + c, 128), 128)] = x[
                2 * DQ + 128 * c : 2 * DQ + 128 * (c + 1), :
            ]
        tail = x[3 * DQ : 3 * DQ + 32, :].astype(F32)
        norms = tail[0:8, :] + tail[8:16, :] + tail[16:24, :]
        for c in range(4):
            at = pl.ds(aligned(q * 4 + c, 128), 128)
            in_norms[0:1, at] = norms[c : c + 1, :]
            in_norms[1:2, at] = norms[4 + c : 5 + c, :]
        part = tail[24:25, :] + tail[25:26, :] + tail[26:27, :]
        total = part if total is None else total + part
    down_norms[...] = total


def shards(tokens, cotangent, routing, router_weight, gate_weight, up_weight, down_weight):
    tp_index = lax.axis_index("tp")
    ep_index = lax.axis_index(EP)
    sc = jnp.stack([tp_index, ep_index]).astype(jnp.int32)
    routing_t = routing.T
    gate_w = gate_weight[0]
    up_w = up_weight[0]
    down_w = down_weight[0]
    feature_block = pl.BlockSpec((TOK, DQ), lambda g, p: (0, p[0]))
    row_block = pl.BlockSpec((DQ, 128), lambda g, p: (p[0], 0))

    far = functools.partial(pltpu.with_memory_space_constraint, memory_space=pltpu.HBM)
    send, place0, place1, stats = call(
        dispatch_kernel,
        "dispatch",
        sc,
        (
            whole(far(tokens)),
            (far(cotangent), feature_block),
            whole(far(routing_t)),
            whole(far(router_weight)),
        ),
        (
            hbm((SENT, DQ + 128), BF16),
            hbm((EXPERTS, TOK), BF16),
            hbm((EXPERTS, TOK), BF16),
            hbm((8, TOK), F32),
        ),
    )
    got = lax.all_to_all(send.reshape(EXPERTS, 8, DQ + 128), EP, 0, 0, tiled=True)

    def shift(x, d):
        return lax.ppermute(x, "tp", [(a, (a + d) % TP) for a in range(TP)])

    packed = call(
        pack_kernel,
        "pack",
        sc,
        (whole(gate_w), whole(up_w), whole(down_w)),
        (vmem((3 * DQ, FQ), BF16),) * 3,
    )
    w = [shift(x, d) for d, x in enumerate(packed, 1)]
    gate_f, up_f, down_f = call(
        assemble_kernel,
        "assemble",
        sc,
        (
            (far(gate_w), row_block),
            (far(up_w), row_block),
            (far(down_w), pl.BlockSpec((FQ, DQ), lambda g, p: (0, p[0]))),
            *map(whole, w),
        ),
        (hbm((DQ, F), BF16), hbm((DQ, F), BF16), hbm((F, DQ), BF16)),
    )
    got = got.reshape(SENT, DQ + 128)
    tok_c, cot_c, info_c, part = [None] * TP, [None] * TP, [None] * TP, [None] * TP
    for d in (2, 1, 3, 0):
        tok_c[d], cot_c[d], info_c[d], part[d] = call(
            functools.partial(hidden_kernel, d),
            f"hidden{d}",
            sc,
            (got, whole(far(gate_f)), whole(far(up_f)), whole(far(down_f))),
            (
                hbm((128, DQ), BF16),
                hbm((128, DQ), BF16),
                hbm((128, 128), BF16),
                vmem((128, 3 * F), BF16),
            ),
        )
        if d:
            part[d] = shift(part[d], d)
    main, side = call(
        grads_kernel,
        "grads",
        sc,
        (*part, whole(info_c[0])),
        (vmem((128, 2 * F + 128), BF16), vmem((128, F), BF16)),
    )
    all_main = [main] + [shift(main, TP - d) for d in (1, 2, 3)]
    all_side = [side] + [shift(side, TP - d) for d in (1, 2, 3)]
    (send_back,) = call(
        back_kernel,
        "back",
        sc,
        (*all_main, *map(whole, tok_c), *map(whole, info_c), whole(gate_f), whole(up_f)),
        (hbm((SENT, DQ // 2 + 128), BF16),),
    )
    home = lax.all_to_all(
        send_back.reshape(EXPERTS, 8, DQ // 2 + 128), EP, 0, 0, tiled=True
    ).reshape(SENT, DQ // 2 + 128)
    blocks = call(
        sums_kernel,
        "sums",
        sc,
        tuple(map(whole, (*all_main, *all_side, *tok_c, *cot_c))),
        (hbm((3 * DQ + 32, 128), BF16),) + (vmem((3 * DQ + 32, 128), BF16),) * 3,
    )
    x = [shift(b, d) for d, b in enumerate(blocks[1:], 1)]
    grad_gate, grad_up, grad_down, in_norms, down_norms = call(
        weights_kernel,
        "weights",
        sc,
        (whole(far(blocks[0])), *map(whole, x)),
        (
            sds((D, FQ), BF16),
            sds((D, FQ), BF16),
            sds((FQ, D), BF16),
            sds((2, D), F32),
            sds((1, FQ), F32),
        ),
    )
    (own_rows,) = call(router_kernel, "router", sc, (home,), (vmem((4, EXPERTS), F32),))
    near = lax.all_gather(own_rows, NEAR, axis=0, tiled=True)
    moves = [
        (i * TP + p, (32 * p + i // 4) * TP + i % 4) for i in range(EXPERTS) for p in range(TP)
    ]
    moved = lax.ppermute(near, ALL, moves)
    grad_tokens, grad_gating = call(
        home_kernel,
        "home",
        sc,
        (home, whole(place0), whole(place1), whole(stats), whole(routing_t), (router_weight, row_block)),
        (sds((TOK, DQ), BF16), sds((2, TOK), F32)),
    )
    grad_router, router_norms = call(
        finish_kernel, "finish", sc, (moved,), (sds((16, EXPERTS), F32), sds((1, 16), F32))
    )
    return (
        grad_tokens,
        grad_gating.T,
        grad_router,
        grad_gate[None],
        grad_up[None],
        grad_down[None],
        in_norms[None],
        down_norms,
        router_norms[0],
    )


def solution(mesh):
    split = Mesh(mesh.devices.reshape(8, 4, 2, 2, TP), ("ep_0", "ep_1", "ep_3", "ep_2", "tp"))
    in_specs = (
        P(EP, None),
        P(EP, None),
        P(EP, None),
        P(),
        P(EP, None, "tp"),
        P(EP, None, "tp"),
        P(EP, "tp", None),
    )
    out_specs = (
        P(EP, "tp"),
        P(EP, None),
        P(EP, None),
        P(EP, None, "tp"),
        P(EP, None, "tp"),
        P(EP, "tp", None),
        P(EP, None, None),
        P(EP, "tp"),
        P(EP),
    )
    return jax.shard_map(
        shards, mesh=split, in_specs=in_specs, out_specs=out_specs, check_vma=False
    )
```

```python
import functools

import jax
import jax.numpy as jnp
from jax import lax
from jax.experimental import pallas as pl
from jax.experimental.pallas import tpu as pltpu
from jax.sharding import Mesh
from jax.sharding import PartitionSpec as P


EP = ("ep_0", "ep_1", "ep_2")
F32 = jnp.float32
BF16 = jnp.bfloat16


TOK = 128
D = 2048
EXPERTS = 128
TP = 4
DQ = D // TP
F = 512
FQ = F // TP
SENT = EXPERTS * 8
CH = D // 8


def dot(a, b, ca=1, cb=0):
    return lax.dot_general(a, b, (((ca,), (cb,)), ((), ())), preferred_element_type=F32)


def iota(shape, dim):
    return lax.broadcasted_iota(jnp.int32, shape, dim)


def pieces(x):
    hi = x.astype(BF16).astype(F32)
    rest = x - hi
    mid = rest.astype(BF16).astype(F32)
    return hi, mid, rest - mid


def aligned(x, n):
    return pl.multiple_of(x * n, n)


def spread(u):
    row = iota((SENT, 128), 0)
    return ((row // 8 == iota((SENT, 128), 1)) & (row % 8 == u)).astype(BF16)


def gather(u):
    row = iota((128, SENT), 1)
    return ((row // 8 == iota((128, SENT), 0)) & (row % 8 == u)).astype(BF16)


def every():
    return (iota((SENT, 128), 0) // 8 == iota((SENT, 128), 1)).astype(BF16)


ON_CHIP = pl.BlockSpec(memory_space=pltpu.VMEM)


def call(kernel, scalars, ins, outs, scratch=()):
    arrays = []
    specs = []
    for x in ins:
        if isinstance(x, tuple):
            arrays.append(x[0])
            specs.append(x[1])
        else:
            arrays.append(pltpu.with_memory_space_constraint(x, pltpu.VMEM))
            specs.append(ON_CHIP)
    return pl.pallas_call(
        kernel,
        grid_spec=pltpu.PrefetchScalarGridSpec(
            num_scalar_prefetch=1,
            grid=(1,),
            in_specs=tuple(specs),
            out_specs=(ON_CHIP,) * len(outs),
            scratch_shapes=scratch,
        ),
        out_shape=tuple(outs),
        compiler_params=pltpu.CompilerParams(vmem_limit_bytes=32 << 20),
    )(scalars, *arrays)


def whole(x):
    return (x, pl.BlockSpec(x.shape, lambda g, p: (0,) * x.ndim))


def sds(shape, dtype):
    return jax.ShapeDtypeStruct(shape, dtype)


def hbm(shape, dtype):
    return pltpu.HBM(shape, dtype)


def vmem(shape, dtype):
    return pltpu.VMEM(shape, dtype)


def dispatch_kernel(sc, tok, cot, routing, router, send, hit0, hit1, stats):
    experts = iota((EXPERTS, TOK), 0)
    picked = [(experts == routing[k : k + 1, :]) for k in range(2)]
    both = (picked[0] | picked[1]).astype(F32)
    logits = dot(router[...], tok[...], 0, 1)
    s = [
        jax.nn.sigmoid(jnp.sum(jnp.where(m, logits, 0.0), axis=0, keepdims=True)) for m in picked
    ]
    total = s[0] + s[1]
    g = [v / total for v in s]
    slope = [v * (1.0 - v) / total for v in s]
    before = (iota((TOK, TOK), 0) < iota((TOK, TOK), 1)).astype(BF16)
    within = dot(both.astype(BF16), before)
    mine = within == sc[0].astype(F32)
    line = iota((128, TOK), 0)
    hits = []
    info = None
    for k, out in ((0, hit0), (1, hit1)):
        hit = jnp.where(picked[k] & mine, 1.0, 0.0)
        out[...] = hit.astype(BF16)
        hits.append(hit)
        own = slope[k] * g[1 - k]
        other = slope[1 - k] * g[k]
        columns = [*pieces(g[k]), *pieces(own), *pieces(other), routing[1 - k : 2 - k, :].astype(F32)]
        table = jnp.zeros((128, TOK), F32)
        for c, v in enumerate(columns):
            table = jnp.where(line == c, v, table)
        part = dot(hit.astype(BF16), table.astype(BF16), 1, 1)
        info = part if info is None else info + part
    any_hit = (hits[0] + hits[1]).astype(BF16)
    toks = dot(any_hit, tok[...]).astype(BF16)
    cots = dot(any_hit, cot[...]).astype(BF16)
    rows = None
    for u in range(8):
        at = slice(CH * u, CH * (u + 1))
        part = dot(spread(u), jnp.concatenate([toks[:, at], cots[:, at]], axis=1))
        rows = part if rows is None else rows + part
    send[:, 0 : 2 * CH] = rows.astype(BF16)
    send[:, 2 * CH :] = dot(every(), info.astype(BF16)).astype(BF16)
    stats[...] = jnp.concatenate(
        [s[0], s[1], total, g[0], g[1], total, total, total], axis=0
    )


def pack_kernel(sc, gate, up, down, out):
    out[0:D, :] = gate[...]
    out[D : 2 * D, :] = up[...]
    for c in range(D // 128):
        out[2 * D + 128 * c : 2 * D + 128 * (c + 1), :] = down[:, 128 * c : 128 * (c + 1)]


def rows_kernel(sc, got, tok_r, cot_r, info_r):
    for u in range(8):
        at = slice(CH * u, CH * (u + 1))
        part = dot(gather(u), got[:, 0 : 2 * CH]).astype(BF16)
        tok_r[:, at] = part[:, 0:CH]
        cot_r[:, at] = part[:, CH:]
    info_r[...] = dot(gather(0), got[:, 2 * CH :]).astype(BF16)


def quarter(tok_r, cot_r, info_r, gate, up, down, grads, back, gg_out):
    toks = tok_r[...]
    pre_gate = dot(toks, gate)
    pre_up = dot(toks, up)
    back_raw = dot(cot_r[...], down, 1, 1)
    about = info_r[...].astype(F32)
    gating = about[:, 0:1] + about[:, 1:2] + about[:, 2:3]
    sig = jax.nn.sigmoid(pre_gate)
    activated = pre_gate * sig
    slope = sig * (1.0 + pre_gate * (1.0 - sig))
    hidden = (activated * pre_up).astype(BF16).astype(F32)
    gg_out[...] = jnp.broadcast_to(jnp.sum(hidden * back_raw, axis=1, keepdims=True), (128, 128))
    scaled = gating * back_raw
    g_gate = (scaled * pre_up * slope).astype(BF16)
    g_up = (scaled * activated).astype(BF16)
    grads[:, 0:FQ] = g_gate
    grads[:, FQ : 2 * FQ] = g_up
    grads[:, 2 * FQ :] = (gating * hidden).astype(BF16)
    back[...] = (dot(g_gate, gate, 1, 1) + dot(g_up, up, 1, 1)).astype(BF16)


def beside(x):
    return jnp.concatenate([x[128 * c : 128 * (c + 1), :] for c in range(D // 128)], axis=1)


def own_kernel(sc, tok_r, cot_r, info_r, gate, up, down, *outs):
    quarter(tok_r, cot_r, info_r, gate[...], up[...], down[...], *outs)


def near_kernel(sc, tok_r, cot_r, info_r, w, *outs):
    quarter(tok_r, cot_r, info_r, w[0:D, :], w[D : 2 * D, :], beside(w[2 * D :, :]), *outs)


def far_kernel(sc, tok_r, cot_r, info_r, wa, wb, *outs):
    half = D // 2
    up = jnp.concatenate([wa[D:, :], wb[0:half, :]], axis=0)
    quarter(tok_r, cot_r, info_r, wa[0:D, :], up, beside(wb[half:, :]), *outs)


def emit_kernel(sc, tok_r, info_r, *refs):
    backs, ggs, send = refs[0:4], refs[4:8], refs[8]
    term = backs[0][...].astype(F32)
    gg = ggs[0][...]
    for d in range(1, TP):
        term = term + backs[d][...].astype(F32)
        gg = gg + ggs[d][...]
    term = term.astype(BF16)
    about = info_r[...].astype(F32)
    own = (about[:, 3:4] + about[:, 4:5] + about[:, 5:6]) * gg
    other = (about[:, 6:7] + about[:, 7:8] + about[:, 8:9]) * gg
    other_expert = about[:, 9:10].astype(jnp.int32)
    lane = iota((128, EXPERTS), 1)
    mix = jnp.where(lane == sc[1], own, 0.0) - jnp.where(lane == other_expert, other, 0.0)
    mix_hi = mix.astype(BF16)
    mix_lo = (mix - mix_hi.astype(F32)).astype(BF16)
    router = dot(tok_r[...], jnp.concatenate([mix_hi, mix_lo], axis=1), 0, 0)
    router = (router[:, 0:EXPERTS] + router[:, EXPERTS:]).reshape(128, 2, 8, EXPERTS)
    rows = None
    for u in range(8):
        part = dot(spread(u), term[:, CH * u : CH * (u + 1)])
        rows = part if rows is None else rows + part
    send[:, 0:CH] = rows.astype(BF16)
    for h in range(2):
        send[:, CH + 128 * h : CH + 128 * (h + 1)] = router[:, h].reshape(SENT, EXPERTS).astype(BF16)
    tail = jnp.zeros((128, 128), F32)
    for c, v in enumerate(pieces(gg)):
        tail = jnp.where(lane == c, v, tail)
    send[:, 2 * CH :] = dot(every(), tail.astype(BF16)).astype(BF16)


def share_kernel(sc, tok_r, cot_r, *refs):
    p = sc[0]
    grads, outs = refs[0:4], refs[4:8]
    for d, out in enumerate(outs):
        at = pl.ds(aligned((p + d) % TP, DQ), DQ)
        out[:, 0:DQ] = tok_r[:, at]
        out[:, DQ : 2 * DQ] = cot_r[:, at]
        for r, g in enumerate(grads):
            f = (p + r) % TP
            for c in range(3):
                out[:, pl.ds(aligned(8 + 4 * c + f, FQ), FQ)] = g[:, FQ * c : FQ * (c + 1)]


def row_sums(x):
    n, width = x.shape
    acc = x[:, 0:128]
    for c in range(1, width // 128):
        acc = acc + x[:, 128 * c : 128 * (c + 1)]
    return jnp.concatenate(
        [jnp.sum(acc[128 * c : 128 * (c + 1), :].T, axis=0, keepdims=True) for c in range(n // 128)],
        axis=0,
    )


def sums_kernel(sc, *refs):
    p = sc[0]
    shared, outs = refs[0:4], refs[4:]
    toks = jnp.concatenate([t[:, 0:DQ] for t in shared], axis=0).T
    cots = jnp.concatenate([t[:, DQ : 2 * DQ] for t in shared], axis=0)
    acc_gate = jnp.zeros((DQ, FQ), F32)
    acc_up = jnp.zeros((DQ, FQ), F32)
    for d, out in enumerate(outs):
        f = (p + d) % TP
        at = [pl.ds(aligned(8 + 4 * c + f, FQ), FQ) for c in range(3)]
        gate_sum = dot(toks, jnp.concatenate([g[:, at[0]] for g in shared], axis=0))
        up_sum = dot(toks, jnp.concatenate([g[:, at[1]] for g in shared], axis=0))
        down_sum = dot(jnp.concatenate([g[:, at[2]] for g in shared], axis=0), cots, 0, 0)
        acc_gate = acc_gate + gate_sum * gate_sum
        acc_up = acc_up + up_sum * up_sum
        out[0:DQ, :] = gate_sum.astype(BF16)
        out[DQ : 2 * DQ, :] = up_sum.astype(BF16)
        for c in range(4):
            out[2 * DQ + 128 * c : 2 * DQ + 128 * (c + 1), :] = down_sum[
                :, 128 * c : 128 * (c + 1)
            ].astype(BF16)
        hi, mid, lo = pieces(row_sums(down_sum * down_sum))
        line = iota((8, 128), 0)
        last = jnp.where(line == 0, hi, jnp.where(line == 1, mid, jnp.where(line == 2, lo, 0.0)))
        out[3 * DQ + 24 : 3 * DQ + 32, :] = last.astype(BF16)
    both = jnp.concatenate([row_sums(acc_gate), row_sums(acc_up)], axis=0)
    norms = jnp.concatenate(pieces(both), axis=0).astype(BF16)
    for out in outs:
        out[3 * DQ : 3 * DQ + 24, :] = norms


def home_kernel(sc, got, hit0, hit1, out):
    hits = [hit0[...], hit1[...]]
    both = (hits[0].astype(F32) + hits[1].astype(F32)).astype(BF16)
    terms = jnp.concatenate(
        [dot(gather(u), got[:, 0:CH]).astype(BF16) for u in range(8)], axis=1
    )
    summed = dot(both, terms, 0, 0).astype(BF16)
    tail = dot(gather(0), got[:, 2 * CH :]).astype(BF16)
    pick = (iota((8, SENT), 0) == iota((8, SENT), 1) % 8).astype(BF16)
    router = dot(pick, got[:, CH : 2 * CH])
    hi, mid, lo = pieces(router)
    lines = [jnp.concatenate([hi, mid + lo], axis=1)]
    flat = []
    for hit in hits:
        flat.append(dot(tail, hit, 0, 0)[0:4, :])
    flat = jnp.concatenate(flat, axis=0)
    lines.append(jnp.concatenate([flat] * 4, axis=1))
    extra = jnp.concatenate(lines, axis=0).astype(BF16)
    for q in range(TP):
        out[q, 0:TOK, :] = summed[:, DQ * q : DQ * (q + 1)]
        out[q, TOK:, :] = extra


def last_kernel(sc, got, stats, routing, router, grad_tokens, grad_gating, grad_router, norms):
    total = got[0].astype(F32)
    for q in range(1, TP):
        total = total + got[q].astype(F32)
    extra = total[TOK:, :]
    rows = [
        extra[8 + 4 * k : 9 + 4 * k, 0:128]
        + extra[9 + 4 * k : 10 + 4 * k, 0:128]
        + extra[10 + 4 * k : 11 + 4 * k, 0:128]
        for k in range(2)
    ]
    grad_gating[...] = jnp.concatenate(rows, axis=0)
    st = stats[...]
    score_sum = st[2:3, :]
    weighted = st[3:4, :] * rows[0] + st[4:5, :] * rows[1]
    experts = iota((EXPERTS, TOK), 0)
    logits = jnp.zeros((EXPERTS, TOK), F32)
    for k in range(2):
        s = st[k : k + 1, :]
        chosen = (rows[k] - weighted) / score_sum * s * (1.0 - s)
        logits = jnp.where(experts == routing[k : k + 1, :], chosen, logits)
    term = dot(logits.astype(BF16), router[...], 0, 1)
    grad_tokens[...] = (total[0:TOK, :] + term).astype(BF16)
    sums = extra[0:8, 0:256] + extra[0:8, 256:512]
    x = jnp.concatenate([sums[:, 0:128], sums[:, 128:256]], axis=0)
    grad_router[...] = x
    squares = lax.dot_general(
        jnp.ones((8, EXPERTS), F32),
        x * x,
        (((1,), (1,)), ((), ())),
        precision=lax.Precision.HIGHEST,
        preferred_element_type=F32,
    )
    norms[...] = squares[0:1, :]


def weights_kernel(sc, own, x1, x2, x3, gate, up, down, in_norms, down_norms):
    p = sc[0]
    total = None
    for d, x in enumerate((own, x1, x2, x3)):
        q = (p + TP - d) % TP
        gate[pl.ds(aligned(q, DQ), DQ), :] = x[0:DQ, :]
        up[pl.ds(aligned(q, DQ), DQ), :] = x[DQ : 2 * DQ, :]
        for c in range(4):
            down[:, pl.ds(aligned(q * 4 + c, 128), 128)] = x[
                2 * DQ + 128 * c : 2 * DQ + 128 * (c + 1), :
            ]
        tail = x[3 * DQ : 3 * DQ + 32, :].astype(F32)
        norms = tail[0:8, :] + tail[8:16, :] + tail[16:24, :]
        for c in range(4):
            at = pl.ds(aligned(q * 4 + c, 128), 128)
            in_norms[0:1, at] = norms[c : c + 1, :]
            in_norms[1:2, at] = norms[4 + c : 5 + c, :]
        part = tail[24:25, :] + tail[25:26, :] + tail[26:27, :]
        total = part if total is None else total + part
    down_norms[...] = total


def layer(tokens, cotangent, routing, router_weight, gate_weight, up_weight, down_weight):
    tp_index = lax.axis_index("tp")
    ep_index = lax.axis_index(EP)
    sc = jnp.stack([tp_index, ep_index]).astype(jnp.int32)
    routing_t = routing.T
    gate_w = gate_weight[0]
    up_w = up_weight[0]
    down_w = down_weight[0]
    far = functools.partial(pltpu.with_memory_space_constraint, memory_space=pltpu.HBM)

    def shift(x, d):
        return lax.ppermute(x, "tp", [(a, (a + d) % TP) for a in range(TP)])

    (packed,) = call(
        pack_kernel,
        sc,
        (whole(far(gate_w)), whole(far(up_w)), whole(far(down_w))),
        (hbm((6 * D // 2, FQ), BF16),),
    )
    from_below = shift(packed, 1)
    from_above = shift(packed, 3)
    far_a = shift(from_below[0 : 3 * D // 2], 1)
    far_b = shift(from_above[3 * D // 2 :], 3)

    send, hit0, hit1, stats = call(
        dispatch_kernel,
        sc,
        (whole(far(tokens)), whole(far(cotangent)), whole(far(routing_t)), whole(far(router_weight))),
        (
            hbm((SENT, 2 * CH + 128), BF16),
            hbm((EXPERTS, TOK), BF16),
            hbm((EXPERTS, TOK), BF16),
            hbm((8, TOK), F32),
        ),
    )
    got = lax.all_to_all(send.reshape(EXPERTS, 8, 2 * CH + 128), EP, 0, 0, tiled=True)
    rows = call(
        rows_kernel,
        sc,
        (got.reshape(SENT, 2 * CH + 128),),
        (sds((128, D), BF16), sds((128, D), BF16), sds((128, 128), BF16)),
    )
    results = (sds((128, 3 * FQ), BF16), sds((128, D), BF16), sds((128, 128), F32))
    inputs = tuple(map(whole, rows))
    quarters = [
        call(own_kernel, sc, (*inputs, whole(gate_w), whole(up_w), whole(down_w)), results),
        call(near_kernel, sc, (*inputs, whole(from_above)), results),
        call(far_kernel, sc, (*inputs, whole(far_a), whole(far_b)), results),
        call(near_kernel, sc, (*inputs, whole(from_below)), results),
    ]
    grads, backs, ggs = zip(*quarters)
    (send_back,) = call(
        emit_kernel,
        sc,
        (inputs[0], inputs[2], *map(whole, backs), *map(whole, ggs)),
        (hbm((SENT, 2 * CH + 128), BF16),),
    )
    home = lax.all_to_all(send_back.reshape(EXPERTS, 8, 2 * CH + 128), EP, 0, 0, tiled=True)
    home = home.reshape(SENT, 2 * CH + 128)
    shared = call(
        share_kernel,
        sc,
        (*inputs[0:2], *map(whole, grads)),
        (hbm((128, 2 * DQ + 3 * F), BF16),) * 4,
    )
    shared = [shared[0]] + [shift(t, d) for d, t in enumerate(shared[1:], 1)]
    blocks = call(sums_kernel, sc, tuple(map(whole, shared)), (hbm((3 * DQ + 32, 128), BF16),) * 4)
    x = [shift(b, d) for d, b in enumerate(blocks[1:], 1)]
    grad_gate, grad_up, grad_down, in_norms, down_norms = call(
        weights_kernel,
        sc,
        (whole(far(blocks[0])), *map(whole, x)),
        (
            sds((D, FQ), BF16),
            sds((D, FQ), BF16),
            sds((FQ, D), BF16),
            sds((2, D), F32),
            sds((1, FQ), F32),
        ),
    )
    (parts,) = call(
        home_kernel, sc, (home, whole(hit0), whole(hit1)), (vmem((TP, TOK + 16, DQ), BF16),)
    )
    parts = lax.all_to_all(parts, "tp", 0, 0, tiled=True)
    grad_tokens, grad_gating, grad_router, router_norms = call(
        last_kernel,
        sc,
        (
            parts,
            whole(stats),
            whole(routing_t),
            (router_weight, pl.BlockSpec((DQ, 128), lambda g, p: (p[0], 0))),
        ),
        (sds((TOK, DQ), BF16), sds((2, TOK), F32), sds((16, EXPERTS), F32), sds((1, 16), F32)),
    )
    return (
        grad_tokens,
        grad_gating.T,
        grad_router,
        grad_gate[None],
        grad_up[None],
        grad_down[None],
        in_norms[None],
        down_norms,
        router_norms[0],
    )


def solution(mesh):
    split = Mesh(mesh.devices.reshape(8, 8, 2, TP), ("ep_0", "ep_1", "ep_2", "tp"))
    in_specs = (
        P(EP, None),
        P(EP, None),
        P(EP, None),
        P(),
        P(EP, None, "tp"),
        P(EP, None, "tp"),
        P(EP, "tp", None),
    )
    out_specs = (
        P(EP, "tp"),
        P(EP, None),
        P(EP, None),
        P(EP, None, "tp"),
        P(EP, None, "tp"),
        P(EP, "tp", None),
        P(EP, None, None),
        P(EP, "tp"),
        P(EP),
    )
    return jax.shard_map(layer, mesh=split, in_specs=in_specs, out_specs=out_specs, check_vma=False)
```

```python
import functools

import jax
import jax.numpy as jnp
from jax import lax
from jax.experimental import pallas as pl
from jax.experimental.pallas import tpu as pltpu
from jax.sharding import Mesh
from jax.sharding import PartitionSpec as P


EP = ("ep_0", "ep_1", "ep_2")
F32 = jnp.float32
BF16 = jnp.bfloat16


TOK = 128
D = 2048
EXPERTS = 128
TP = 4
DQ = D // TP
F = 512
FQ = F // TP
SENT = EXPERTS * 8
CH = D // 8


def dot(a, b, ca=1, cb=0):
    return lax.dot_general(a, b, (((ca,), (cb,)), ((), ())), preferred_element_type=F32)


def iota(shape, dim):
    return lax.broadcasted_iota(jnp.int32, shape, dim)


def pieces(x):
    hi = x.astype(BF16).astype(F32)
    rest = x - hi
    mid = rest.astype(BF16).astype(F32)
    return hi, mid, rest - mid


def spread(chunks):
    row = iota((SENT, SENT), 0)
    col = iota((SENT, SENT), 1)
    place = ((row // 8 == col % 128) & (row % 8 == col // 128)).astype(BF16)
    return dot(place, jnp.concatenate(chunks, axis=0)).astype(BF16)


def gather(u):
    row = iota((128, SENT), 1)
    return ((row // 8 == iota((128, SENT), 0)) & (row % 8 == u)).astype(BF16)


def every():
    return (iota((SENT, 128), 0) // 8 == iota((SENT, 128), 1)).astype(BF16)


ON_CHIP = pl.BlockSpec(memory_space=pltpu.VMEM)


def call(kernel, scalars, ins, outs, scratch=()):
    arrays = []
    specs = []
    for x in ins:
        if isinstance(x, tuple):
            arrays.append(x[0])
            specs.append(x[1])
        else:
            arrays.append(pltpu.with_memory_space_constraint(x, pltpu.VMEM))
            specs.append(ON_CHIP)
    return pl.pallas_call(
        kernel,
        grid_spec=pltpu.PrefetchScalarGridSpec(
            num_scalar_prefetch=1,
            grid=(1,),
            in_specs=tuple(specs),
            out_specs=(ON_CHIP,) * len(outs),
            scratch_shapes=scratch,
        ),
        out_shape=tuple(outs),
        compiler_params=pltpu.CompilerParams(vmem_limit_bytes=32 << 20),
    )(scalars, *arrays)


def whole(x):
    return (x, pl.BlockSpec(x.shape, lambda g, p: (0,) * x.ndim))


def sds(shape, dtype):
    return jax.ShapeDtypeStruct(shape, dtype)


def hbm(shape, dtype):
    return pltpu.HBM(shape, dtype)


def vmem(shape, dtype):
    return pltpu.VMEM(shape, dtype)


def dispatch_kernel(sc, tok, cot, routing, router, send, hit0, hit1, stats):
    experts = iota((EXPERTS, TOK), 0)
    picked = [(experts == routing[k : k + 1, :]) for k in range(2)]
    both = (picked[0] | picked[1]).astype(F32)
    logits = dot(router[...], tok[...], 0, 1)
    s = [
        jax.nn.sigmoid(jnp.sum(jnp.where(m, logits, 0.0), axis=0, keepdims=True)) for m in picked
    ]
    total = s[0] + s[1]
    g = [v / total for v in s]
    slope = [v * (1.0 - v) / total for v in s]
    before = (iota((TOK, TOK), 0) < iota((TOK, TOK), 1)).astype(BF16)
    within = dot(both.astype(BF16), before)
    mine = within == sc[0].astype(F32)
    line = iota((128, TOK), 0)
    hits = []
    info = None
    for k, out in ((0, hit0), (1, hit1)):
        hit = jnp.where(picked[k] & mine, 1.0, 0.0)
        out[...] = hit.astype(BF16)
        hits.append(hit)
        own = slope[k] * g[1 - k]
        other = slope[1 - k] * g[k]
        columns = [*pieces(g[k]), *pieces(own), *pieces(other), routing[1 - k : 2 - k, :].astype(F32)]
        table = jnp.zeros((128, TOK), F32)
        for c, v in enumerate(columns):
            table = jnp.where(line == c, v, table)
        part = dot(hit.astype(BF16), table.astype(BF16), 1, 1)
        info = part if info is None else info + part
    any_hit = (hits[0] + hits[1]).astype(BF16)
    toks = dot(any_hit, tok[...]).astype(BF16)
    cots = dot(any_hit, cot[...]).astype(BF16)
    send[:, 0 : 2 * CH] = spread(
        [
            jnp.concatenate([x[:, CH * u : CH * (u + 1)] for x in (toks, cots)], axis=1)
            for u in range(8)
        ]
    )
    send[:, 2 * CH :] = dot(every(), info.astype(BF16)).astype(BF16)
    stats[...] = jnp.concatenate(
        [s[0], s[1], total, g[0], g[1], total, total, total], axis=0
    )


def pack_kernel(sc, gate, up, down, out):
    out[:, 0:FQ] = gate[...]
    out[:, FQ : 2 * FQ] = up[...]
    out[:, 2 * FQ :] = down[...].T


def rows_kernel(sc, got, pair, info):
    for u in range(8):
        part = dot(gather(u), got[:, 0 : 2 * CH]).astype(BF16)
        pair[:, CH * u : CH * (u + 1)] = part[:, 0:CH]
        pair[:, D + CH * u : D + CH * (u + 1)] = part[:, CH:]
    info[...] = dot(gather(0), got[:, 2 * CH :]).astype(BF16)


def quarter(pair, about, parts, grads):
    pre = None
    back_raw = None
    at = 0
    for w in parts:
        n = w.shape[0]
        x = dot(pair[:, at : at + n], w[:, 0 : 2 * FQ])
        y = dot(pair[:, D + at : D + at + n], w[:, 2 * FQ :])
        pre = x if pre is None else pre + x
        back_raw = y if back_raw is None else back_raw + y
        at += n
    pre_gate = pre[:, 0:FQ]
    pre_up = pre[:, FQ:]
    gating = about[:, 0:1] + about[:, 1:2] + about[:, 2:3]
    sig = jax.nn.sigmoid(pre_gate)
    activated = pre_gate * sig
    slope = sig * (1.0 + pre_gate * (1.0 - sig))
    hidden = (activated * pre_up).astype(BF16).astype(F32)
    gg = jnp.sum(hidden * back_raw, axis=1, keepdims=True)
    scaled = gating * back_raw
    g_in = jnp.concatenate([scaled * pre_up * slope, scaled * activated], axis=1).astype(BF16)
    grads[:, 0 : 2 * FQ] = g_in
    grads[:, 2 * FQ :] = (gating * hidden).astype(BF16)
    backs = [dot(g_in, w[:, 0 : 2 * FQ], 1, 1) for w in parts]
    return gg, backs


def three_kernel(sc, pair, info, own, above, below, grads0, grads1, grads3, back, gg_out):
    about = info[...].astype(F32)
    gg = None
    for w, grads in ((own, grads0), (above, grads1), (below, grads3)):
        part, backs = quarter(pair, about, (w,), grads)
        if gg is None:
            gg = part
            back[...] = backs[0]
        else:
            gg = gg + part
            back[...] += backs[0]
    gg_out[...] = jnp.broadcast_to(gg, (128, 128))


def emit_kernel(sc, pair, info, wa, wb, back, gg_in, grads, send):
    about = info[...].astype(F32)
    gg, backs = quarter(pair, about, (wa, wb), grads)
    gg = gg + gg_in[:, 0:1]
    term = (back[...] + jnp.concatenate(backs, axis=1)).astype(BF16)
    own = (about[:, 3:4] + about[:, 4:5] + about[:, 5:6]) * gg
    other = (about[:, 6:7] + about[:, 7:8] + about[:, 8:9]) * gg
    other_expert = about[:, 9:10].astype(jnp.int32)
    lane = iota((128, EXPERTS), 1)
    mix = jnp.where(lane == sc[1], own, 0.0) - jnp.where(lane == other_expert, other, 0.0)
    mix_hi = mix.astype(BF16)
    mix_lo = (mix - mix_hi.astype(F32)).astype(BF16)
    router = dot(pair[:, 0:D], jnp.concatenate([mix_hi, mix_lo], axis=1), 0, 0)
    router = (router[:, 0:EXPERTS] + router[:, EXPERTS:]).reshape(128, 2, 8, EXPERTS)
    send[:, 0:CH] = spread([term[:, CH * u : CH * (u + 1)] for u in range(8)])
    for h in range(2):
        send[:, CH + 128 * h : CH + 128 * (h + 1)] = router[:, h].reshape(SENT, EXPERTS).astype(BF16)
    tail = jnp.zeros((128, 128), F32)
    for c, v in enumerate(pieces(gg)):
        tail = jnp.where(lane == c, v, tail)
    send[:, 2 * CH :] = dot(every(), tail.astype(BF16)).astype(BF16)


def row_sums(x):
    n, width = x.shape
    acc = x[:, 0:128]
    for c in range(1, width // 128):
        acc = acc + x[:, 128 * c : 128 * (c + 1)]
    return jnp.concatenate(
        [jnp.sum(acc[128 * c : 128 * (c + 1), :].T, axis=0, keepdims=True) for c in range(n // 128)],
        axis=0,
    )


def sums_kernel(sc, *refs):
    pairs, grads = refs[0:4], refs[4:8]
    gate, up, down, down_norms, norms = refs[8:]
    toks = jnp.concatenate([x[:, 0:D] for x in pairs], axis=0)
    cots = jnp.concatenate([x[:, D:] for x in pairs], axis=0)
    g_in = jnp.concatenate([g[:, 0 : 2 * FQ] for g in grads], axis=0)
    scaled = jnp.concatenate([g[:, 2 * FQ :] for g in grads], axis=0)
    in_sums = dot(toks, g_in, 0, 0)
    gate[...] = in_sums[:, 0:FQ].astype(BF16)
    up[...] = in_sums[:, FQ:].astype(BF16)
    squares = in_sums * in_sums
    lines = []
    for x in (squares[:, 0:FQ], squares[:, FQ:]):
        hi, mid, lo = pieces(row_sums(x))
        lines += [hi, mid + lo]
    norms[...] = jnp.concatenate(lines, axis=1).astype(BF16)
    down_sum = dot(scaled, cots, 0, 0)
    down[...] = down_sum.astype(BF16)
    down_norms[...] = row_sums(down_sum * down_sum)


def home_kernel(sc, got, hit0, hit1, norms, out):
    hits = [hit0[...], hit1[...]]
    both = (hits[0].astype(F32) + hits[1].astype(F32)).astype(BF16)
    terms = jnp.concatenate(
        [dot(gather(u), got[:, 0:CH]).astype(BF16) for u in range(8)], axis=1
    )
    summed = dot(both, terms, 0, 0).astype(BF16)
    tail = dot(gather(0), got[:, 2 * CH :]).astype(BF16)
    pick = (iota((8, SENT), 0) == iota((8, SENT), 1) % 8).astype(BF16)
    router = dot(pick, got[:, CH : 2 * CH])
    hi, mid, lo = pieces(router)
    lines = [jnp.concatenate([hi, mid + lo], axis=1)]
    flat = []
    for hit in hits:
        flat.append(dot(tail, hit, 0, 0)[0:4, :])
    flat = jnp.concatenate(flat, axis=0)
    lines.append(jnp.concatenate([flat] * 4, axis=1))
    extra = jnp.concatenate(lines, axis=0).astype(BF16)
    for q in range(TP):
        out[q, 0:TOK, :] = summed[:, DQ * q : DQ * (q + 1)]
        out[q, TOK : TOK + 16, :] = extra
        out[q, TOK + 16 :, :] = norms[...]


def last_kernel(
    sc, got, stats, routing, router, grad_tokens, grad_gating, grad_router, norms, in_norms
):
    total = got[0].astype(F32)
    for q in range(1, TP):
        total = total + got[q].astype(F32)
    extra = total[TOK:, :]
    rows = [
        extra[8 + 4 * k : 9 + 4 * k, 0:128]
        + extra[9 + 4 * k : 10 + 4 * k, 0:128]
        + extra[10 + 4 * k : 11 + 4 * k, 0:128]
        for k in range(2)
    ]
    grad_gating[...] = jnp.concatenate(rows, axis=0)
    st = stats[...]
    score_sum = st[2:3, :]
    weighted = st[3:4, :] * rows[0] + st[4:5, :] * rows[1]
    experts = iota((EXPERTS, TOK), 0)
    logits = jnp.zeros((EXPERTS, TOK), F32)
    for k in range(2):
        s = st[k : k + 1, :]
        chosen = (rows[k] - weighted) / score_sum * s * (1.0 - s)
        logits = jnp.where(experts == routing[k : k + 1, :], chosen, logits)
    term = dot(logits.astype(BF16), router[...], 0, 1)
    grad_tokens[...] = (total[0:TOK, :] + term).astype(BF16)
    sums = extra[0:8, 0:256] + extra[0:8, 256:512]
    x = jnp.concatenate([sums[:, 0:128], sums[:, 128:256]], axis=0)
    grad_router[...] = x
    squares = lax.dot_general(
        jnp.ones((8, EXPERTS), F32),
        x * x,
        (((1,), (1,)), ((), ())),
        precision=lax.Precision.HIGHEST,
        preferred_element_type=F32,
    )
    norms[...] = squares[0:1, :]
    for k in range(2):
        sums = extra[16:32, 256 * k : 256 * k + 128] + extra[16:32, 256 * k + 128 : 256 * (k + 1)]
        for c in range(D // 128):
            in_norms[k : k + 1, 128 * c : 128 * (c + 1)] = sums[c : c + 1, :]


def layer(tokens, cotangent, routing, router_weight, gate_weight, up_weight, down_weight):
    tp_index = lax.axis_index("tp")
    ep_index = lax.axis_index(EP)
    sc = jnp.stack([tp_index, ep_index]).astype(jnp.int32)
    routing_t = routing.T
    gate_w = gate_weight[0]
    up_w = up_weight[0]
    down_w = down_weight[0]
    far = functools.partial(pltpu.with_memory_space_constraint, memory_space=pltpu.HBM)

    def shift(x, d):
        return lax.ppermute(x, "tp", [(a, (a + d) % TP) for a in range(TP)])

    (packed,) = call(
        pack_kernel,
        sc,
        (whole(far(gate_w)), whole(far(up_w)), whole(far(down_w))),
        (hbm((D, 3 * FQ), BF16),),
    )
    from_below = shift(packed, 1)
    from_above = shift(packed, 3)
    far_a = shift(from_below[0 : D // 2], 1)
    far_b = shift(from_above[D // 2 :], 3)

    send, hit0, hit1, stats = call(
        dispatch_kernel,
        sc,
        (whole(far(tokens)), whole(far(cotangent)), whole(far(routing_t)), whole(far(router_weight))),
        (
            hbm((SENT, 2 * CH + 128), BF16),
            hbm((EXPERTS, TOK), BF16),
            hbm((EXPERTS, TOK), BF16),
            hbm((8, TOK), F32),
        ),
    )
    got = lax.all_to_all(send.reshape(EXPERTS, 8, 2 * CH + 128), EP, 0, 0, tiled=True)
    pair, info = call(
        rows_kernel,
        sc,
        (got.reshape(SENT, 2 * CH + 128),),
        (hbm((128, 2 * D), BF16), hbm((128, 128), BF16)),
    )
    pairs = [pair]
    for d in (1, 2, 3):
        pairs.append(shift(pair, d))
    quarter_grads = hbm((128, 3 * FQ), BF16)
    grads = [None] * TP
    grads[0], grads[1], grads[3], back, gg = call(
        three_kernel,
        sc,
        tuple(whole(far(x)) for x in (pair, info, packed, from_above, from_below)),
        (quarter_grads,) * 3 + (vmem((128, D), F32), vmem((128, 128), F32)),
    )
    grads[2], send_back = call(
        emit_kernel,
        sc,
        (*(whole(far(x)) for x in (pair, info, far_a, far_b)), back, gg),
        (quarter_grads, hbm((SENT, 2 * CH + 128), BF16)),
    )
    home = lax.all_to_all(send_back.reshape(EXPERTS, 8, 2 * CH + 128), EP, 0, 0, tiled=True)
    home = home.reshape(SENT, 2 * CH + 128)
    grads = [grads[0]] + [shift(grads[d], d) for d in (1, 2, 3)]
    grad_gate, grad_up, grad_down, down_norms, norms = call(
        sums_kernel,
        sc,
        tuple(whole(far(x)) for x in (*pairs, *grads)),
        (
            sds((D, FQ), BF16),
            sds((D, FQ), BF16),
            sds((FQ, D), BF16),
            sds((1, FQ), F32),
            hbm((16, 4 * 128), BF16),
        ),
    )
    (parts,) = call(
        home_kernel,
        sc,
        (home, whole(hit0), whole(hit1), whole(norms)),
        (vmem((TP, TOK + 32, DQ), BF16),),
    )
    parts = lax.all_to_all(parts, "tp", 0, 0, tiled=True)
    grad_tokens, grad_gating, grad_router, router_norms, in_norms = call(
        last_kernel,
        sc,
        (
            parts,
            whole(stats),
            whole(routing_t),
            (router_weight, pl.BlockSpec((DQ, 128), lambda g, p: (p[0], 0))),
        ),
        (
            sds((TOK, DQ), BF16),
            sds((2, TOK), F32),
            sds((16, EXPERTS), F32),
            sds((1, 16), F32),
            sds((2, D), F32),
        ),
    )
    return (
        grad_tokens,
        grad_gating.T,
        grad_router,
        grad_gate[None],
        grad_up[None],
        grad_down[None],
        in_norms[None],
        down_norms,
        router_norms[0],
    )


def solution(mesh):
    split = Mesh(mesh.devices.reshape(8, 8, 2, TP), ("ep_0", "ep_1", "ep_2", "tp"))
    in_specs = (
        P(EP, None),
        P(EP, None),
        P(EP, None),
        P(),
        P(EP, None, "tp"),
        P(EP, None, "tp"),
        P(EP, "tp", None),
    )
    out_specs = (
        P(EP, "tp"),
        P(EP, None),
        P(EP, None),
        P(EP, None, "tp"),
        P(EP, None, "tp"),
        P(EP, "tp", None),
        P(EP, None, None),
        P(EP, "tp"),
        P(EP),
    )
    return jax.shard_map(layer, mesh=split, in_specs=in_specs, out_specs=out_specs, check_vma=False)
```

```python
import functools

import jax
import jax.numpy as jnp
from jax import lax
from jax.experimental import pallas as pl
from jax.experimental.pallas import tpu as pltpu
from jax.sharding import Mesh
from jax.sharding import PartitionSpec as P


EP = ("ep_0", "ep_1", "ep_2")
F32 = jnp.float32
BF16 = jnp.bfloat16


TOK = 128
D = 2048
EXPERTS = 128
TP = 4
DQ = D // TP
F = 512
FQ = F // TP
SENT = EXPERTS * 8
CH = D // 8


def dot(a, b, ca=1, cb=0):
    return lax.dot_general(a, b, (((ca,), (cb,)), ((), ())), preferred_element_type=F32)


def iota(shape, dim):
    return lax.broadcasted_iota(jnp.int32, shape, dim)


def pieces(x):
    hi = x.astype(BF16).astype(F32)
    rest = x - hi
    mid = rest.astype(BF16).astype(F32)
    return hi, mid, rest - mid


def spread(scratch, chunks):
    width = scratch.shape[0]
    for u, chunk in enumerate(chunks):
        for c in range(width):
            scratch[c, pl.ds(u, 128, stride=8), :] = chunk[:, 128 * c : 128 * (c + 1)].astype(F32)
    return jnp.concatenate([scratch[c].astype(BF16) for c in range(width)], axis=1)


def fill(scratch, got):
    for c in range(scratch.shape[0]):
        scratch[c] = got[:, 128 * c : 128 * (c + 1)].astype(F32)


def gather(scratch, u):
    return jnp.concatenate(
        [scratch[c, pl.ds(u, 128, stride=8), :].astype(BF16) for c in range(scratch.shape[0])], axis=1
    )


def every():
    return (iota((SENT, 128), 0) // 8 == iota((SENT, 128), 1)).astype(BF16)


ON_CHIP = pl.BlockSpec(memory_space=pltpu.VMEM)


def call(kernel, scalars, ins, outs, scratch=()):
    arrays = []
    specs = []
    for x in ins:
        if isinstance(x, tuple):
            arrays.append(x[0])
            specs.append(x[1])
        else:
            arrays.append(pltpu.with_memory_space_constraint(x, pltpu.VMEM))
            specs.append(ON_CHIP)
    return pl.pallas_call(
        kernel,
        grid_spec=pltpu.PrefetchScalarGridSpec(
            num_scalar_prefetch=1,
            grid=(1,),
            in_specs=tuple(specs),
            out_specs=(ON_CHIP,) * len(outs),
            scratch_shapes=scratch,
        ),
        out_shape=tuple(outs),
        compiler_params=pltpu.CompilerParams(vmem_limit_bytes=32 << 20),
    )(scalars, *arrays)


def whole(x):
    return (x, pl.BlockSpec(x.shape, lambda g, p: (0,) * x.ndim))


def sds(shape, dtype):
    return jax.ShapeDtypeStruct(shape, dtype)


def hbm(shape, dtype):
    return pltpu.HBM(shape, dtype)


def vmem(shape, dtype):
    return pltpu.VMEM(shape, dtype)


def dispatch_kernel(sc, tok, cot, routing, router, send, hit0, hit1, stats, scratch):
    experts = iota((EXPERTS, TOK), 0)
    picked = [(experts == routing[k : k + 1, :]) for k in range(2)]
    both = (picked[0] | picked[1]).astype(F32)
    logits = dot(router[...], tok[...], 0, 1)
    s = [
        jax.nn.sigmoid(jnp.sum(jnp.where(m, logits, 0.0), axis=0, keepdims=True)) for m in picked
    ]
    total = s[0] + s[1]
    g = [v / total for v in s]
    slope = [v * (1.0 - v) / total for v in s]
    before = (iota((TOK, TOK), 0) < iota((TOK, TOK), 1)).astype(BF16)
    within = dot(both.astype(BF16), before)
    mine = within == sc[0].astype(F32)
    line = iota((128, TOK), 0)
    hits = []
    info = None
    for k, out in ((0, hit0), (1, hit1)):
        hit = jnp.where(picked[k] & mine, 1.0, 0.0)
        out[...] = hit.astype(BF16)
        hits.append(hit)
        own = slope[k] * g[1 - k]
        other = slope[1 - k] * g[k]
        columns = [*pieces(g[k]), *pieces(own), *pieces(other), routing[1 - k : 2 - k, :].astype(F32)]
        table = jnp.zeros((128, TOK), F32)
        for c, v in enumerate(columns):
            table = jnp.where(line == c, v, table)
        part = dot(hit.astype(BF16), table.astype(BF16), 1, 1)
        info = part if info is None else info + part
    any_hit = (hits[0] + hits[1]).astype(BF16)
    toks = dot(any_hit, tok[...])
    cots = dot(any_hit, cot[...])
    send[:, 0 : 2 * CH] = spread(
        scratch,
        [
            jnp.concatenate([x[:, CH * u : CH * (u + 1)] for x in (toks, cots)], axis=1)
            for u in range(8)
        ],
    )
    send[:, 2 * CH :] = dot(every(), info.astype(BF16)).astype(BF16)
    stats[...] = jnp.concatenate(
        [s[0], s[1], total, g[0], g[1], total, total, total], axis=0
    )


def pack_kernel(sc, gate, up, down, out):
    out[:, 0:FQ] = gate[...]
    out[:, FQ : 2 * FQ] = up[...]
    out[:, 2 * FQ :] = down[...].T


def rows_kernel(sc, got, pair, info, scratch):
    fill(scratch, got)
    for u in range(8):
        part = gather(scratch, u)
        pair[:, CH * u : CH * (u + 1)] = part[:, 0:CH]
        pair[:, D + CH * u : D + CH * (u + 1)] = part[:, CH : 2 * CH]
        if u == 0:
            info[...] = part[:, 2 * CH :]


def quarter(pair, about, parts, grads):
    pre = None
    back_raw = None
    at = 0
    for w in parts:
        n = w.shape[0]
        x = dot(pair[:, at : at + n], w[:, 0 : 2 * FQ])
        y = dot(pair[:, D + at : D + at + n], w[:, 2 * FQ :])
        pre = x if pre is None else pre + x
        back_raw = y if back_raw is None else back_raw + y
        at += n
    pre_gate = pre[:, 0:FQ]
    pre_up = pre[:, FQ:]
    gating = about[:, 0:1] + about[:, 1:2] + about[:, 2:3]
    sig = jax.nn.sigmoid(pre_gate)
    activated = pre_gate * sig
    slope = sig * (1.0 + pre_gate * (1.0 - sig))
    hidden = (activated * pre_up).astype(BF16).astype(F32)
    gg = jnp.sum(hidden * back_raw, axis=1, keepdims=True)
    scaled = gating * back_raw
    g_in = jnp.concatenate([scaled * pre_up * slope, scaled * activated], axis=1).astype(BF16)
    grads[:, 0 : 2 * FQ] = g_in
    grads[:, 2 * FQ :] = (gating * hidden).astype(BF16)
    backs = [dot(g_in, w[:, 0 : 2 * FQ], 1, 1) for w in parts]
    return gg, backs


def three_kernel(sc, pair, info, own, above, below, grads0, grads1, grads3, back, gg_out, held, sems):
    copies = [
        pltpu.make_async_copy(w, held.at[k], sems.at[k]) for k, w in enumerate((own, above, below))
    ]
    for c in copies:
        c.start()
    about = info[...].astype(F32)
    gg = None
    for k, grads in enumerate((grads0, grads1, grads3)):
        copies[k].wait()
        part, backs = quarter(pair, about, (held.at[k],), grads)
        if gg is None:
            gg = part
            back[...] = backs[0]
        else:
            gg = gg + part
            back[...] += backs[0]
    gg_out[...] = jnp.broadcast_to(gg, (128, 128))


def emit_kernel(sc, pair, info, wa, wb, back, gg_in, grads, send, scratch):
    about = info[...].astype(F32)
    gg, backs = quarter(pair, about, (wa, wb), grads)
    gg = gg + gg_in[:, 0:1]
    term = back[...] + jnp.concatenate(backs, axis=1)
    own = (about[:, 3:4] + about[:, 4:5] + about[:, 5:6]) * gg
    other = (about[:, 6:7] + about[:, 7:8] + about[:, 8:9]) * gg
    other_expert = about[:, 9:10].astype(jnp.int32)
    lane = iota((128, EXPERTS), 1)
    mix = jnp.where(lane == sc[1], own, 0.0) - jnp.where(lane == other_expert, other, 0.0)
    mix_hi = mix.astype(BF16)
    mix_lo = (mix - mix_hi.astype(F32)).astype(BF16)
    router = dot(pair[:, 0:D], jnp.concatenate([mix_hi, mix_lo], axis=1), 0, 0)
    router = (router[:, 0:EXPERTS] + router[:, EXPERTS:]).reshape(128, 2, 8, EXPERTS)
    send[:, 0:CH] = spread(scratch, [term[:, CH * u : CH * (u + 1)] for u in range(8)])
    for h in range(2):
        send[:, CH + 128 * h : CH + 128 * (h + 1)] = router[:, h].reshape(SENT, EXPERTS).astype(BF16)
    tail = jnp.zeros((128, 128), F32)
    for c, v in enumerate(pieces(gg)):
        tail = jnp.where(lane == c, v, tail)
    send[:, 2 * CH :] = dot(every(), tail.astype(BF16)).astype(BF16)


def row_sums(x):
    n, width = x.shape
    acc = x[:, 0:128]
    for c in range(1, width // 128):
        acc = acc + x[:, 128 * c : 128 * (c + 1)]
    return jnp.concatenate(
        [jnp.sum(acc[128 * c : 128 * (c + 1), :].T, axis=0, keepdims=True) for c in range(n // 128)],
        axis=0,
    )


def sums_kernel(sc, *refs):
    pairs, grads = refs[0:5], refs[5:9]
    gate, up, down, down_norms, norms = refs[9:]
    toks = jnp.concatenate([x[:, 0:D] for x in pairs], axis=0)
    cots = jnp.concatenate([x[:, D:] for x in pairs], axis=0)
    g_in = jnp.concatenate([g[:, 0 : 2 * FQ] for g in grads], axis=0)
    scaled = jnp.concatenate([g[:, 2 * FQ :] for g in grads], axis=0)
    in_sums = dot(toks, g_in, 0, 0)
    gate[...] = in_sums[:, 0:FQ].astype(BF16)
    up[...] = in_sums[:, FQ:].astype(BF16)
    squares = in_sums * in_sums
    lines = []
    for x in (squares[:, 0:FQ], squares[:, FQ:]):
        hi, mid, lo = pieces(row_sums(x))
        lines += [hi, mid + lo]
    norms[...] = jnp.concatenate(lines, axis=1).astype(BF16)
    down_sum = dot(scaled, cots, 0, 0)
    down[...] = down_sum.astype(BF16)
    down_norms[...] = row_sums(down_sum * down_sum)


def home_kernel(sc, got, hit0, hit1, norms, out, scratch):
    fill(scratch, got)
    hits = [hit0[...], hit1[...]]
    both = (hits[0].astype(F32) + hits[1].astype(F32)).astype(BF16)
    lines = [gather(scratch, u) for u in range(8)]
    terms = jnp.concatenate([x[:, 0:CH] for x in lines], axis=1)
    summed = dot(both, terms, 0, 0).astype(BF16)
    tail = lines[0][:, 2 * CH :]
    pick = (iota((8, SENT), 0) == iota((8, SENT), 1) % 8).astype(BF16)
    router = dot(pick, got[:, CH : 2 * CH])
    hi, mid, lo = pieces(router)
    lines = [jnp.concatenate([hi, mid + lo], axis=1)]
    flat = []
    for hit in hits:
        flat.append(dot(tail, hit, 0, 0)[0:4, :])
    flat = jnp.concatenate(flat, axis=0)
    lines.append(jnp.concatenate([flat] * 4, axis=1))
    extra = jnp.concatenate(lines, axis=0).astype(BF16)
    for q in range(TP):
        out[q, 0:TOK, :] = summed[:, DQ * q : DQ * (q + 1)]
        out[q, TOK : TOK + 16, :] = extra
        out[q, TOK + 16 :, :] = norms[...]


def last_kernel(
    sc, got, stats, routing, router, grad_tokens, grad_gating, grad_router, norms, in_norms
):
    total = got[0].astype(F32)
    for q in range(1, TP):
        total = total + got[q].astype(F32)
    extra = total[TOK:, :]
    rows = [
        extra[8 + 4 * k : 9 + 4 * k, 0:128]
        + extra[9 + 4 * k : 10 + 4 * k, 0:128]
        + extra[10 + 4 * k : 11 + 4 * k, 0:128]
        for k in range(2)
    ]
    grad_gating[...] = jnp.concatenate(rows, axis=0)
    st = stats[...]
    score_sum = st[2:3, :]
    weighted = st[3:4, :] * rows[0] + st[4:5, :] * rows[1]
    experts = iota((EXPERTS, TOK), 0)
    logits = jnp.zeros((EXPERTS, TOK), F32)
    for k in range(2):
        s = st[k : k + 1, :]
        chosen = (rows[k] - weighted) / score_sum * s * (1.0 - s)
        logits = jnp.where(experts == routing[k : k + 1, :], chosen, logits)
    term = dot(logits.astype(BF16), router[...], 0, 1)
    grad_tokens[...] = (total[0:TOK, :] + term).astype(BF16)
    sums = extra[0:8, 0:256] + extra[0:8, 256:512]
    x = jnp.concatenate([sums[:, 0:128], sums[:, 128:256]], axis=0)
    grad_router[...] = x
    squares = lax.dot_general(
        jnp.ones((8, EXPERTS), F32),
        x * x,
        (((1,), (1,)), ((), ())),
        precision=lax.Precision.HIGHEST,
        preferred_element_type=F32,
    )
    norms[...] = squares[0:1, :]
    for k in range(2):
        sums = extra[16:32, 256 * k : 256 * k + 128] + extra[16:32, 256 * k + 128 : 256 * (k + 1)]
        for c in range(D // 128):
            in_norms[k : k + 1, 128 * c : 128 * (c + 1)] = sums[c : c + 1, :]


def layer(tokens, cotangent, routing, router_weight, gate_weight, up_weight, down_weight):
    tp_index = lax.axis_index("tp")
    ep_index = lax.axis_index(EP)
    sc = jnp.stack([tp_index, ep_index]).astype(jnp.int32)
    routing_t = routing.T
    gate_w = gate_weight[0]
    up_w = up_weight[0]
    down_w = down_weight[0]
    far = functools.partial(pltpu.with_memory_space_constraint, memory_space=pltpu.HBM)

    def shift(x, d):
        return lax.ppermute(x, "tp", [(a, (a + d) % TP) for a in range(TP)])

    (packed,) = call(
        pack_kernel,
        sc,
        (whole(far(gate_w)), whole(far(up_w)), whole(far(down_w))),
        (hbm((D, 3 * FQ), BF16),),
    )
    from_below = shift(packed, 1)
    from_above = shift(packed, 3)
    far_a = shift(from_below[0 : D // 2], 1)
    far_b = shift(from_above[D // 2 :], 3)

    send, hit0, hit1, stats = call(
        dispatch_kernel,
        sc,
        (whole(far(tokens)), whole(far(cotangent)), whole(far(routing_t)), whole(far(router_weight))),
        (
            hbm((SENT, 2 * CH + 128), BF16),
            hbm((EXPERTS, TOK), BF16),
            hbm((EXPERTS, TOK), BF16),
            hbm((8, TOK), F32),
        ),
        (pltpu.VMEM((2 * CH // 128, SENT, 128), F32),),
    )
    got = lax.all_to_all(send.reshape(EXPERTS, 8, 2 * CH + 128), EP, 0, 0, tiled=True)
    pair, info = call(
        rows_kernel,
        sc,
        (got.reshape(SENT, 2 * CH + 128),),
        (hbm((128, 2 * D), BF16), hbm((128, 128), BF16)),
        (pltpu.VMEM((2 * CH // 128 + 1, SENT, 128), F32),),
    )
    pair_1 = shift(pair, 1)
    pair_3 = shift(pair, 3)
    top = shift(pair_1[0:64], 1)
    bottom = shift(pair_3[64:], 3)
    pairs = [pair, pair_1, top, bottom, pair_3]
    quarter_grads = hbm((128, 3 * FQ), BF16)
    grads = [None] * TP
    grads[0], grads[1], grads[3], back, gg = call(
        three_kernel,
        sc,
        (
            *(whole(far(x)) for x in (pair, info)),
            *((far(x), pl.BlockSpec(memory_space=pltpu.HBM)) for x in (packed, from_above, from_below)),
        ),
        (quarter_grads,) * 3 + (vmem((128, D), F32), vmem((128, 128), F32)),
        (pltpu.VMEM((3, D, 3 * FQ), BF16), pltpu.SemaphoreType.DMA((3,))),
    )
    grads[2], send_back = call(
        emit_kernel,
        sc,
        (*(whole(far(x)) for x in (pair, info, far_a, far_b)), back, gg),
        (quarter_grads, hbm((SENT, 2 * CH + 128), BF16)),
        (pltpu.VMEM((CH // 128, SENT, 128), F32),),
    )
    home = lax.all_to_all(send_back.reshape(EXPERTS, 8, 2 * CH + 128), EP, 0, 0, tiled=True)
    home = home.reshape(SENT, 2 * CH + 128)
    grads = [grads[0]] + [shift(grads[d], d) for d in (1, 2, 3)]
    grad_gate, grad_up, grad_down, down_norms, norms = call(
        sums_kernel,
        sc,
        tuple(whole(far(x)) for x in (*pairs, *grads)),
        (
            sds((D, FQ), BF16),
            sds((D, FQ), BF16),
            sds((FQ, D), BF16),
            sds((1, FQ), F32),
            hbm((16, 4 * 128), BF16),
        ),
    )
    (parts,) = call(
        home_kernel,
        sc,
        (home, whole(hit0), whole(hit1), whole(norms)),
        (vmem((TP, TOK + 32, DQ), BF16),),
        (pltpu.VMEM((2 * CH // 128 + 1, SENT, 128), F32),),
    )
    parts = lax.all_to_all(parts, "tp", 0, 0, tiled=True)
    grad_tokens, grad_gating, grad_router, router_norms, in_norms = call(
        last_kernel,
        sc,
        (
            parts,
            whole(stats),
            whole(routing_t),
            (router_weight, pl.BlockSpec((DQ, 128), lambda g, p: (p[0], 0))),
        ),
        (
            sds((TOK, DQ), BF16),
            sds((2, TOK), F32),
            sds((16, EXPERTS), F32),
            sds((1, 16), F32),
            sds((2, D), F32),
        ),
    )
    return (
        grad_tokens,
        grad_gating.T,
        grad_router,
        grad_gate[None],
        grad_up[None],
        grad_down[None],
        in_norms[None],
        down_norms,
        router_norms[0],
    )


def solution(mesh):
    split = Mesh(mesh.devices.reshape(8, 8, 2, TP), ("ep_0", "ep_1", "ep_2", "tp"))
    in_specs = (
        P(EP, None),
        P(EP, None),
        P(EP, None),
        P(),
        P(EP, None, "tp"),
        P(EP, None, "tp"),
        P(EP, "tp", None),
    )
    out_specs = (
        P(EP, "tp"),
        P(EP, None),
        P(EP, None),
        P(EP, None, "tp"),
        P(EP, None, "tp"),
        P(EP, "tp", None),
        P(EP, None, None),
        P(EP, "tp"),
        P(EP),
    )
    return jax.shard_map(layer, mesh=split, in_specs=in_specs, out_specs=out_specs, check_vma=False)
```

```python
import functools

import jax
import jax.numpy as jnp
from jax import lax
from jax.experimental import pallas as pl
from jax.experimental.pallas import tpu as pltpu
from jax.sharding import Mesh
from jax.sharding import PartitionSpec as P


EP = ("ep_0", "ep_1", "ep_2")
F32 = jnp.float32
BF16 = jnp.bfloat16


TOK = 128
D = 2048
EXPERTS = 128
TP = 4
DQ = D // TP
F = 512
FQ = F // TP
SENT = EXPERTS * 8
CH = D // 8


def dot(a, b, ca=1, cb=0):
    return lax.dot_general(a, b, (((ca,), (cb,)), ((), ())), preferred_element_type=F32)


def iota(shape, dim):
    return lax.broadcasted_iota(jnp.int32, shape, dim)


def pieces(x):
    hi = x.astype(BF16).astype(F32)
    rest = x - hi
    mid = rest.astype(BF16).astype(F32)
    return hi, mid, rest - mid


def spread(scratch, chunks):
    width = scratch.shape[0]
    for u, chunk in enumerate(chunks):
        for c in range(width):
            scratch[c, pl.ds(u, 128, stride=8), :] = chunk[:, 128 * c : 128 * (c + 1)].astype(F32)
    return jnp.concatenate([scratch[c].astype(BF16) for c in range(width)], axis=1)


def fill(scratch, got):
    for c in range(scratch.shape[0]):
        scratch[c] = got[:, 128 * c : 128 * (c + 1)].astype(F32)


def gather(scratch, u):
    return jnp.concatenate(
        [scratch[c, pl.ds(u, 128, stride=8), :].astype(BF16) for c in range(scratch.shape[0])], axis=1
    )


def every():
    return (iota((SENT, 128), 0) // 8 == iota((SENT, 128), 1)).astype(BF16)


ON_CHIP = pl.BlockSpec(memory_space=pltpu.VMEM)


def call(kernel, scalars, ins, outs, scratch=()):
    arrays = []
    specs = []
    for x in ins:
        if isinstance(x, tuple):
            arrays.append(x[0])
            specs.append(x[1])
        else:
            arrays.append(pltpu.with_memory_space_constraint(x, pltpu.VMEM))
            specs.append(ON_CHIP)
    return pl.pallas_call(
        kernel,
        grid_spec=pltpu.PrefetchScalarGridSpec(
            num_scalar_prefetch=1,
            grid=(1,),
            in_specs=tuple(specs),
            out_specs=(ON_CHIP,) * len(outs),
            scratch_shapes=scratch,
        ),
        out_shape=tuple(outs),
        compiler_params=pltpu.CompilerParams(vmem_limit_bytes=32 << 20),
    )(scalars, *arrays)


def whole(x):
    return (x, pl.BlockSpec(x.shape, lambda g, p: (0,) * x.ndim))


def sds(shape, dtype):
    return jax.ShapeDtypeStruct(shape, dtype)


def hbm(shape, dtype):
    return pltpu.HBM(shape, dtype)


def vmem(shape, dtype):
    return pltpu.VMEM(shape, dtype)


def dispatch_kernel(sc, tok, cot, routing, router, send, hit0, hit1, stats, scratch):
    experts = iota((EXPERTS, TOK), 0)
    picked = [(experts == routing[k : k + 1, :]) for k in range(2)]
    both = (picked[0] | picked[1]).astype(F32)
    logits = dot(router[...], tok[...], 0, 1)
    s = [
        jax.nn.sigmoid(jnp.sum(jnp.where(m, logits, 0.0), axis=0, keepdims=True)) for m in picked
    ]
    total = s[0] + s[1]
    g = [v / total for v in s]
    slope = [v * (1.0 - v) / total for v in s]
    before = (iota((TOK, TOK), 0) < iota((TOK, TOK), 1)).astype(BF16)
    within = dot(both.astype(BF16), before)
    mine = within == sc[0].astype(F32)
    line = iota((128, TOK), 0)
    hits = []
    info = None
    for k, out in ((0, hit0), (1, hit1)):
        hit = jnp.where(picked[k] & mine, 1.0, 0.0)
        out[...] = hit.astype(BF16)
        hits.append(hit)
        own = slope[k] * g[1 - k]
        other = slope[1 - k] * g[k]
        columns = [*pieces(g[k]), *pieces(own), *pieces(other), routing[1 - k : 2 - k, :].astype(F32)]
        table = jnp.zeros((128, TOK), F32)
        for c, v in enumerate(columns):
            table = jnp.where(line == c, v, table)
        part = dot(hit.astype(BF16), table.astype(BF16), 1, 1)
        info = part if info is None else info + part
    any_hit = (hits[0] + hits[1]).astype(BF16)
    toks = dot(any_hit, tok[...])
    cots = dot(any_hit, cot[...])
    send[:, 0 : 2 * CH] = spread(
        scratch,
        [
            jnp.concatenate([x[:, CH * u : CH * (u + 1)] for x in (toks, cots)], axis=1)
            for u in range(8)
        ],
    )
    send[:, 2 * CH :] = dot(every(), info.astype(BF16)).astype(BF16)
    stats[...] = jnp.concatenate(
        [s[0], s[1], total, g[0], g[1], total, total, total], axis=0
    )


def rows_kernel(sc, got, pair, info, scratch):
    fill(scratch, got)
    for u in range(8):
        part = gather(scratch, u)
        pair[:, CH * u : CH * (u + 1)] = part[:, 0:CH]
        pair[:, D + CH * u : D + CH * (u + 1)] = part[:, CH : 2 * CH]
        if u == 0:
            info[...] = part[:, 2 * CH :]


def quarter(pair, about, both, down, grads):
    pre = dot(pair[:, 0:D], both)
    back_raw = dot(pair[:, D:], down, 1, 1)
    pre_gate = pre[:, 0:FQ]
    pre_up = pre[:, FQ:]
    gating = about[:, 0:1] + about[:, 1:2] + about[:, 2:3]
    sig = jax.nn.sigmoid(pre_gate)
    activated = pre_gate * sig
    slope = sig * (1.0 + pre_gate * (1.0 - sig))
    hidden = (activated * pre_up).astype(BF16).astype(F32)
    gg = jnp.sum(hidden * back_raw, axis=1, keepdims=True)
    scaled = gating * back_raw
    g_in = jnp.concatenate([scaled * pre_up * slope, scaled * activated], axis=1).astype(BF16)
    grads[:, 0 : 2 * FQ] = g_in
    grads[:, 2 * FQ :] = (gating * hidden).astype(BF16)
    return gg, dot(g_in, both, 1, 1)


def three_kernel(sc, pair, info, *refs):
    weights, outs = refs[0:9], refs[9:12]
    back, gg_out, held, held_down, sems = refs[12:]
    copies = []
    for k in range(3):
        gate, up, down = weights[3 * k : 3 * k + 3]
        targets = (held.at[k, :, 0:FQ], held.at[k, :, FQ : 2 * FQ], held_down.at[k])
        copies.append(
            [
                pltpu.make_async_copy(x, t, sems.at[3 * k + c])
                for c, (x, t) in enumerate(zip((gate, up, down), targets))
            ]
        )
        for c in copies[k]:
            c.start()
    about = info[...].astype(F32)
    gg = None
    for k, grads in enumerate(outs):
        for c in copies[k]:
            c.wait()
        part, term = quarter(pair, about, held[k], held_down[k], grads)
        if gg is None:
            gg = part
            back[...] = term
        else:
            gg = gg + part
            back[...] += term
    gg_out[...] = jnp.broadcast_to(gg, (128, 128))


def emit_kernel(sc, pair, info, gate, up_a, up_b, down, back, gg_in, grads, send, scratch):
    about = info[...].astype(F32)
    up = jnp.concatenate([up_a[...], up_b[...]], axis=0)
    both = jnp.concatenate([gate[...], up], axis=1)
    gg, term = quarter(pair, about, both, down[...], grads)
    gg = gg + gg_in[:, 0:1]
    term = back[...] + term
    own = (about[:, 3:4] + about[:, 4:5] + about[:, 5:6]) * gg
    other = (about[:, 6:7] + about[:, 7:8] + about[:, 8:9]) * gg
    other_expert = about[:, 9:10].astype(jnp.int32)
    lane = iota((128, EXPERTS), 1)
    mix = jnp.where(lane == sc[1], own, 0.0) - jnp.where(lane == other_expert, other, 0.0)
    mix_hi = mix.astype(BF16)
    mix_lo = (mix - mix_hi.astype(F32)).astype(BF16)
    router = dot(pair[:, 0:D], jnp.concatenate([mix_hi, mix_lo], axis=1), 0, 0)
    router = (router[:, 0:EXPERTS] + router[:, EXPERTS:]).reshape(128, 2, 8, EXPERTS)
    send[:, 0:CH] = spread(scratch, [term[:, CH * u : CH * (u + 1)] for u in range(8)])
    for h in range(2):
        send[:, CH + 128 * h : CH + 128 * (h + 1)] = router[:, h].reshape(SENT, EXPERTS).astype(BF16)
    tail = jnp.zeros((128, 128), F32)
    for c, v in enumerate(pieces(gg)):
        tail = jnp.where(lane == c, v, tail)
    send[:, 2 * CH :] = dot(every(), tail.astype(BF16)).astype(BF16)


def row_sums(x):
    n, width = x.shape
    acc = x[:, 0:128]
    for c in range(1, width // 128):
        acc = acc + x[:, 128 * c : 128 * (c + 1)]
    return jnp.concatenate(
        [jnp.sum(acc[128 * c : 128 * (c + 1), :].T, axis=0, keepdims=True) for c in range(n // 128)],
        axis=0,
    )


def hop_kernel(sc, pair_1, pair_3, grads_1, grads_3, out_1, out_3):
    for out, rows, grads in ((out_1, pair_1[0:64, :], grads_1), (out_3, pair_3[64:, :], grads_3)):
        out[:, 0 : 2 * D] = rows
        for h in range(2):
            at = 2 * D + 3 * FQ * h
            out[:, at : at + 3 * FQ] = grads[64 * h : 64 * (h + 1), :]


def sums_kernel(sc, pair, pair_1, pair_3, hop_1, hop_3, grads_0, grads_2, *outs):
    gate, up, down, down_norms, norms = outs
    pairs = [pair[...], pair_1[...], hop_1[:, 0 : 2 * D], hop_3[:, 0 : 2 * D], pair_3[...]]
    grads = [grads_0[...]]
    halves = [slice(2 * D + 3 * FQ * h, 2 * D + 3 * FQ * (h + 1)) for h in range(2)]
    grads += [hop_1[:, at] for at in halves] + [grads_2[...]] + [hop_3[:, at] for at in halves]
    toks = jnp.concatenate([x[:, 0:D] for x in pairs], axis=0)
    cots = jnp.concatenate([x[:, D:] for x in pairs], axis=0)
    g_in = jnp.concatenate([g[:, 0 : 2 * FQ] for g in grads], axis=0)
    scaled = jnp.concatenate([g[:, 2 * FQ :] for g in grads], axis=0)
    in_sums = dot(toks, g_in, 0, 0)
    gate[...] = in_sums[:, 0:FQ].astype(BF16)
    up[...] = in_sums[:, FQ:].astype(BF16)
    squares = in_sums * in_sums
    lines = []
    for x in (squares[:, 0:FQ], squares[:, FQ:]):
        hi, mid, lo = pieces(row_sums(x))
        lines += [hi, mid + lo]
    norms[...] = jnp.concatenate(lines, axis=1).astype(BF16)
    down_sum = dot(scaled, cots, 0, 0)
    down[...] = down_sum.astype(BF16)
    down_norms[...] = row_sums(down_sum * down_sum)


def home_kernel(sc, got, hit0, hit1, norms, out, scratch):
    fill(scratch, got)
    hits = [hit0[...], hit1[...]]
    both = (hits[0].astype(F32) + hits[1].astype(F32)).astype(BF16)
    lines = [gather(scratch, u) for u in range(8)]
    terms = jnp.concatenate([x[:, 0:CH] for x in lines], axis=1)
    summed = dot(both, terms, 0, 0).astype(BF16)
    tail = lines[0][:, 2 * CH :]
    pick = (iota((8, SENT), 0) == iota((8, SENT), 1) % 8).astype(BF16)
    router = dot(pick, got[:, CH : 2 * CH])
    hi, mid, lo = pieces(router)
    lines = [jnp.concatenate([hi, mid + lo], axis=1)]
    flat = []
    for hit in hits:
        flat.append(dot(tail, hit, 0, 0)[0:4, :])
    flat = jnp.concatenate(flat, axis=0)
    lines.append(jnp.concatenate([flat] * 4, axis=1))
    extra = jnp.concatenate(lines, axis=0).astype(BF16)
    for q in range(TP):
        out[q, 0:TOK, :] = summed[:, DQ * q : DQ * (q + 1)]
        out[q, TOK : TOK + 16, :] = extra
        out[q, TOK + 16 :, :] = norms[...]


def last_kernel(
    sc, got, stats, routing, router, grad_tokens, grad_gating, grad_router, norms, in_norms
):
    total = got[0].astype(F32)
    for q in range(1, TP):
        total = total + got[q].astype(F32)
    extra = total[TOK:, :]
    rows = [
        extra[8 + 4 * k : 9 + 4 * k, 0:128]
        + extra[9 + 4 * k : 10 + 4 * k, 0:128]
        + extra[10 + 4 * k : 11 + 4 * k, 0:128]
        for k in range(2)
    ]
    grad_gating[...] = jnp.concatenate(rows, axis=0)
    st = stats[...]
    score_sum = st[2:3, :]
    weighted = st[3:4, :] * rows[0] + st[4:5, :] * rows[1]
    experts = iota((EXPERTS, TOK), 0)
    logits = jnp.zeros((EXPERTS, TOK), F32)
    for k in range(2):
        s = st[k : k + 1, :]
        chosen = (rows[k] - weighted) / score_sum * s * (1.0 - s)
        logits = jnp.where(experts == routing[k : k + 1, :], chosen, logits)
    term = dot(logits.astype(BF16), router[...], 0, 1)
    grad_tokens[...] = (total[0:TOK, :] + term).astype(BF16)
    sums = extra[0:8, 0:256] + extra[0:8, 256:512]
    x = jnp.concatenate([sums[:, 0:128], sums[:, 128:256]], axis=0)
    grad_router[...] = x
    squares = lax.dot_general(
        jnp.ones((8, EXPERTS), F32),
        x * x,
        (((1,), (1,)), ((), ())),
        precision=lax.Precision.HIGHEST,
        preferred_element_type=F32,
    )
    norms[...] = squares[0:1, :]
    for k in range(2):
        sums = extra[16:32, 256 * k : 256 * k + 128] + extra[16:32, 256 * k + 128 : 256 * (k + 1)]
        for c in range(D // 128):
            in_norms[k : k + 1, 128 * c : 128 * (c + 1)] = sums[c : c + 1, :]


def layer(tokens, cotangent, routing, router_weight, gate_weight, up_weight, down_weight):
    tp_index = lax.axis_index("tp")
    ep_index = lax.axis_index(EP)
    sc = jnp.stack([tp_index, ep_index]).astype(jnp.int32)
    routing_t = routing.T
    gate_w = gate_weight[0]
    up_w = up_weight[0]
    down_w = down_weight[0]
    far = functools.partial(pltpu.with_memory_space_constraint, memory_space=pltpu.HBM)

    def shift(x, d):
        return lax.ppermute(x, "tp", [(a, (a + d) % TP) for a in range(TP)])

    gate_1 = shift(gate_w, 1)
    down_3 = shift(down_w, 3)
    up_1 = shift(up_w, 1)
    up_3 = shift(up_w, 3)
    gate_2 = shift(gate_1, 1)
    down_2 = shift(down_3, 3)
    down_1 = shift(down_w, 1)
    gate_3 = shift(gate_w, 3)
    up_2a = shift(up_1[0 : D // 2], 1)
    up_2b = shift(up_3[D // 2 :], 3)

    send, hit0, hit1, stats = call(
        dispatch_kernel,
        sc,
        (whole(far(tokens)), whole(far(cotangent)), whole(far(routing_t)), whole(far(router_weight))),
        (
            hbm((SENT, 2 * CH + 128), BF16),
            hbm((EXPERTS, TOK), BF16),
            hbm((EXPERTS, TOK), BF16),
            hbm((8, TOK), F32),
        ),
        (pltpu.VMEM((2 * CH // 128, SENT, 128), F32),),
    )
    got = lax.all_to_all(send.reshape(EXPERTS, 8, 2 * CH + 128), EP, 0, 0, tiled=True)
    pair, info = call(
        rows_kernel,
        sc,
        (got.reshape(SENT, 2 * CH + 128),),
        (vmem((128, 2 * D), BF16), hbm((128, 128), BF16)),
        (pltpu.VMEM((2 * CH // 128 + 1, SENT, 128), F32),),
    )
    pair_1 = shift(pair, 1)
    pair_3 = shift(pair, 3)
    quarter_grads = hbm((128, 3 * FQ), BF16)
    grads = [None] * TP
    in_place = pl.BlockSpec(memory_space=pltpu.HBM)
    weights = (gate_w, up_w, down_w, gate_3, up_3, down_3, gate_1, up_1, down_1)
    grads[0], grads[1], grads[3], back, gg = call(
        three_kernel,
        sc,
        (pair, whole(far(info)), *((far(x), in_place) for x in weights)),
        (quarter_grads,) * 3 + (vmem((128, D), F32), vmem((128, 128), F32)),
        (
            pltpu.VMEM((3, D, 2 * FQ), BF16),
            pltpu.VMEM((3, FQ, D), BF16),
            pltpu.SemaphoreType.DMA((9,)),
        ),
    )
    grads[2], send_back = call(
        emit_kernel,
        sc,
        (pair, *(whole(far(x)) for x in (info, gate_2, up_2a, up_2b, down_2)), back, gg),
        (quarter_grads, hbm((SENT, 2 * CH + 128), BF16)),
        (pltpu.VMEM((CH // 128, SENT, 128), F32),),
    )
    home = lax.all_to_all(send_back.reshape(EXPERTS, 8, 2 * CH + 128), EP, 0, 0, tiled=True)
    home = home.reshape(SENT, 2 * CH + 128)
    hops = call(
        hop_kernel,
        sc,
        tuple(whole(far(x)) for x in (pair_1, pair_3, grads[1], grads[3])),
        (hbm((64, 2 * D + 6 * FQ), BF16),) * 2,
    )
    hop_1 = shift(hops[0], 1)
    hop_3 = shift(hops[1], 3)
    grads_2 = shift(grads[2], 2)
    grad_gate, grad_up, grad_down, down_norms, norms = call(
        sums_kernel,
        sc,
        tuple(whole(far(x)) for x in (pair, pair_1, pair_3, hop_1, hop_3, grads[0], grads_2)),
        (
            sds((D, FQ), BF16),
            sds((D, FQ), BF16),
            sds((FQ, D), BF16),
            sds((1, FQ), F32),
            vmem((16, 4 * 128), BF16),
        ),
    )
    (parts,) = call(
        home_kernel,
        sc,
        (home, whole(hit0), whole(hit1), norms),
        (vmem((TP, TOK + 32, DQ), BF16),),
        (pltpu.VMEM((2 * CH // 128 + 1, SENT, 128), F32),),
    )
    parts = lax.all_to_all(parts, "tp", 0, 0, tiled=True)
    grad_tokens, grad_gating, grad_router, router_norms, in_norms = call(
        last_kernel,
        sc,
        (
            parts,
            whole(stats),
            whole(routing_t),
            (router_weight, pl.BlockSpec((DQ, 128), lambda g, p: (p[0], 0))),
        ),
        (
            sds((TOK, DQ), BF16),
            sds((2, TOK), F32),
            sds((16, EXPERTS), F32),
            sds((1, 16), F32),
            sds((2, D), F32),
        ),
    )
    return (
        grad_tokens,
        grad_gating.T,
        grad_router,
        grad_gate[None],
        grad_up[None],
        grad_down[None],
        in_norms[None],
        down_norms,
        router_norms[0],
    )


def solution(mesh):
    split = Mesh(mesh.devices.reshape(8, 8, 2, TP), ("ep_0", "ep_1", "ep_2", "tp"))
    in_specs = (
        P(EP, None),
        P(EP, None),
        P(EP, None),
        P(),
        P(EP, None, "tp"),
        P(EP, None, "tp"),
        P(EP, "tp", None),
    )
    out_specs = (
        P(EP, "tp"),
        P(EP, None),
        P(EP, None),
        P(EP, None, "tp"),
        P(EP, None, "tp"),
        P(EP, "tp", None),
        P(EP, None, None),
        P(EP, "tp"),
        P(EP),
    )
    return jax.shard_map(layer, mesh=split, in_specs=in_specs, out_specs=out_specs, check_vma=False)
```

```python
import functools

import jax
import jax.numpy as jnp
from jax import lax
from jax.experimental import pallas as pl
from jax.experimental.pallas import tpu as pltpu
from jax.sharding import Mesh
from jax.sharding import PartitionSpec as P


EP = ("ep_0", "ep_1", "ep_2")
F32 = jnp.float32
BF16 = jnp.bfloat16


TOK = 128
D = 2048
EXPERTS = 128
TP = 4
DQ = D // TP
F = 512
FQ = F // TP
SENT = EXPERTS * 8
CH = D // 8


def dot(a, b, ca=1, cb=0):
    return lax.dot_general(a, b, (((ca,), (cb,)), ((), ())), preferred_element_type=F32)


def iota(shape, dim):
    return lax.broadcasted_iota(jnp.int32, shape, dim)


def pieces(x):
    hi = x.astype(BF16).astype(F32)
    rest = x - hi
    mid = rest.astype(BF16).astype(F32)
    return hi, mid, rest - mid


def spread(scratch, chunks):
    width = scratch.shape[0]
    for u, chunk in enumerate(chunks):
        for c in range(width):
            scratch[c, pl.ds(u, 128, stride=8), :] = chunk[:, 128 * c : 128 * (c + 1)].astype(F32)
    return jnp.concatenate([scratch[c].astype(BF16) for c in range(width)], axis=1)


def fill(scratch, got):
    for c in range(scratch.shape[0]):
        scratch[c] = got[:, 128 * c : 128 * (c + 1)].astype(F32)


def gather(scratch, u):
    return jnp.concatenate(
        [scratch[c, pl.ds(u, 128, stride=8), :].astype(BF16) for c in range(scratch.shape[0])], axis=1
    )


def every():
    return (iota((SENT, 128), 0) // 8 == iota((SENT, 128), 1)).astype(BF16)


ON_CHIP = pl.BlockSpec(memory_space=pltpu.VMEM)


def call(kernel, scalars, ins, outs, scratch=()):
    arrays = []
    specs = []
    for x in ins:
        if isinstance(x, tuple):
            arrays.append(x[0])
            specs.append(x[1])
        else:
            arrays.append(pltpu.with_memory_space_constraint(x, pltpu.VMEM))
            specs.append(ON_CHIP)
    return pl.pallas_call(
        kernel,
        grid_spec=pltpu.PrefetchScalarGridSpec(
            num_scalar_prefetch=1,
            grid=(1,),
            in_specs=tuple(specs),
            out_specs=(ON_CHIP,) * len(outs),
            scratch_shapes=scratch,
        ),
        out_shape=tuple(outs),
        compiler_params=pltpu.CompilerParams(vmem_limit_bytes=32 << 20),
    )(scalars, *arrays)


def whole(x):
    return (x, pl.BlockSpec(x.shape, lambda g, p: (0,) * x.ndim))


def sds(shape, dtype):
    return jax.ShapeDtypeStruct(shape, dtype)


def hbm(shape, dtype):
    return pltpu.HBM(shape, dtype)


def vmem(shape, dtype):
    return pltpu.VMEM(shape, dtype)


def dispatch_kernel(sc, tok, cot, routing, router, send, hit0, hit1, stats, scratch):
    experts = iota((EXPERTS, TOK), 0)
    picked = [(experts == routing[k : k + 1, :]) for k in range(2)]
    both = (picked[0] | picked[1]).astype(F32)
    logits = dot(router[...], tok[...], 0, 1)
    s = [
        jax.nn.sigmoid(jnp.sum(jnp.where(m, logits, 0.0), axis=0, keepdims=True)) for m in picked
    ]
    total = s[0] + s[1]
    g = [v / total for v in s]
    slope = [v * (1.0 - v) / total for v in s]
    before = (iota((TOK, TOK), 0) < iota((TOK, TOK), 1)).astype(BF16)
    within = dot(both.astype(BF16), before)
    mine = within == sc[0].astype(F32)
    line = iota((128, TOK), 0)
    hits = []
    info = None
    for k, out in ((0, hit0), (1, hit1)):
        hit = jnp.where(picked[k] & mine, 1.0, 0.0)
        out[...] = hit.astype(BF16)
        hits.append(hit)
        own = slope[k] * g[1 - k]
        other = slope[1 - k] * g[k]
        columns = [*pieces(g[k]), *pieces(own), *pieces(other), routing[1 - k : 2 - k, :].astype(F32)]
        table = jnp.zeros((128, TOK), F32)
        for c, v in enumerate(columns):
            table = jnp.where(line == c, v, table)
        part = dot(hit.astype(BF16), table.astype(BF16), 1, 1)
        info = part if info is None else info + part
    any_hit = (hits[0] + hits[1]).astype(BF16)
    toks = dot(any_hit, tok[...])
    cots = dot(any_hit, cot[...])
    send[:, 0 : 2 * CH] = spread(
        scratch,
        [
            jnp.concatenate([x[:, CH * u : CH * (u + 1)] for x in (toks, cots)], axis=1)
            for u in range(8)
        ],
    )
    send[:, 2 * CH :] = dot(every(), info.astype(BF16)).astype(BF16)
    stats[...] = jnp.concatenate(
        [s[0], s[1], total, g[0], g[1], total, total, total], axis=0
    )


def rows_kernel(sc, got, pair, info, scratch):
    fill(scratch, got)
    for u in range(8):
        part = gather(scratch, u)
        pair[:, CH * u : CH * (u + 1)] = part[:, 0:CH]
        pair[:, D + CH * u : D + CH * (u + 1)] = part[:, CH : 2 * CH]
        if u == 0:
            info[...] = part[:, 2 * CH :]


def quarter(pair, about, both, down, grads):
    pre = dot(pair[:, 0:D], both)
    back_raw = dot(pair[:, D:], down, 1, 1)
    pre_gate = pre[:, 0:FQ]
    pre_up = pre[:, FQ:]
    gating = about[:, 0:1] + about[:, 1:2] + about[:, 2:3]
    sig = jax.nn.sigmoid(pre_gate)
    activated = pre_gate * sig
    slope = sig * (1.0 + pre_gate * (1.0 - sig))
    hidden = (activated * pre_up).astype(BF16).astype(F32)
    gg = jnp.sum(hidden * back_raw, axis=1, keepdims=True)
    scaled = gating * back_raw
    g_in = jnp.concatenate([scaled * pre_up * slope, scaled * activated], axis=1).astype(BF16)
    grads[:, 0 : 2 * FQ] = g_in
    grads[:, 2 * FQ :] = (gating * hidden).astype(BF16)
    return gg, dot(g_in, both, 1, 1)


def three_kernel(sc, pair, info, *refs):
    weights, outs = refs[0:9], refs[9:12]
    back, gg_out, held, held_down, sems = refs[12:]
    copies = []
    for k in range(3):
        gate, up, down = weights[3 * k : 3 * k + 3]
        targets = (held.at[k, :, 0:FQ], held.at[k, :, FQ : 2 * FQ], held_down.at[k])
        copies.append(
            [
                pltpu.make_async_copy(x, t, sems.at[3 * k + c])
                for c, (x, t) in enumerate(zip((gate, up, down), targets))
            ]
        )
        for c in copies[k]:
            c.start()
    about = info[...].astype(F32)
    gg = None
    for k, grads in enumerate(outs):
        for c in copies[k]:
            c.wait()
        part, term = quarter(pair, about, held[k], held_down[k], grads)
        if gg is None:
            gg = part
            back[...] = term
        else:
            gg = gg + part
            back[...] += term
    gg_out[...] = jnp.broadcast_to(gg, (128, 128))


def emit_kernel(sc, pair, info, gate, up_a, up_b, down, back, gg_in, grads, send, scratch):
    about = info[...].astype(F32)
    up = jnp.concatenate([up_a[...], up_b[...]], axis=0)
    both = jnp.concatenate([gate[...], up], axis=1)
    gg, term = quarter(pair, about, both, down[...], grads)
    gg = gg + gg_in[:, 0:1]
    term = back[...] + term
    own = (about[:, 3:4] + about[:, 4:5] + about[:, 5:6]) * gg
    other = (about[:, 6:7] + about[:, 7:8] + about[:, 8:9]) * gg
    other_expert = about[:, 9:10].astype(jnp.int32)
    lane = iota((128, EXPERTS), 1)
    mix = jnp.where(lane == sc[1], own, 0.0) - jnp.where(lane == other_expert, other, 0.0)
    mix_hi = mix.astype(BF16)
    mix_lo = (mix - mix_hi.astype(F32)).astype(BF16)
    router = dot(pair[:, 0:D], jnp.concatenate([mix_hi, mix_lo], axis=1), 0, 0)
    router = (router[:, 0:EXPERTS] + router[:, EXPERTS:]).reshape(128, 2, 8, EXPERTS)
    send[:, 0:CH] = spread(scratch, [term[:, CH * u : CH * (u + 1)] for u in range(8)])
    for h in range(2):
        send[:, CH + 128 * h : CH + 128 * (h + 1)] = router[:, h].reshape(SENT, EXPERTS).astype(BF16)
    tail = jnp.zeros((128, 128), F32)
    for c, v in enumerate(pieces(gg)):
        tail = jnp.where(lane == c, v, tail)
    send[:, 2 * CH :] = dot(every(), tail.astype(BF16)).astype(BF16)


def row_sums(x):
    n, width = x.shape
    acc = x[:, 0:128]
    for c in range(1, width // 128):
        acc = acc + x[:, 128 * c : 128 * (c + 1)]
    return jnp.concatenate(
        [jnp.sum(acc[128 * c : 128 * (c + 1), :].T, axis=0, keepdims=True) for c in range(n // 128)],
        axis=0,
    )


def sums_kernel(sc, pair, pair_1, top, bottom, pair_3, *refs):
    grads = refs[0:4]
    gate, up, down, down_norms, norms = refs[4:]
    pairs = (pair, pair_1, top, bottom, pair_3)
    toks = jnp.concatenate([x[:, 0:D] for x in pairs], axis=0)
    cots = jnp.concatenate([x[:, D:] for x in pairs], axis=0)
    g_in = jnp.concatenate([g[:, 0 : 2 * FQ] for g in grads], axis=0)
    scaled = jnp.concatenate([g[:, 2 * FQ :] for g in grads], axis=0)
    in_sums = dot(toks, g_in, 0, 0)
    gate[...] = in_sums[:, 0:FQ].astype(BF16)
    up[...] = in_sums[:, FQ:].astype(BF16)
    squares = in_sums * in_sums
    lines = []
    for x in (squares[:, 0:FQ], squares[:, FQ:]):
        hi, mid, lo = pieces(row_sums(x))
        lines += [hi, mid + lo]
    norms[...] = jnp.concatenate(lines, axis=1).astype(BF16)
    down_sum = dot(scaled, cots, 0, 0)
    down[...] = down_sum.astype(BF16)
    down_norms[...] = row_sums(down_sum * down_sum)


def home_kernel(sc, got, hit0, hit1, norms, out, scratch):
    fill(scratch, got)
    hits = [hit0[...], hit1[...]]
    both = (hits[0].astype(F32) + hits[1].astype(F32)).astype(BF16)
    lines = [gather(scratch, u) for u in range(8)]
    terms = jnp.concatenate([x[:, 0:CH] for x in lines], axis=1)
    summed = dot(both, terms, 0, 0).astype(BF16)
    tail = lines[0][:, 2 * CH :]
    pick = (iota((8, SENT), 0) == iota((8, SENT), 1) % 8).astype(BF16)
    router = dot(pick, got[:, CH : 2 * CH])
    hi, mid, lo = pieces(router)
    lines = [jnp.concatenate([hi, mid + lo], axis=1)]
    flat = []
    for hit in hits:
        flat.append(dot(tail, hit, 0, 0)[0:4, :])
    flat = jnp.concatenate(flat, axis=0)
    lines.append(jnp.concatenate([flat] * 4, axis=1))
    extra = jnp.concatenate(lines, axis=0).astype(BF16)
    for q in range(TP):
        out[q, 0:TOK, :] = summed[:, DQ * q : DQ * (q + 1)]
        out[q, TOK : TOK + 16, :] = extra
        out[q, TOK + 16 :, :] = norms[...]


def last_kernel(
    sc, got, stats, routing, router, grad_tokens, grad_gating, grad_router, norms, in_norms
):
    total = got[0].astype(F32)
    for q in range(1, TP):
        total = total + got[q].astype(F32)
    extra = total[TOK:, :]
    rows = [
        extra[8 + 4 * k : 9 + 4 * k, 0:128]
        + extra[9 + 4 * k : 10 + 4 * k, 0:128]
        + extra[10 + 4 * k : 11 + 4 * k, 0:128]
        for k in range(2)
    ]
    grad_gating[...] = jnp.concatenate(rows, axis=0)
    st = stats[...]
    score_sum = st[2:3, :]
    weighted = st[3:4, :] * rows[0] + st[4:5, :] * rows[1]
    experts = iota((EXPERTS, TOK), 0)
    logits = jnp.zeros((EXPERTS, TOK), F32)
    for k in range(2):
        s = st[k : k + 1, :]
        chosen = (rows[k] - weighted) / score_sum * s * (1.0 - s)
        logits = jnp.where(experts == routing[k : k + 1, :], chosen, logits)
    term = dot(logits.astype(BF16), router[...], 0, 1)
    grad_tokens[...] = (total[0:TOK, :] + term).astype(BF16)
    sums = extra[0:8, 0:256] + extra[0:8, 256:512]
    x = jnp.concatenate([sums[:, 0:128], sums[:, 128:256]], axis=0)
    grad_router[...] = x
    squares = lax.dot_general(
        jnp.ones((8, EXPERTS), F32),
        x * x,
        (((1,), (1,)), ((), ())),
        precision=lax.Precision.HIGHEST,
        preferred_element_type=F32,
    )
    norms[...] = squares[0:1, :]
    for k in range(2):
        sums = extra[16:32, 256 * k : 256 * k + 128] + extra[16:32, 256 * k + 128 : 256 * (k + 1)]
        for c in range(D // 128):
            in_norms[k : k + 1, 128 * c : 128 * (c + 1)] = sums[c : c + 1, :]


def layer(tokens, cotangent, routing, router_weight, gate_weight, up_weight, down_weight):
    tp_index = lax.axis_index("tp")
    ep_index = lax.axis_index(EP)
    sc = jnp.stack([tp_index, ep_index]).astype(jnp.int32)
    routing_t = routing.T
    gate_w = gate_weight[0]
    up_w = up_weight[0]
    down_w = down_weight[0]
    far = functools.partial(pltpu.with_memory_space_constraint, memory_space=pltpu.HBM)

    def shift(x, d):
        return lax.ppermute(x, "tp", [(a, (a + d) % TP) for a in range(TP)])

    gate_1 = shift(gate_w, 1)
    down_3 = shift(down_w, 3)
    up_1 = shift(up_w, 1)
    up_3 = shift(up_w, 3)
    down_1 = shift(down_w, 1)
    gate_3 = shift(gate_w, 3)
    gate_2 = shift(gate_1, 1)
    down_2 = shift(down_3, 3)
    up_2a = shift(up_1[0 : D // 2], 1)
    up_2b = shift(up_3[D // 2 :], 3)

    send, hit0, hit1, stats = call(
        dispatch_kernel,
        sc,
        (whole(far(tokens)), whole(far(cotangent)), whole(far(routing_t)), whole(far(router_weight))),
        (
            hbm((SENT, 2 * CH + 128), BF16),
            hbm((EXPERTS, TOK), BF16),
            hbm((EXPERTS, TOK), BF16),
            hbm((8, TOK), F32),
        ),
        (pltpu.VMEM((2 * CH // 128, SENT, 128), F32),),
    )
    got = lax.all_to_all(send.reshape(EXPERTS, 8, 2 * CH + 128), EP, 0, 0, tiled=True)
    pair, info = call(
        rows_kernel,
        sc,
        (got.reshape(SENT, 2 * CH + 128),),
        (vmem((128, 2 * D), BF16), hbm((128, 128), BF16)),
        (pltpu.VMEM((2 * CH // 128 + 1, SENT, 128), F32),),
    )
    pair_1 = shift(pair, 1)
    pair_3 = shift(pair, 3)
    quarter_grads = hbm((128, 3 * FQ), BF16)
    grads = [None] * TP
    in_place = pl.BlockSpec(memory_space=pltpu.HBM)
    weights = (gate_w, up_w, down_w, gate_3, up_3, down_3, gate_1, up_1, down_1)
    grads[0], grads[1], grads[3], back, gg = call(
        three_kernel,
        sc,
        (pair, whole(far(info)), *((far(x), in_place) for x in weights)),
        (quarter_grads,) * 3 + (vmem((128, D), F32), vmem((128, 128), F32)),
        (
            pltpu.VMEM((3, D, 2 * FQ), BF16),
            pltpu.VMEM((3, FQ, D), BF16),
            pltpu.SemaphoreType.DMA((9,)),
        ),
    )
    grads[2], send_back = call(
        emit_kernel,
        sc,
        (pair, *(whole(far(x)) for x in (info, gate_2, up_2a, up_2b, down_2)), back, gg),
        (quarter_grads, hbm((SENT, 2 * CH + 128), BF16)),
        (pltpu.VMEM((CH // 128, SENT, 128), F32),),
    )
    home = lax.all_to_all(send_back.reshape(EXPERTS, 8, 2 * CH + 128), EP, 0, 0, tiled=True)
    home = home.reshape(SENT, 2 * CH + 128)
    grads[2] = shift(grads[2], 2)
    top = shift(pair_1[0:64], 1)
    bottom = shift(pair_3[64:], 3)
    grads[1] = shift(grads[1], 1)
    grads[3] = shift(grads[3], 3)
    grad_gate, grad_up, grad_down, down_norms, norms = call(
        sums_kernel,
        sc,
        tuple(whole(far(x)) for x in (pair, pair_1, top, bottom, pair_3, *grads)),
        (
            sds((D, FQ), BF16),
            sds((D, FQ), BF16),
            sds((FQ, D), BF16),
            sds((1, FQ), F32),
            vmem((16, 4 * 128), BF16),
        ),
    )
    (parts,) = call(
        home_kernel,
        sc,
        (home, whole(hit0), whole(hit1), norms),
        (vmem((TP, TOK + 32, DQ), BF16),),
        (pltpu.VMEM((2 * CH // 128 + 1, SENT, 128), F32),),
    )
    parts = lax.all_to_all(parts, "tp", 0, 0, tiled=True)
    grad_tokens, grad_gating, grad_router, router_norms, in_norms = call(
        last_kernel,
        sc,
        (
            parts,
            whole(stats),
            whole(routing_t),
            (router_weight, pl.BlockSpec((DQ, 128), lambda g, p: (p[0], 0))),
        ),
        (
            sds((TOK, DQ), BF16),
            sds((2, TOK), F32),
            sds((16, EXPERTS), F32),
            sds((1, 16), F32),
            sds((2, D), F32),
        ),
    )
    return (
        grad_tokens,
        grad_gating.T,
        grad_router,
        grad_gate[None],
        grad_up[None],
        grad_down[None],
        in_norms[None],
        down_norms,
        router_norms[0],
    )


def solution(mesh):
    split = Mesh(mesh.devices.reshape(8, 8, 2, TP), ("ep_0", "ep_1", "ep_2", "tp"))
    in_specs = (
        P(EP, None),
        P(EP, None),
        P(EP, None),
        P(),
        P(EP, None, "tp"),
        P(EP, None, "tp"),
        P(EP, "tp", None),
    )
    out_specs = (
        P(EP, "tp"),
        P(EP, None),
        P(EP, None),
        P(EP, None, "tp"),
        P(EP, None, "tp"),
        P(EP, "tp", None),
        P(EP, None, None),
        P(EP, "tp"),
        P(EP),
    )
    return jax.shard_map(layer, mesh=split, in_specs=in_specs, out_specs=out_specs, check_vma=False)
```

```python
import functools

import jax
import jax.numpy as jnp
from jax import lax
from jax.experimental import pallas as pl
from jax.experimental.pallas import tpu as pltpu
from jax.sharding import Mesh
from jax.sharding import PartitionSpec as P


EP = ("ep_0", "ep_1", "ep_2")
F32 = jnp.float32
BF16 = jnp.bfloat16


TOK = 128
D = 2048
EXPERTS = 128
TP = 4
DQ = D // TP
F = 512
FQ = F // TP
SENT = EXPERTS * 8
CH = D // 8


def dot(a, b, ca=1, cb=0):
    return lax.dot_general(a, b, (((ca,), (cb,)), ((), ())), preferred_element_type=F32)


def iota(shape, dim):
    return lax.broadcasted_iota(jnp.int32, shape, dim)


def pieces(x):
    hi = x.astype(BF16).astype(F32)
    rest = x - hi
    mid = rest.astype(BF16).astype(F32)
    return hi, mid, rest - mid


def spread(scratch, chunks):
    width = scratch.shape[0]
    for u, chunk in enumerate(chunks):
        for c in range(width):
            scratch[c, pl.ds(u, 128, stride=8), :] = chunk[:, 128 * c : 128 * (c + 1)].astype(F32)
    return jnp.concatenate([scratch[c].astype(BF16) for c in range(width)], axis=1)


def fill(scratch, got):
    for c in range(scratch.shape[0]):
        scratch[c] = got[:, 128 * c : 128 * (c + 1)].astype(F32)


def gather(scratch, u):
    return jnp.concatenate(
        [scratch[c, pl.ds(u, 128, stride=8), :].astype(BF16) for c in range(scratch.shape[0])], axis=1
    )


def every():
    return (iota((SENT, 128), 0) // 8 == iota((SENT, 128), 1)).astype(BF16)


ON_CHIP = pl.BlockSpec(memory_space=pltpu.VMEM)


def call(kernel, scalars, ins, outs, scratch=()):
    arrays = []
    specs = []
    for x in ins:
        if isinstance(x, tuple):
            arrays.append(x[0])
            specs.append(x[1])
        else:
            arrays.append(pltpu.with_memory_space_constraint(x, pltpu.VMEM))
            specs.append(ON_CHIP)
    return pl.pallas_call(
        kernel,
        grid_spec=pltpu.PrefetchScalarGridSpec(
            num_scalar_prefetch=1,
            grid=(1,),
            in_specs=tuple(specs),
            out_specs=(ON_CHIP,) * len(outs),
            scratch_shapes=scratch,
        ),
        out_shape=tuple(outs),
        compiler_params=pltpu.CompilerParams(vmem_limit_bytes=32 << 20),
    )(scalars, *arrays)


def whole(x):
    return (x, pl.BlockSpec(x.shape, lambda g, p: (0,) * x.ndim))


def sds(shape, dtype):
    return jax.ShapeDtypeStruct(shape, dtype)


def hbm(shape, dtype):
    return pltpu.HBM(shape, dtype)


def vmem(shape, dtype):
    return pltpu.VMEM(shape, dtype)


def dispatch_kernel(sc, tok, cot, routing, router, send, hit0, hit1, stats, scratch):
    experts = iota((EXPERTS, TOK), 0)
    picked = [(experts == routing[k : k + 1, :]) for k in range(2)]
    both = (picked[0] | picked[1]).astype(F32)
    logits = dot(router[...], tok[...], 0, 1)
    s = [
        jax.nn.sigmoid(jnp.sum(jnp.where(m, logits, 0.0), axis=0, keepdims=True)) for m in picked
    ]
    total = s[0] + s[1]
    g = [v / total for v in s]
    slope = [v * (1.0 - v) / total for v in s]
    before = (iota((TOK, TOK), 0) < iota((TOK, TOK), 1)).astype(BF16)
    within = dot(both.astype(BF16), before)
    mine = within == sc[0].astype(F32)
    line = iota((128, TOK), 0)
    hits = []
    info = None
    for k, out in ((0, hit0), (1, hit1)):
        hit = jnp.where(picked[k] & mine, 1.0, 0.0)
        out[...] = hit.astype(BF16)
        hits.append(hit)
        own = slope[k] * g[1 - k]
        other = slope[1 - k] * g[k]
        columns = [*pieces(g[k]), *pieces(own), *pieces(other), routing[1 - k : 2 - k, :].astype(F32)]
        table = jnp.zeros((128, TOK), F32)
        for c, v in enumerate(columns):
            table = jnp.where(line == c, v, table)
        part = dot(hit.astype(BF16), table.astype(BF16), 1, 1)
        info = part if info is None else info + part
    any_hit = (hits[0] + hits[1]).astype(BF16)
    toks = dot(any_hit, tok[...])
    cots = dot(any_hit, cot[...])
    send[:, 0 : 2 * CH] = spread(
        scratch,
        [
            jnp.concatenate([x[:, CH * u : CH * (u + 1)] for x in (toks, cots)], axis=1)
            for u in range(8)
        ],
    )
    send[:, 2 * CH :] = dot(every(), info.astype(BF16)).astype(BF16)
    stats[...] = jnp.concatenate(
        [s[0], s[1], total, g[0], g[1], total, total, total], axis=0
    )


def rows_kernel(sc, got, pair, scratch):
    fill(scratch, got)
    for u in range(8):
        part = gather(scratch, u)
        pair[:, CH * u : CH * (u + 1)] = part[:, 0:CH]
        pair[:, D + CH * u : D + CH * (u + 1)] = part[:, CH : 2 * CH]
        if u == 0:
            pair[:, 2 * D :] = part[:, 2 * CH :]


def hidden_grads(pair, both, down):
    pre = dot(pair[:, 0:D], both)
    back_raw = dot(pair[:, D : 2 * D], down, 1, 1)
    about = pair[:, 2 * D :].astype(F32)
    pre_gate = pre[:, 0:FQ]
    pre_up = pre[:, FQ:]
    gating = about[:, 0:1] + about[:, 1:2] + about[:, 2:3]
    sig = jax.nn.sigmoid(pre_gate)
    activated = pre_gate * sig
    slope = sig * (1.0 + pre_gate * (1.0 - sig))
    hidden = (activated * pre_up).astype(BF16).astype(F32)
    gg = jnp.sum(hidden * back_raw, axis=1, keepdims=True)
    scaled = gating * back_raw
    g_in = jnp.concatenate([scaled * pre_up * slope, scaled * activated], axis=1).astype(BF16)
    return g_in, (gating * hidden).astype(BF16), gg


def three_kernel(sc, pair, *refs):
    weights = refs[0:9]
    grads, back, gg_out, held, held_down, sems = refs[9:]
    copies = []
    for k in range(3):
        gate, up, down = weights[3 * k : 3 * k + 3]
        targets = (held.at[k, :, 0:FQ], held.at[k, :, FQ : 2 * FQ], held_down.at[k])
        copies.append(
            [
                pltpu.make_async_copy(x, t, sems.at[3 * k + c])
                for c, (x, t) in enumerate(zip((gate, up, down), targets))
            ]
        )
        for c in copies[k]:
            c.start()
    gg = None
    for k in range(3):
        for c in copies[k]:
            c.wait()
        g_in, scaled, part = hidden_grads(pair, held[k], held_down[k])
        term = dot(g_in, held[k], 1, 1)
        if k == 0:
            grads[:, 0 : 2 * FQ] = g_in
            grads[:, 2 * FQ :] = scaled
            gg = part
            back[...] = term
        else:
            gg = gg + part
            back[...] += term
    gg_out[...] = jnp.broadcast_to(gg, (128, 128))


def redo_kernel(sc, pair_1, pair_3, gate, up, down, out_1, out_3):
    both = jnp.concatenate([gate[...], up[...]], axis=1)
    for pair, out in ((pair_1, out_1), (pair_3, out_3)):
        g_in, scaled, _ = hidden_grads(pair, both, down[...])
        out[:, 0 : 2 * FQ] = g_in
        out[:, 2 * FQ :] = scaled


def emit_kernel(sc, pair, gate, up_a, up_b, down, back, gg_in, send, scratch):
    about = pair[:, 2 * D :].astype(F32)
    up = jnp.concatenate([up_a[...], up_b[...]], axis=0)
    both = jnp.concatenate([gate[...], up], axis=1)
    g_in, _, gg = hidden_grads(pair, both, down[...])
    term = back[...] + dot(g_in, both, 1, 1)
    gg = gg + gg_in[:, 0:1]
    own = (about[:, 3:4] + about[:, 4:5] + about[:, 5:6]) * gg
    other = (about[:, 6:7] + about[:, 7:8] + about[:, 8:9]) * gg
    other_expert = about[:, 9:10].astype(jnp.int32)
    lane = iota((128, EXPERTS), 1)
    mix = jnp.where(lane == sc[1], own, 0.0) - jnp.where(lane == other_expert, other, 0.0)
    mix_hi = mix.astype(BF16)
    mix_lo = (mix - mix_hi.astype(F32)).astype(BF16)
    router = dot(pair[:, 0:D], jnp.concatenate([mix_hi, mix_lo], axis=1), 0, 0)
    router = (router[:, 0:EXPERTS] + router[:, EXPERTS:]).reshape(128, 2, 8, EXPERTS)
    send[:, 0:CH] = spread(scratch, [term[:, CH * u : CH * (u + 1)] for u in range(8)])
    for h in range(2):
        send[:, CH + 128 * h : CH + 128 * (h + 1)] = router[:, h].reshape(SENT, EXPERTS).astype(BF16)
    tail = jnp.zeros((128, 128), F32)
    for c, v in enumerate(pieces(gg)):
        tail = jnp.where(lane == c, v, tail)
    send[:, 2 * CH :] = dot(every(), tail.astype(BF16)).astype(BF16)


def row_sums(x):
    n, width = x.shape
    acc = x[:, 0:128]
    for c in range(1, width // 128):
        acc = acc + x[:, 128 * c : 128 * (c + 1)]
    return jnp.concatenate(
        [jnp.sum(acc[128 * c : 128 * (c + 1), :].T, axis=0, keepdims=True) for c in range(n // 128)],
        axis=0,
    )


def sums_kernel(
    sc, pair, pair_1, top, bottom, pair_3, grads_0, grads_1, grads_3, gate_w, up_w, down_w, *outs
):
    gate, up, down, down_norms, norms = outs
    distant = jnp.concatenate([top[...], bottom[...]], axis=0)
    both = jnp.concatenate([gate_w[...], up_w[...]], axis=1)
    far_in, far_scaled, _ = hidden_grads(distant, both, down_w[...])
    pairs = (pair, pair_1, distant, pair_3)
    toks = jnp.concatenate([x[:, 0:D] for x in pairs], axis=0)
    cots = jnp.concatenate([x[:, D : 2 * D] for x in pairs], axis=0)
    at = slice(0, 2 * FQ)
    g_in = jnp.concatenate([grads_0[:, at], grads_1[:, at], far_in, grads_3[:, at]], axis=0)
    at = slice(2 * FQ, 3 * FQ)
    scaled = jnp.concatenate([grads_0[:, at], grads_1[:, at], far_scaled, grads_3[:, at]], axis=0)
    in_sums = dot(toks, g_in, 0, 0)
    gate[...] = in_sums[:, 0:FQ].astype(BF16)
    up[...] = in_sums[:, FQ:].astype(BF16)
    squares = in_sums * in_sums
    lines = []
    for x in (squares[:, 0:FQ], squares[:, FQ:]):
        hi, mid, lo = pieces(row_sums(x))
        lines += [hi, mid + lo]
    norms[...] = jnp.concatenate(lines, axis=1).astype(BF16)
    down_sum = dot(scaled, cots, 0, 0)
    down[...] = down_sum.astype(BF16)
    down_norms[...] = row_sums(down_sum * down_sum)


def home_kernel(sc, got, hit0, hit1, norms, out, scratch):
    fill(scratch, got)
    hits = [hit0[...], hit1[...]]
    both = (hits[0].astype(F32) + hits[1].astype(F32)).astype(BF16)
    lines = [gather(scratch, u) for u in range(8)]
    terms = jnp.concatenate([x[:, 0:CH] for x in lines], axis=1)
    summed = dot(both, terms, 0, 0).astype(BF16)
    tail = lines[0][:, 2 * CH :]
    pick = (iota((8, SENT), 0) == iota((8, SENT), 1) % 8).astype(BF16)
    router = dot(pick, got[:, CH : 2 * CH])
    hi, mid, lo = pieces(router)
    lines = [jnp.concatenate([hi, mid + lo], axis=1)]
    flat = []
    for hit in hits:
        flat.append(dot(tail, hit, 0, 0)[0:4, :])
    flat = jnp.concatenate(flat, axis=0)
    lines.append(jnp.concatenate([flat] * 4, axis=1))
    extra = jnp.concatenate(lines, axis=0).astype(BF16)
    for q in range(TP):
        out[q, 0:TOK, :] = summed[:, DQ * q : DQ * (q + 1)]
        out[q, TOK : TOK + 16, :] = extra
        out[q, TOK + 16 :, :] = norms[...]


def last_kernel(
    sc, got, stats, routing, router, grad_tokens, grad_gating, grad_router, norms, in_norms
):
    total = got[0].astype(F32)
    for q in range(1, TP):
        total = total + got[q].astype(F32)
    extra = total[TOK:, :]
    rows = [
        extra[8 + 4 * k : 9 + 4 * k, 0:128]
        + extra[9 + 4 * k : 10 + 4 * k, 0:128]
        + extra[10 + 4 * k : 11 + 4 * k, 0:128]
        for k in range(2)
    ]
    grad_gating[...] = jnp.concatenate(rows, axis=0)
    st = stats[...]
    score_sum = st[2:3, :]
    weighted = st[3:4, :] * rows[0] + st[4:5, :] * rows[1]
    experts = iota((EXPERTS, TOK), 0)
    logits = jnp.zeros((EXPERTS, TOK), F32)
    for k in range(2):
        s = st[k : k + 1, :]
        chosen = (rows[k] - weighted) / score_sum * s * (1.0 - s)
        logits = jnp.where(experts == routing[k : k + 1, :], chosen, logits)
    term = dot(logits.astype(BF16), router[...], 0, 1)
    grad_tokens[...] = (total[0:TOK, :] + term).astype(BF16)
    sums = extra[0:8, 0:256] + extra[0:8, 256:512]
    x = jnp.concatenate([sums[:, 0:128], sums[:, 128:256]], axis=0)
    grad_router[...] = x
    squares = lax.dot_general(
        jnp.ones((8, EXPERTS), F32),
        x * x,
        (((1,), (1,)), ((), ())),
        precision=lax.Precision.HIGHEST,
        preferred_element_type=F32,
    )
    norms[...] = squares[0:1, :]
    for k in range(2):
        sums = extra[16:32, 256 * k : 256 * k + 128] + extra[16:32, 256 * k + 128 : 256 * (k + 1)]
        for c in range(D // 128):
            in_norms[k : k + 1, 128 * c : 128 * (c + 1)] = sums[c : c + 1, :]


def layer(tokens, cotangent, routing, router_weight, gate_weight, up_weight, down_weight):
    tp_index = lax.axis_index("tp")
    ep_index = lax.axis_index(EP)
    sc = jnp.stack([tp_index, ep_index]).astype(jnp.int32)
    routing_t = routing.T
    gate_w = gate_weight[0]
    up_w = up_weight[0]
    down_w = down_weight[0]
    far = functools.partial(pltpu.with_memory_space_constraint, memory_space=pltpu.HBM)

    def shift(x, d):
        return lax.ppermute(x, "tp", [(a, (a + d) % TP) for a in range(TP)])

    gate_1 = shift(gate_w, 1)
    down_3 = shift(down_w, 3)
    up_1 = shift(up_w, 1)
    up_3 = shift(up_w, 3)
    down_1 = shift(down_w, 1)
    gate_3 = shift(gate_w, 3)
    gate_2 = shift(gate_1, 1)
    down_2 = shift(down_3, 3)
    up_2a = shift(up_1[0 : D // 2], 1)
    up_2b = shift(up_3[D // 2 :], 3)

    send, hit0, hit1, stats = call(
        dispatch_kernel,
        sc,
        (whole(far(tokens)), whole(far(cotangent)), whole(far(routing_t)), whole(far(router_weight))),
        (
            hbm((SENT, 2 * CH + 128), BF16),
            hbm((EXPERTS, TOK), BF16),
            hbm((EXPERTS, TOK), BF16),
            hbm((8, TOK), F32),
        ),
        (pltpu.VMEM((2 * CH // 128, SENT, 128), F32),),
    )
    got = lax.all_to_all(send.reshape(EXPERTS, 8, 2 * CH + 128), EP, 0, 0, tiled=True)
    (pair,) = call(
        rows_kernel,
        sc,
        (got.reshape(SENT, 2 * CH + 128),),
        (vmem((128, 2 * D + 128), BF16),),
        (pltpu.VMEM((2 * CH // 128 + 1, SENT, 128), F32),),
    )
    pair_1 = shift(pair, 1)
    pair_3 = shift(pair, 3)
    quarter_grads = hbm((128, 3 * FQ), BF16)
    in_place = pl.BlockSpec(memory_space=pltpu.HBM)
    weights = (gate_w, up_w, down_w, gate_3, up_3, down_3, gate_1, up_1, down_1)
    grads_0, back, gg = call(
        three_kernel,
        sc,
        (pair, *((far(x), in_place) for x in weights)),
        (quarter_grads, vmem((128, D), F32), vmem((128, 128), F32)),
        (
            pltpu.VMEM((3, D, 2 * FQ), BF16),
            pltpu.VMEM((3, FQ, D), BF16),
            pltpu.SemaphoreType.DMA((9,)),
        ),
    )
    (send_back,) = call(
        emit_kernel,
        sc,
        (pair, *(whole(far(x)) for x in (gate_2, up_2a, up_2b, down_2)), back, gg),
        (hbm((SENT, 2 * CH + 128), BF16),),
        (pltpu.VMEM((CH // 128, SENT, 128), F32),),
    )
    home = lax.all_to_all(send_back.reshape(EXPERTS, 8, 2 * CH + 128), EP, 0, 0, tiled=True)
    home = home.reshape(SENT, 2 * CH + 128)
    top = shift(pair_1[0:64], 1)
    bottom = shift(pair_3[64:], 3)
    own_weights = tuple(whole(far(x)) for x in (gate_w, up_w, down_w))
    grads_1, grads_3 = call(
        redo_kernel,
        sc,
        (*(whole(far(x)) for x in (pair_1, pair_3)), *own_weights),
        (quarter_grads,) * 2,
    )
    grad_gate, grad_up, grad_down, down_norms, norms = call(
        sums_kernel,
        sc,
        (
            *(whole(far(x)) for x in (pair, pair_1, top, bottom, pair_3, grads_0, grads_1, grads_3)),
            *own_weights,
        ),
        (
            sds((D, FQ), BF16),
            sds((D, FQ), BF16),
            sds((FQ, D), BF16),
            sds((1, FQ), F32),
            vmem((16, 4 * 128), BF16),
        ),
    )
    (parts,) = call(
        home_kernel,
        sc,
        (home, whole(hit0), whole(hit1), norms),
        (vmem((TP, TOK + 32, DQ), BF16),),
        (pltpu.VMEM((2 * CH // 128 + 1, SENT, 128), F32),),
    )
    parts = lax.all_to_all(parts, "tp", 0, 0, tiled=True)
    grad_tokens, grad_gating, grad_router, router_norms, in_norms = call(
        last_kernel,
        sc,
        (
            parts,
            whole(stats),
            whole(routing_t),
            (router_weight, pl.BlockSpec((DQ, 128), lambda g, p: (p[0], 0))),
        ),
        (
            sds((TOK, DQ), BF16),
            sds((2, TOK), F32),
            sds((16, EXPERTS), F32),
            sds((1, 16), F32),
            sds((2, D), F32),
        ),
    )
    return (
        grad_tokens,
        grad_gating.T,
        grad_router,
        grad_gate[None],
        grad_up[None],
        grad_down[None],
        in_norms[None],
        down_norms,
        router_norms[0],
    )


def solution(mesh):
    split = Mesh(mesh.devices.reshape(8, 8, 2, TP), ("ep_0", "ep_1", "ep_2", "tp"))
    in_specs = (
        P(EP, None),
        P(EP, None),
        P(EP, None),
        P(),
        P(EP, None, "tp"),
        P(EP, None, "tp"),
        P(EP, "tp", None),
    )
    out_specs = (
        P(EP, "tp"),
        P(EP, None),
        P(EP, None),
        P(EP, None, "tp"),
        P(EP, None, "tp"),
        P(EP, "tp", None),
        P(EP, None, None),
        P(EP, "tp"),
        P(EP),
    )
    return jax.shard_map(layer, mesh=split, in_specs=in_specs, out_specs=out_specs, check_vma=False)
```

```python
import functools

import jax
import jax.numpy as jnp
from jax import lax
from jax.experimental import pallas as pl
from jax.experimental.pallas import tpu as pltpu
from jax.sharding import Mesh
from jax.sharding import PartitionSpec as P


EP = ("ep_0", "ep_1", "ep_2")
F32 = jnp.float32
BF16 = jnp.bfloat16


TOK = 128
D = 2048
EXPERTS = 128
TP = 4
DQ = D // TP
F = 512
FQ = F // TP
SENT = EXPERTS * 8
CH = D // 8


def dot(a, b, ca=1, cb=0):
    return lax.dot_general(a, b, (((ca,), (cb,)), ((), ())), preferred_element_type=F32)


def iota(shape, dim):
    return lax.broadcasted_iota(jnp.int32, shape, dim)


def pieces(x):
    hi = x.astype(BF16).astype(F32)
    rest = x - hi
    mid = rest.astype(BF16).astype(F32)
    return hi, mid, rest - mid


def spread(scratch, chunks):
    width = scratch.shape[0]
    for u, chunk in enumerate(chunks):
        for c in range(width):
            scratch[c, pl.ds(u, 128, stride=8), :] = chunk[:, 128 * c : 128 * (c + 1)].astype(F32)
    return jnp.concatenate([scratch[c].astype(BF16) for c in range(width)], axis=1)


def fill(scratch, got):
    for c in range(scratch.shape[0]):
        scratch[c] = got[:, 128 * c : 128 * (c + 1)].astype(F32)


def gather(scratch, u):
    return jnp.concatenate(
        [scratch[c, pl.ds(u, 128, stride=8), :].astype(BF16) for c in range(scratch.shape[0])], axis=1
    )


def every():
    return (iota((SENT, 128), 0) // 8 == iota((SENT, 128), 1)).astype(BF16)


ON_CHIP = pl.BlockSpec(memory_space=pltpu.VMEM)


def call(kernel, scalars, ins, outs, scratch=()):
    arrays = []
    specs = []
    for x in ins:
        if isinstance(x, tuple):
            arrays.append(x[0])
            specs.append(x[1])
        else:
            arrays.append(pltpu.with_memory_space_constraint(x, pltpu.VMEM))
            specs.append(ON_CHIP)
    return pl.pallas_call(
        kernel,
        grid_spec=pltpu.PrefetchScalarGridSpec(
            num_scalar_prefetch=1,
            grid=(1,),
            in_specs=tuple(specs),
            out_specs=(ON_CHIP,) * len(outs),
            scratch_shapes=scratch,
        ),
        out_shape=tuple(outs),
        compiler_params=pltpu.CompilerParams(vmem_limit_bytes=32 << 20),
    )(scalars, *arrays)


def whole(x):
    return (x, pl.BlockSpec(x.shape, lambda g, p: (0,) * x.ndim))


def sds(shape, dtype):
    return jax.ShapeDtypeStruct(shape, dtype)


def hbm(shape, dtype):
    return pltpu.HBM(shape, dtype)


def vmem(shape, dtype):
    return pltpu.VMEM(shape, dtype)


def dispatch_kernel(sc, tok, cot, routing, router, send, hit0, hit1, stats, scratch):
    experts = iota((EXPERTS, TOK), 0)
    picked = [(experts == routing[k : k + 1, :]) for k in range(2)]
    both = (picked[0] | picked[1]).astype(F32)
    logits = dot(router[...], tok[...], 0, 1)
    s = [
        jax.nn.sigmoid(jnp.sum(jnp.where(m, logits, 0.0), axis=0, keepdims=True)) for m in picked
    ]
    total = s[0] + s[1]
    g = [v / total for v in s]
    slope = [v * (1.0 - v) / total for v in s]
    before = (iota((TOK, TOK), 0) < iota((TOK, TOK), 1)).astype(BF16)
    within = dot(both.astype(BF16), before)
    mine = within == sc[0].astype(F32)
    line = iota((128, TOK), 0)
    hits = []
    info = None
    for k, out in ((0, hit0), (1, hit1)):
        hit = jnp.where(picked[k] & mine, 1.0, 0.0)
        out[...] = hit.astype(BF16)
        hits.append(hit)
        own = slope[k] * g[1 - k]
        other = slope[1 - k] * g[k]
        columns = [*pieces(g[k]), *pieces(own), *pieces(other), routing[1 - k : 2 - k, :].astype(F32)]
        table = jnp.zeros((128, TOK), F32)
        for c, v in enumerate(columns):
            table = jnp.where(line == c, v, table)
        part = dot(hit.astype(BF16), table.astype(BF16), 1, 1)
        info = part if info is None else info + part
    any_hit = (hits[0] + hits[1]).astype(BF16)
    toks = dot(any_hit, tok[...])
    cots = dot(any_hit, cot[...])
    send[:, 0 : 2 * CH] = spread(
        scratch,
        [
            jnp.concatenate([x[:, CH * u : CH * (u + 1)] for x in (toks, cots)], axis=1)
            for u in range(8)
        ],
    )
    send[:, 2 * CH :] = dot(every(), info.astype(BF16)).astype(BF16)
    stats[...] = jnp.concatenate(
        [s[0], s[1], total, g[0], g[1], total, total, total], axis=0
    )


def rows_kernel(sc, got, pair, scratch):
    fill(scratch, got)
    for u in range(8):
        part = gather(scratch, u)
        pair[:, CH * u : CH * (u + 1)] = part[:, 0:CH]
        pair[:, D + CH * u : D + CH * (u + 1)] = part[:, CH : 2 * CH]
        if u == 0:
            pair[:, 2 * D :] = part[:, 2 * CH :]


def hidden_grads(pair, both, down):
    pre = dot(pair[:, 0:D], both)
    back_raw = dot(pair[:, D : 2 * D], down, 1, 1)
    about = pair[:, 2 * D :].astype(F32)
    pre_gate = pre[:, 0:FQ]
    pre_up = pre[:, FQ:]
    gating = about[:, 0:1] + about[:, 1:2] + about[:, 2:3]
    sig = jax.nn.sigmoid(pre_gate)
    activated = pre_gate * sig
    slope = sig * (1.0 + pre_gate * (1.0 - sig))
    hidden = (activated * pre_up).astype(BF16).astype(F32)
    gg = jnp.sum(hidden * back_raw, axis=1, keepdims=True)
    scaled = gating * back_raw
    g_in = jnp.concatenate([scaled * pre_up * slope, scaled * activated], axis=1).astype(BF16)
    return g_in, (gating * hidden).astype(BF16), gg


def three_kernel(sc, pair, *refs):
    weights = refs[0:9]
    grads, back, gg_out, held, held_down, sems = refs[9:]
    copies = []
    for k in range(3):
        gate, up, down = weights[3 * k : 3 * k + 3]
        targets = (held.at[k, :, 0:FQ], held.at[k, :, FQ : 2 * FQ], held_down.at[k])
        copies.append(
            [
                pltpu.make_async_copy(x, t, sems.at[3 * k + c])
                for c, (x, t) in enumerate(zip((gate, up, down), targets))
            ]
        )
        for c in copies[k]:
            c.start()
    gg = None
    for k in range(3):
        for c in copies[k]:
            c.wait()
        g_in, scaled, part = hidden_grads(pair, held[k], held_down[k])
        term = dot(g_in, held[k], 1, 1)
        if k == 0:
            grads[:, 0 : 2 * FQ] = g_in
            grads[:, 2 * FQ :] = scaled
            gg = part
            back[...] = term
        else:
            gg = gg + part
            back[...] += term
    gg_out[...] = jnp.broadcast_to(gg, (128, 128))


def redo_kernel(sc, pair_1, pair_3, gate, up, down, out_1, out_3):
    both = jnp.concatenate([gate[...], up[...]], axis=1)
    for pair, out in ((pair_1, out_1), (pair_3, out_3)):
        g_in, scaled, _ = hidden_grads(pair, both, down[...])
        out[:, 0 : 2 * FQ] = g_in
        out[:, 2 * FQ :] = scaled


def emit_kernel(sc, pair, gate, up, down, back, gg_in, send, scratch):
    about = pair[:, 2 * D :].astype(F32)
    both = jnp.concatenate([gate[...], up[...]], axis=1)
    g_in, _, gg = hidden_grads(pair, both, down[...])
    term = back[...] + dot(g_in, both, 1, 1)
    gg = gg + gg_in[:, 0:1]
    own = (about[:, 3:4] + about[:, 4:5] + about[:, 5:6]) * gg
    other = (about[:, 6:7] + about[:, 7:8] + about[:, 8:9]) * gg
    other_expert = about[:, 9:10].astype(jnp.int32)
    lane = iota((128, EXPERTS), 1)
    mix = jnp.where(lane == sc[1], own, 0.0) - jnp.where(lane == other_expert, other, 0.0)
    mix_hi = mix.astype(BF16)
    mix_lo = (mix - mix_hi.astype(F32)).astype(BF16)
    router = dot(pair[:, 0:D], jnp.concatenate([mix_hi, mix_lo], axis=1), 0, 0)
    router = (router[:, 0:EXPERTS] + router[:, EXPERTS:]).reshape(128, 2, 8, EXPERTS)
    send[:, 0:CH] = spread(scratch, [term[:, CH * u : CH * (u + 1)] for u in range(8)])
    for h in range(2):
        send[:, CH + 128 * h : CH + 128 * (h + 1)] = router[:, h].reshape(SENT, EXPERTS).astype(BF16)
    tail = jnp.zeros((128, 128), F32)
    for c, v in enumerate(pieces(gg)):
        tail = jnp.where(lane == c, v, tail)
    send[:, 2 * CH :] = dot(every(), tail.astype(BF16)).astype(BF16)


def row_sums(x):
    n, width = x.shape
    acc = x[:, 0:128]
    for c in range(1, width // 128):
        acc = acc + x[:, 128 * c : 128 * (c + 1)]
    return jnp.concatenate(
        [jnp.sum(acc[128 * c : 128 * (c + 1), :].T, axis=0, keepdims=True) for c in range(n // 128)],
        axis=0,
    )


def sums_kernel(
    sc, pair, pair_1, top, bottom, pair_3, grads_0, grads_1, grads_3, gate_w, up_w, down_w, *outs
):
    gate, up, down, down_norms, norms = outs
    distant = jnp.concatenate([top[...], bottom[...]], axis=0)
    both = jnp.concatenate([gate_w[...], up_w[...]], axis=1)
    far_in, far_scaled, _ = hidden_grads(distant, both, down_w[...])
    pairs = (pair, pair_1, distant, pair_3)
    toks = jnp.concatenate([x[:, 0:D] for x in pairs], axis=0)
    cots = jnp.concatenate([x[:, D : 2 * D] for x in pairs], axis=0)
    at = slice(0, 2 * FQ)
    g_in = jnp.concatenate([grads_0[:, at], grads_1[:, at], far_in, grads_3[:, at]], axis=0)
    at = slice(2 * FQ, 3 * FQ)
    scaled = jnp.concatenate([grads_0[:, at], grads_1[:, at], far_scaled, grads_3[:, at]], axis=0)
    in_sums = dot(toks, g_in, 0, 0)
    gate[...] = in_sums[:, 0:FQ].astype(BF16)
    up[...] = in_sums[:, FQ:].astype(BF16)
    squares = in_sums * in_sums
    lines = []
    for x in (squares[:, 0:FQ], squares[:, FQ:]):
        hi, mid, lo = pieces(row_sums(x))
        lines += [hi, mid + lo]
    norms[...] = jnp.concatenate(lines, axis=1).astype(BF16)
    down_sum = dot(scaled, cots, 0, 0)
    down[...] = down_sum.astype(BF16)
    down_norms[...] = row_sums(down_sum * down_sum)


def home_kernel(sc, got, hit0, hit1, norms, out, scratch):
    fill(scratch, got)
    hits = [hit0[...], hit1[...]]
    both = (hits[0].astype(F32) + hits[1].astype(F32)).astype(BF16)
    lines = [gather(scratch, u) for u in range(8)]
    terms = jnp.concatenate([x[:, 0:CH] for x in lines], axis=1)
    summed = dot(both, terms, 0, 0).astype(BF16)
    tail = lines[0][:, 2 * CH :]
    pick = (iota((8, SENT), 0) == iota((8, SENT), 1) % 8).astype(BF16)
    router = dot(pick, got[:, CH : 2 * CH])
    hi, mid, lo = pieces(router)
    lines = [jnp.concatenate([hi, mid + lo], axis=1)]
    flat = []
    for hit in hits:
        flat.append(dot(tail, hit, 0, 0)[0:4, :])
    flat = jnp.concatenate(flat, axis=0)
    lines.append(jnp.concatenate([flat] * 4, axis=1))
    extra = jnp.concatenate(lines, axis=0).astype(BF16)
    for q in range(TP):
        out[q, 0:TOK, :] = summed[:, DQ * q : DQ * (q + 1)]
        out[q, TOK : TOK + 16, :] = extra
        out[q, TOK + 16 :, :] = norms[...]


def last_kernel(
    sc, got, stats, routing, router, grad_tokens, grad_gating, grad_router, norms, in_norms
):
    total = got[0].astype(F32)
    for q in range(1, TP):
        total = total + got[q].astype(F32)
    extra = total[TOK:, :]
    rows = [
        extra[8 + 4 * k : 9 + 4 * k, 0:128]
        + extra[9 + 4 * k : 10 + 4 * k, 0:128]
        + extra[10 + 4 * k : 11 + 4 * k, 0:128]
        for k in range(2)
    ]
    grad_gating[...] = jnp.concatenate(rows, axis=0)
    st = stats[...]
    score_sum = st[2:3, :]
    weighted = st[3:4, :] * rows[0] + st[4:5, :] * rows[1]
    experts = iota((EXPERTS, TOK), 0)
    logits = jnp.zeros((EXPERTS, TOK), F32)
    for k in range(2):
        s = st[k : k + 1, :]
        chosen = (rows[k] - weighted) / score_sum * s * (1.0 - s)
        logits = jnp.where(experts == routing[k : k + 1, :], chosen, logits)
    term = dot(logits.astype(BF16), router[...], 0, 1)
    grad_tokens[...] = (total[0:TOK, :] + term).astype(BF16)
    sums = extra[0:8, 0:256] + extra[0:8, 256:512]
    x = jnp.concatenate([sums[:, 0:128], sums[:, 128:256]], axis=0)
    grad_router[...] = x
    squares = lax.dot_general(
        jnp.ones((8, EXPERTS), F32),
        x * x,
        (((1,), (1,)), ((), ())),
        precision=lax.Precision.HIGHEST,
        preferred_element_type=F32,
    )
    norms[...] = squares[0:1, :]
    for k in range(2):
        sums = extra[16:32, 256 * k : 256 * k + 128] + extra[16:32, 256 * k + 128 : 256 * (k + 1)]
        for c in range(D // 128):
            in_norms[k : k + 1, 128 * c : 128 * (c + 1)] = sums[c : c + 1, :]


def layer(tokens, cotangent, routing, router_weight, gate_weight, up_weight, down_weight):
    tp_index = lax.axis_index("tp")
    ep_index = lax.axis_index(EP)
    sc = jnp.stack([tp_index, ep_index]).astype(jnp.int32)
    routing_t = routing.T
    gate_w = gate_weight[0]
    up_w = up_weight[0]
    down_w = down_weight[0]
    far = functools.partial(pltpu.with_memory_space_constraint, memory_space=pltpu.HBM)

    def shift(x, d):
        return lax.ppermute(x, "tp", [(a, (a + d) % TP) for a in range(TP)])

    gate_1 = shift(gate_w, 1)
    down_3 = shift(down_w, 3)
    up_1 = shift(up_w, 1)
    up_3 = shift(up_w, 3)
    gate_2 = shift(gate_1, 1)
    gate_3 = shift(gate_w, 3)
    down_1 = shift(down_w, 1)
    down_2 = shift(down_3, 3)
    up_2 = shift(up_1, 1)

    send, hit0, hit1, stats = call(
        dispatch_kernel,
        sc,
        (whole(far(tokens)), whole(far(cotangent)), whole(far(routing_t)), whole(far(router_weight))),
        (
            hbm((SENT, 2 * CH + 128), BF16),
            hbm((EXPERTS, TOK), BF16),
            hbm((EXPERTS, TOK), BF16),
            hbm((8, TOK), F32),
        ),
        (pltpu.VMEM((2 * CH // 128, SENT, 128), F32),),
    )
    got = lax.all_to_all(send.reshape(EXPERTS, 8, 2 * CH + 128), EP, 0, 0, tiled=True)
    (pair,) = call(
        rows_kernel,
        sc,
        (got.reshape(SENT, 2 * CH + 128),),
        (vmem((128, 2 * D + 128), BF16),),
        (pltpu.VMEM((2 * CH // 128 + 1, SENT, 128), F32),),
    )
    pair_1 = shift(pair, 1)
    pair_3 = shift(pair, 3)
    quarter_grads = hbm((128, 3 * FQ), BF16)
    in_place = pl.BlockSpec(memory_space=pltpu.HBM)
    weights = (gate_w, up_w, down_w, gate_3, up_3, down_3, gate_1, up_1, down_1)
    grads_0, back, gg = call(
        three_kernel,
        sc,
        (pair, *((far(x), in_place) for x in weights)),
        (quarter_grads, vmem((128, D), F32), vmem((128, 128), F32)),
        (
            pltpu.VMEM((3, D, 2 * FQ), BF16),
            pltpu.VMEM((3, FQ, D), BF16),
            pltpu.SemaphoreType.DMA((9,)),
        ),
    )
    (send_back,) = call(
        emit_kernel,
        sc,
        (pair, *(whole(far(x)) for x in (gate_2, up_2, down_2)), back, gg),
        (hbm((SENT, 2 * CH + 128), BF16),),
        (pltpu.VMEM((CH // 128, SENT, 128), F32),),
    )
    home = lax.all_to_all(send_back.reshape(EXPERTS, 8, 2 * CH + 128), EP, 0, 0, tiled=True)
    home = home.reshape(SENT, 2 * CH + 128)
    top = shift(pair_1[0:64], 1)
    bottom = shift(pair_3[64:], 3)
    own_weights = tuple(whole(far(x)) for x in (gate_w, up_w, down_w))
    grads_1, grads_3 = call(
        redo_kernel,
        sc,
        (*(whole(far(x)) for x in (pair_1, pair_3)), *own_weights),
        (quarter_grads,) * 2,
    )
    grad_gate, grad_up, grad_down, down_norms, norms = call(
        sums_kernel,
        sc,
        (
            *(whole(far(x)) for x in (pair, pair_1, top, bottom, pair_3, grads_0, grads_1, grads_3)),
            *own_weights,
        ),
        (
            sds((D, FQ), BF16),
            sds((D, FQ), BF16),
            sds((FQ, D), BF16),
            sds((1, FQ), F32),
            vmem((16, 4 * 128), BF16),
        ),
    )
    (parts,) = call(
        home_kernel,
        sc,
        (home, whole(hit0), whole(hit1), norms),
        (vmem((TP, TOK + 32, DQ), BF16),),
        (pltpu.VMEM((2 * CH // 128 + 1, SENT, 128), F32),),
    )
    parts = lax.all_to_all(parts, "tp", 0, 0, tiled=True)
    grad_tokens, grad_gating, grad_router, router_norms, in_norms = call(
        last_kernel,
        sc,
        (
            parts,
            whole(stats),
            whole(routing_t),
            (router_weight, pl.BlockSpec((DQ, 128), lambda g, p: (p[0], 0))),
        ),
        (
            sds((TOK, DQ), BF16),
            sds((2, TOK), F32),
            sds((16, EXPERTS), F32),
            sds((1, 16), F32),
            sds((2, D), F32),
        ),
    )
    return (
        grad_tokens,
        grad_gating.T,
        grad_router,
        grad_gate[None],
        grad_up[None],
        grad_down[None],
        in_norms[None],
        down_norms,
        router_norms[0],
    )


def solution(mesh):
    split = Mesh(mesh.devices.reshape(8, 8, 2, TP), ("ep_0", "ep_1", "ep_2", "tp"))
    in_specs = (
        P(EP, None),
        P(EP, None),
        P(EP, None),
        P(),
        P(EP, None, "tp"),
        P(EP, None, "tp"),
        P(EP, "tp", None),
    )
    out_specs = (
        P(EP, "tp"),
        P(EP, None),
        P(EP, None),
        P(EP, None, "tp"),
        P(EP, None, "tp"),
        P(EP, "tp", None),
        P(EP, None, None),
        P(EP, "tp"),
        P(EP),
    )
    return jax.shard_map(layer, mesh=split, in_specs=in_specs, out_specs=out_specs, check_vma=False)
```

```python
import functools

import jax
import jax.numpy as jnp
from jax import lax
from jax.experimental import pallas as pl
from jax.experimental.pallas import tpu as pltpu
from jax.sharding import Mesh
from jax.sharding import PartitionSpec as P


EP = ("ep_0", "ep_1", "ep_2")
F32 = jnp.float32
BF16 = jnp.bfloat16


TOK = 128
D = 2048
EXPERTS = 128
TP = 4
DQ = D // TP
F = 512
FQ = F // TP
SENT = EXPERTS * 8
CH = D // 8


def dot(a, b, ca=1, cb=0):
    return lax.dot_general(a, b, (((ca,), (cb,)), ((), ())), preferred_element_type=F32)


def iota(shape, dim):
    return lax.broadcasted_iota(jnp.int32, shape, dim)


def pieces(x):
    hi = x.astype(BF16).astype(F32)
    rest = x - hi
    mid = rest.astype(BF16).astype(F32)
    return hi, mid, rest - mid


def spread(scratch, chunks):
    width = scratch.shape[0]
    for u, chunk in enumerate(chunks):
        for c in range(width):
            scratch[c, pl.ds(u, 128, stride=8), :] = chunk[:, 128 * c : 128 * (c + 1)].astype(F32)
    return jnp.concatenate([scratch[c].astype(BF16) for c in range(width)], axis=1)


def fill(scratch, got):
    for c in range(scratch.shape[0]):
        scratch[c] = got[:, 128 * c : 128 * (c + 1)].astype(F32)


def gather(scratch, u):
    return jnp.concatenate(
        [scratch[c, pl.ds(u, 128, stride=8), :].astype(BF16) for c in range(scratch.shape[0])], axis=1
    )


def every():
    return (iota((SENT, 128), 0) // 8 == iota((SENT, 128), 1)).astype(BF16)


ON_CHIP = pl.BlockSpec(memory_space=pltpu.VMEM)


def call(kernel, scalars, ins, outs, scratch=()):
    arrays = []
    specs = []
    for x in ins:
        if isinstance(x, tuple):
            arrays.append(x[0])
            specs.append(x[1])
        else:
            arrays.append(pltpu.with_memory_space_constraint(x, pltpu.VMEM))
            specs.append(ON_CHIP)
    return pl.pallas_call(
        kernel,
        grid_spec=pltpu.PrefetchScalarGridSpec(
            num_scalar_prefetch=1,
            grid=(1,),
            in_specs=tuple(specs),
            out_specs=(ON_CHIP,) * len(outs),
            scratch_shapes=scratch,
        ),
        out_shape=tuple(outs),
        compiler_params=pltpu.CompilerParams(vmem_limit_bytes=32 << 20),
    )(scalars, *arrays)


def whole(x):
    return (x, pl.BlockSpec(x.shape, lambda g, p: (0,) * x.ndim))


def sds(shape, dtype):
    return jax.ShapeDtypeStruct(shape, dtype)


def hbm(shape, dtype):
    return pltpu.HBM(shape, dtype)


def vmem(shape, dtype):
    return pltpu.VMEM(shape, dtype)


def dispatch_kernel(sc, tok, cot, routing, router, send, hit0, hit1, stats, scratch):
    experts = iota((EXPERTS, TOK), 0)
    picked = [(experts == routing[k : k + 1, :]) for k in range(2)]
    both = (picked[0] | picked[1]).astype(F32)
    logits = dot(tok[...], router[...]).T
    s = [
        jax.nn.sigmoid(jnp.sum(jnp.where(m, logits, 0.0), axis=0, keepdims=True)) for m in picked
    ]
    total = s[0] + s[1]
    g = [v / total for v in s]
    slope = [v * (1.0 - v) / total for v in s]
    before = (iota((TOK, TOK), 0) < iota((TOK, TOK), 1)).astype(BF16)
    within = dot(both.astype(BF16), before)
    mine = within == sc[0].astype(F32)
    line = iota((128, TOK), 0)
    hits = []
    info = None
    for k, out in ((0, hit0), (1, hit1)):
        hit = jnp.where(picked[k] & mine, 1.0, 0.0)
        out[...] = hit.astype(BF16)
        hits.append(hit)
        own = slope[k] * g[1 - k]
        other = slope[1 - k] * g[k]
        columns = [*pieces(g[k]), *pieces(own), *pieces(other), routing[1 - k : 2 - k, :].astype(F32)]
        table = jnp.zeros((128, TOK), F32)
        for c, v in enumerate(columns):
            table = jnp.where(line == c, v, table)
        part = dot(hit.astype(BF16), table.astype(BF16), 1, 1)
        info = part if info is None else info + part
    any_hit = (hits[0] + hits[1]).astype(BF16)
    toks = dot(any_hit, tok[...])
    cots = dot(any_hit, cot[...])
    send[:, 0 : 2 * CH] = spread(
        scratch,
        [
            jnp.concatenate([x[:, CH * u : CH * (u + 1)] for x in (toks, cots)], axis=1)
            for u in range(8)
        ],
    )
    send[:, 2 * CH :] = dot(every(), info.astype(BF16)).astype(BF16)
    stats[...] = jnp.concatenate(
        [s[0], s[1], total, g[0], g[1], total, total, total], axis=0
    )


def rows_kernel(sc, got, pair, scratch):
    fill(scratch, got)
    for u in range(8):
        part = gather(scratch, u)
        pair[:, CH * u : CH * (u + 1)] = part[:, 0:CH]
        pair[:, D + CH * u : D + CH * (u + 1)] = part[:, CH : 2 * CH]
        if u == 0:
            pair[:, 2 * D :] = part[:, 2 * CH :]


def hidden_grads(pair, both, down, pre=None):
    if pre is None:
        pre = dot(pair[:, 0:D], both)
    back_raw = dot(pair[:, D : 2 * D], down, 1, 1)
    about = pair[:, 2 * D :].astype(F32)
    pre_gate = pre[:, 0:FQ]
    pre_up = pre[:, FQ:]
    gating = about[:, 0:1] + about[:, 1:2] + about[:, 2:3]
    sig = jax.nn.sigmoid(pre_gate)
    activated = pre_gate * sig
    slope = sig * (1.0 + pre_gate * (1.0 - sig))
    hidden = (activated * pre_up).astype(BF16).astype(F32)
    gg = jnp.sum(hidden * back_raw, axis=1, keepdims=True)
    scaled = gating * back_raw
    g_in = jnp.concatenate([scaled * pre_up * slope, scaled * activated], axis=1).astype(BF16)
    return g_in, (gating * hidden).astype(BF16), gg


def three_kernel(sc, pair, *refs):
    weights = refs[0:9]
    grads, back, gg_out, held, held_down, sems = refs[9:]
    copies = []
    for k in range(3):
        gate, up, down = weights[3 * k : 3 * k + 3]
        targets = (held.at[k, :, 0:FQ], held.at[k, :, FQ : 2 * FQ], held_down.at[k])
        copies.append(
            [
                pltpu.make_async_copy(x, t, sems.at[3 * k + c])
                for c, (x, t) in enumerate(zip((gate, up, down), targets))
            ]
        )
        for c in copies[k]:
            c.start()
    gg = None
    for k in range(3):
        for c in copies[k]:
            c.wait()
        g_in, scaled, part = hidden_grads(pair, held[k], held_down[k])
        term = dot(g_in, held[k], 1, 1)
        if k == 0:
            grads[:, 0 : 2 * FQ] = g_in
            grads[:, 2 * FQ :] = scaled
            gg = part
            back[...] = term
        else:
            gg = gg + part
            back[...] += term
    gg_out[...] = jnp.broadcast_to(gg, (128, 128))


def redo_kernel(sc, pair_1, pair_3, gate, up, down, out_1, out_3):
    both = jnp.concatenate([gate[...], up[...]], axis=1)
    for pair, out in ((pair_1, out_1), (pair_3, out_3)):
        g_in, scaled, _ = hidden_grads(pair, both, down[...])
        out[:, 0 : 2 * FQ] = g_in
        out[:, 2 * FQ :] = scaled


def emit_kernel(
    sc, pair, gate, up, down, back, gg_in, send, scratch, held, held_down, sems
):
    copies = [
        pltpu.make_async_copy(x, t, sems.at[c])
        for c, (x, t) in enumerate(
            ((gate, held.at[:, 0:FQ]), (up, held.at[:, FQ : 2 * FQ]), (down, held_down))
        )
    ]
    for c in copies:
        c.start()
    about = pair[:, 2 * D :].astype(F32)
    for c in copies[0:2]:
        c.wait()
    pre = dot(pair[:, 0:D], held[...])
    copies[2].wait()
    g_in, _, gg = hidden_grads(pair, held[...], held_down[...], pre)
    term = back[...] + dot(g_in, held[...], 1, 1)
    gg = gg + gg_in[:, 0:1]
    own = (about[:, 3:4] + about[:, 4:5] + about[:, 5:6]) * gg
    other = (about[:, 6:7] + about[:, 7:8] + about[:, 8:9]) * gg
    other_expert = about[:, 9:10].astype(jnp.int32)
    lane = iota((128, EXPERTS), 1)
    mix = jnp.where(lane == sc[1], own, 0.0) - jnp.where(lane == other_expert, other, 0.0)
    mix_hi = mix.astype(BF16)
    mix_lo = (mix - mix_hi.astype(F32)).astype(BF16)
    router = dot(pair[:, 0:D], jnp.concatenate([mix_hi, mix_lo], axis=1), 0, 0)
    router = (router[:, 0:EXPERTS] + router[:, EXPERTS:]).reshape(128, 2, 8, EXPERTS)
    send[:, 0:CH] = spread(scratch, [term[:, CH * u : CH * (u + 1)] for u in range(8)])
    for h in range(2):
        send[:, CH + 128 * h : CH + 128 * (h + 1)] = router[:, h].reshape(SENT, EXPERTS).astype(BF16)
    tail = jnp.zeros((128, 128), F32)
    for c, v in enumerate(pieces(gg)):
        tail = jnp.where(lane == c, v, tail)
    send[:, 2 * CH :] = dot(every(), tail.astype(BF16)).astype(BF16)


def row_sums(x):
    n, width = x.shape
    acc = x[:, 0:128]
    for c in range(1, width // 128):
        acc = acc + x[:, 128 * c : 128 * (c + 1)]
    return jnp.concatenate(
        [jnp.sum(acc[128 * c : 128 * (c + 1), :].T, axis=0, keepdims=True) for c in range(n // 128)],
        axis=0,
    )


def sums_kernel(
    sc, pair, pair_1, top, bottom, pair_3, grads_0, grads_1, grads_3, gate_w, up_w, down_w, *outs
):
    gate, up, down, down_norms, norms = outs
    distant = jnp.concatenate([top[...], bottom[...]], axis=0)
    both = jnp.concatenate([gate_w[...], up_w[...]], axis=1)
    far_in, far_scaled, _ = hidden_grads(distant, both, down_w[...])
    pairs = (pair, pair_1, distant, pair_3)
    toks = jnp.concatenate([x[:, 0:D] for x in pairs], axis=0)
    cots = jnp.concatenate([x[:, D : 2 * D] for x in pairs], axis=0)
    at = slice(0, 2 * FQ)
    g_in = jnp.concatenate([grads_0[:, at], grads_1[:, at], far_in, grads_3[:, at]], axis=0)
    at = slice(2 * FQ, 3 * FQ)
    scaled = jnp.concatenate([grads_0[:, at], grads_1[:, at], far_scaled, grads_3[:, at]], axis=0)
    in_sums = dot(toks, g_in, 0, 0)
    gate[...] = in_sums[:, 0:FQ].astype(BF16)
    up[...] = in_sums[:, FQ:].astype(BF16)
    squares = in_sums * in_sums
    lines = []
    for x in (squares[:, 0:FQ], squares[:, FQ:]):
        hi, mid, lo = pieces(row_sums(x))
        lines += [hi, mid + lo]
    norms[...] = jnp.concatenate(lines, axis=1).astype(BF16)
    down_sum = dot(scaled, cots, 0, 0)
    down[...] = down_sum.astype(BF16)
    down_norms[...] = row_sums(down_sum * down_sum)


def home_kernel(sc, got, hit0, hit1, norms, out, scratch):
    fill(scratch, got)
    hits = [hit0[...], hit1[...]]
    both = (hits[0].astype(F32) + hits[1].astype(F32)).astype(BF16)
    lines = [gather(scratch, u) for u in range(8)]
    terms = jnp.concatenate([x[:, 0:CH] for x in lines], axis=1)
    summed = dot(both, terms, 0, 0).astype(BF16)
    tail = lines[0][:, 2 * CH :]
    pick = (iota((8, SENT), 0) == iota((8, SENT), 1) % 8).astype(BF16)
    router = dot(pick, got[:, CH : 2 * CH])
    hi, mid, lo = pieces(router)
    lines = [jnp.concatenate([hi, mid + lo], axis=1)]
    flat = []
    for hit in hits:
        flat.append(dot(tail, hit, 0, 0)[0:4, :])
    flat = jnp.concatenate(flat, axis=0)
    lines.append(jnp.concatenate([flat] * 4, axis=1))
    extra = jnp.concatenate(lines, axis=0).astype(BF16)
    for q in range(TP):
        out[q, 0:TOK, :] = summed[:, DQ * q : DQ * (q + 1)]
        out[q, TOK : TOK + 16, :] = extra
        out[q, TOK + 16 :, :] = norms[...]


def last_kernel(
    sc, got, stats, routing, router, grad_tokens, grad_gating, grad_router, norms, in_norms
):
    total = got[0].astype(F32)
    for q in range(1, TP):
        total = total + got[q].astype(F32)
    extra = total[TOK:, :]
    rows = [
        extra[8 + 4 * k : 9 + 4 * k, 0:128]
        + extra[9 + 4 * k : 10 + 4 * k, 0:128]
        + extra[10 + 4 * k : 11 + 4 * k, 0:128]
        for k in range(2)
    ]
    grad_gating[...] = jnp.concatenate(rows, axis=0)
    st = stats[...]
    score_sum = st[2:3, :]
    weighted = st[3:4, :] * rows[0] + st[4:5, :] * rows[1]
    experts = iota((EXPERTS, TOK), 0)
    logits = jnp.zeros((EXPERTS, TOK), F32)
    for k in range(2):
        s = st[k : k + 1, :]
        chosen = (rows[k] - weighted) / score_sum * s * (1.0 - s)
        logits = jnp.where(experts == routing[k : k + 1, :], chosen, logits)
    term = dot(logits.astype(BF16), router[...], 0, 1)
    grad_tokens[...] = (total[0:TOK, :] + term).astype(BF16)
    sums = extra[0:8, 0:256] + extra[0:8, 256:512]
    x = jnp.concatenate([sums[:, 0:128], sums[:, 128:256]], axis=0)
    grad_router[...] = x
    squares = lax.dot_general(
        jnp.ones((8, EXPERTS), F32),
        x * x,
        (((1,), (1,)), ((), ())),
        precision=lax.Precision.HIGHEST,
        preferred_element_type=F32,
    )
    norms[...] = squares[0:1, :]
    for k in range(2):
        sums = extra[16:32, 256 * k : 256 * k + 128] + extra[16:32, 256 * k + 128 : 256 * (k + 1)]
        for c in range(D // 128):
            in_norms[k : k + 1, 128 * c : 128 * (c + 1)] = sums[c : c + 1, :]


def layer(tokens, cotangent, routing, router_weight, gate_weight, up_weight, down_weight):
    tp_index = lax.axis_index("tp")
    ep_index = lax.axis_index(EP)
    sc = jnp.stack([tp_index, ep_index]).astype(jnp.int32)
    routing_t = routing.T
    gate_w = gate_weight[0]
    up_w = up_weight[0]
    down_w = down_weight[0]
    far = functools.partial(pltpu.with_memory_space_constraint, memory_space=pltpu.HBM)

    def shift(x, d):
        return lax.ppermute(x, "tp", [(a, (a + d) % TP) for a in range(TP)])

    gate_1 = shift(gate_w, 1)
    down_3 = shift(down_w, 3)
    up_1 = shift(up_w, 1)
    gate_2 = shift(gate_1, 1)
    up_3 = shift(up_w, 3)
    down_1 = shift(down_w, 1)
    gate_3 = shift(gate_w, 3)
    up_2 = shift(up_1, 1)
    down_2 = shift(down_3, 3)

    send, hit0, hit1, stats = call(
        dispatch_kernel,
        sc,
        (whole(far(tokens)), whole(far(cotangent)), whole(far(routing_t)), whole(far(router_weight))),
        (
            hbm((SENT, 2 * CH + 128), BF16),
            hbm((EXPERTS, TOK), BF16),
            hbm((EXPERTS, TOK), BF16),
            hbm((8, TOK), F32),
        ),
        (pltpu.VMEM((2 * CH // 128, SENT, 128), F32),),
    )
    got = lax.all_to_all(send.reshape(EXPERTS, 8, 2 * CH + 128), EP, 0, 0, tiled=True)
    (pair,) = call(
        rows_kernel,
        sc,
        (got.reshape(SENT, 2 * CH + 128),),
        (vmem((128, 2 * D + 128), BF16),),
        (pltpu.VMEM((2 * CH // 128 + 1, SENT, 128), F32),),
    )
    pair_1 = shift(pair, 1)
    pair_3 = shift(pair, 3)
    quarter_grads = hbm((128, 3 * FQ), BF16)
    in_place = pl.BlockSpec(memory_space=pltpu.HBM)
    weights = (gate_w, up_w, down_w, gate_3, up_3, down_3, gate_1, up_1, down_1)
    grads_0, back, gg = call(
        three_kernel,
        sc,
        (pair, *((far(x), in_place) for x in weights)),
        (quarter_grads, vmem((128, D), F32), vmem((128, 128), F32)),
        (
            pltpu.VMEM((3, D, 2 * FQ), BF16),
            pltpu.VMEM((3, FQ, D), BF16),
            pltpu.SemaphoreType.DMA((9,)),
        ),
    )
    (send_back,) = call(
        emit_kernel,
        sc,
        (pair, *((far(x), in_place) for x in (gate_2, up_2, down_2)), back, gg),
        (hbm((SENT, 2 * CH + 128), BF16),),
        (
            pltpu.VMEM((CH // 128, SENT, 128), F32),
            pltpu.VMEM((D, 2 * FQ), BF16),
            pltpu.VMEM((FQ, D), BF16),
            pltpu.SemaphoreType.DMA((3,)),
        ),
    )
    home = lax.all_to_all(send_back.reshape(EXPERTS, 8, 2 * CH + 128), EP, 0, 0, tiled=True)
    home = home.reshape(SENT, 2 * CH + 128)
    top = shift(pair_1[0:64], 1)
    bottom = shift(pair_3[64:], 3)
    own_weights = tuple(whole(far(x)) for x in (gate_w, up_w, down_w))
    grads_1, grads_3 = call(
        redo_kernel,
        sc,
        (*(whole(far(x)) for x in (pair_1, pair_3)), *own_weights),
        (quarter_grads,) * 2,
    )
    grad_gate, grad_up, grad_down, down_norms, norms = call(
        sums_kernel,
        sc,
        (
            *(whole(far(x)) for x in (pair, pair_1, top, bottom, pair_3, grads_0, grads_1, grads_3)),
            *own_weights,
        ),
        (
            sds((D, FQ), BF16),
            sds((D, FQ), BF16),
            sds((FQ, D), BF16),
            sds((1, FQ), F32),
            vmem((16, 4 * 128), BF16),
        ),
    )
    (parts,) = call(
        home_kernel,
        sc,
        (home, whole(hit0), whole(hit1), norms),
        (vmem((TP, TOK + 32, DQ), BF16),),
        (pltpu.VMEM((2 * CH // 128 + 1, SENT, 128), F32),),
    )
    parts = lax.all_to_all(parts, "tp", 0, 0, tiled=True)
    grad_tokens, grad_gating, grad_router, router_norms, in_norms = call(
        last_kernel,
        sc,
        (
            parts,
            whole(stats),
            whole(routing_t),
            (router_weight, pl.BlockSpec((DQ, 128), lambda g, p: (p[0], 0))),
        ),
        (
            sds((TOK, DQ), BF16),
            sds((2, TOK), F32),
            sds((16, EXPERTS), F32),
            sds((1, 16), F32),
            sds((2, D), F32),
        ),
    )
    return (
        grad_tokens,
        grad_gating.T,
        grad_router,
        grad_gate[None],
        grad_up[None],
        grad_down[None],
        in_norms[None],
        down_norms,
        router_norms[0],
    )


def solution(mesh):
    split = Mesh(mesh.devices.reshape(8, 8, 2, TP), ("ep_0", "ep_1", "ep_2", "tp"))
    in_specs = (
        P(EP, None),
        P(EP, None),
        P(EP, None),
        P(),
        P(EP, None, "tp"),
        P(EP, None, "tp"),
        P(EP, "tp", None),
    )
    out_specs = (
        P(EP, "tp"),
        P(EP, None),
        P(EP, None),
        P(EP, None, "tp"),
        P(EP, None, "tp"),
        P(EP, "tp", None),
        P(EP, None, None),
        P(EP, "tp"),
        P(EP),
    )
    return jax.shard_map(layer, mesh=split, in_specs=in_specs, out_specs=out_specs, check_vma=False)
```

```python
import functools

import jax
import jax.numpy as jnp
from jax import lax
from jax.experimental import pallas as pl
from jax.experimental.pallas import tpu as pltpu
from jax.sharding import Mesh
from jax.sharding import PartitionSpec as P


EP = ("ep_0", "ep_1", "ep_2")
F32 = jnp.float32
BF16 = jnp.bfloat16


TOK = 128
D = 2048
EXPERTS = 128
TP = 4
DQ = D // TP
F = 512
FQ = F // TP
SENT = EXPERTS * 8
CH = D // 8


def dot(a, b, ca=1, cb=0):
    return lax.dot_general(a, b, (((ca,), (cb,)), ((), ())), preferred_element_type=F32)


def iota(shape, dim):
    return lax.broadcasted_iota(jnp.int32, shape, dim)


def pieces(x):
    hi = x.astype(BF16).astype(F32)
    rest = x - hi
    mid = rest.astype(BF16).astype(F32)
    return hi, mid, rest - mid


def spread(scratch, chunks):
    width = scratch.shape[0]
    for u, chunk in enumerate(chunks):
        for c in range(width):
            scratch[c, pl.ds(u, 128, stride=8), :] = chunk[:, 128 * c : 128 * (c + 1)].astype(F32)
    return jnp.concatenate([scratch[c].astype(BF16) for c in range(width)], axis=1)


def fill(scratch, got):
    for c in range(scratch.shape[0]):
        scratch[c] = got[:, 128 * c : 128 * (c + 1)].astype(F32)


def gather(scratch, u):
    return jnp.concatenate(
        [scratch[c, pl.ds(u, 128, stride=8), :].astype(BF16) for c in range(scratch.shape[0])], axis=1
    )


ON_CHIP = pl.BlockSpec(memory_space=pltpu.VMEM)


def call(kernel, scalars, ins, outs, scratch=()):
    arrays = []
    specs = []
    for x in ins:
        if isinstance(x, tuple):
            arrays.append(x[0])
            specs.append(x[1])
        else:
            arrays.append(pltpu.with_memory_space_constraint(x, pltpu.VMEM))
            specs.append(ON_CHIP)
    return pl.pallas_call(
        kernel,
        grid_spec=pltpu.PrefetchScalarGridSpec(
            num_scalar_prefetch=1,
            grid=(1,),
            in_specs=tuple(specs),
            out_specs=(ON_CHIP,) * len(outs),
            scratch_shapes=scratch,
        ),
        out_shape=tuple(outs),
        compiler_params=pltpu.CompilerParams(vmem_limit_bytes=32 << 20),
    )(scalars, *arrays)


def whole(x):
    return (x, pl.BlockSpec(x.shape, lambda g, p: (0,) * x.ndim))


def sds(shape, dtype):
    return jax.ShapeDtypeStruct(shape, dtype)


def hbm(shape, dtype):
    return pltpu.HBM(shape, dtype)


def vmem(shape, dtype):
    return pltpu.VMEM(shape, dtype)


def dispatch_kernel(sc, tok, cot, routing, router, send, hit0, hit1, stats, scratch):
    experts = iota((EXPERTS, TOK), 0)
    picked = [(experts == routing[k : k + 1, :]) for k in range(2)]
    both = (picked[0] | picked[1]).astype(F32)
    logits = dot(tok[...], router[...]).T
    s = [
        jax.nn.sigmoid(jnp.sum(jnp.where(m, logits, 0.0), axis=0, keepdims=True)) for m in picked
    ]
    total = s[0] + s[1]
    g = [v / total for v in s]
    slope = [v * (1.0 - v) / total for v in s]
    before = (iota((TOK, TOK), 0) < iota((TOK, TOK), 1)).astype(BF16)
    within = dot(both.astype(BF16), before)
    mine = within == sc[0].astype(F32)
    line = iota((128, TOK), 0)
    hits = []
    info = None
    for k, out in ((0, hit0), (1, hit1)):
        hit = jnp.where(picked[k] & mine, 1.0, 0.0)
        out[...] = hit.astype(BF16)
        hits.append(hit)
        own = slope[k] * g[1 - k]
        other = slope[1 - k] * g[k]
        columns = [*pieces(g[k]), *pieces(own), *pieces(other), routing[1 - k : 2 - k, :].astype(F32)]
        table = jnp.zeros((128, TOK), F32)
        for c, v in enumerate(columns):
            table = jnp.where(line == c, v, table)
        part = dot(hit.astype(BF16), table.astype(BF16), 1, 1)
        info = part if info is None else info + part
    any_hit = (hits[0] + hits[1]).astype(BF16)
    toks = dot(any_hit, tok[...])
    cots = dot(any_hit, cot[...])
    send[...] = spread(
        scratch,
        [
            jnp.concatenate([*(x[:, CH * u : CH * (u + 1)] for x in (toks, cots)), info], axis=1)
            for u in range(8)
        ],
    )
    stats[...] = jnp.concatenate(
        [s[0], s[1], total, g[0], g[1], total, total, total], axis=0
    )


def rows_kernel(sc, got, pair, scratch):
    fill(scratch, got)
    for u in range(8):
        part = gather(scratch, u)
        pair[:, CH * u : CH * (u + 1)] = part[:, 0:CH]
        pair[:, D + CH * u : D + CH * (u + 1)] = part[:, CH : 2 * CH]
        if u == 0:
            pair[:, 2 * D :] = part[:, 2 * CH :]


def hidden_grads(pair, both, down, pre=None):
    if pre is None:
        pre = dot(pair[:, 0:D], both)
    back_raw = dot(pair[:, D : 2 * D], down, 1, 1)
    about = pair[:, 2 * D :].astype(F32)
    pre_gate = pre[:, 0:FQ]
    pre_up = pre[:, FQ:]
    gating = about[:, 0:1] + about[:, 1:2] + about[:, 2:3]
    sig = jax.nn.sigmoid(pre_gate)
    activated = pre_gate * sig
    slope = sig * (1.0 + pre_gate * (1.0 - sig))
    hidden = (activated * pre_up).astype(BF16).astype(F32)
    gg = jnp.sum(hidden * back_raw, axis=1, keepdims=True)
    scaled = gating * back_raw
    g_in = jnp.concatenate([scaled * pre_up * slope, scaled * activated], axis=1).astype(BF16)
    return g_in, (gating * hidden).astype(BF16), gg


def three_kernel(sc, pair, *refs):
    weights = refs[0:9]
    grads, back, gg_out, held, held_down, sems = refs[9:]
    copies = []
    for k in range(3):
        gate, up, down = weights[3 * k : 3 * k + 3]
        targets = (held.at[k, :, 0:FQ], held.at[k, :, FQ : 2 * FQ], held_down.at[k])
        copies.append(
            [
                pltpu.make_async_copy(x, t, sems.at[3 * k + c])
                for c, (x, t) in enumerate(zip((gate, up, down), targets))
            ]
        )
        for c in copies[k]:
            c.start()
    gg = None
    for k in range(3):
        for c in copies[k]:
            c.wait()
        g_in, scaled, part = hidden_grads(pair, held[k], held_down[k])
        term = dot(g_in, held[k], 1, 1)
        if k == 0:
            grads[:, 0 : 2 * FQ] = g_in
            grads[:, 2 * FQ :] = scaled
            gg = part
            back[...] = term
        else:
            gg = gg + part
            back[...] += term
    gg_out[...] = jnp.broadcast_to(gg, (128, 128))


def redo_kernel(sc, pair_1, pair_3, gate, up, down, out_1, out_3):
    both = jnp.concatenate([gate[...], up[...]], axis=1)
    for pair, out in ((pair_1, out_1), (pair_3, out_3)):
        g_in, scaled, _ = hidden_grads(pair, both, down[...])
        out[:, 0 : 2 * FQ] = g_in
        out[:, 2 * FQ :] = scaled


def emit_kernel(
    sc, pair, gate, up, down, back, gg_in, send, scratch, held, held_down, sems
):
    copies = [
        pltpu.make_async_copy(x, t, sems.at[c])
        for c, (x, t) in enumerate(
            ((gate, held.at[:, 0:FQ]), (up, held.at[:, FQ : 2 * FQ]), (down, held_down))
        )
    ]
    for c in copies:
        c.start()
    about = pair[:, 2 * D :].astype(F32)
    for c in copies[0:2]:
        c.wait()
    pre = dot(pair[:, 0:D], held[...])
    copies[2].wait()
    g_in, _, gg = hidden_grads(pair, held[...], held_down[...], pre)
    term = back[...] + dot(g_in, held[...], 1, 1)
    gg = gg + gg_in[:, 0:1]
    own = (about[:, 3:4] + about[:, 4:5] + about[:, 5:6]) * gg
    other = (about[:, 6:7] + about[:, 7:8] + about[:, 8:9]) * gg
    other_expert = about[:, 9:10].astype(jnp.int32)
    lane = iota((128, EXPERTS), 1)
    mix = jnp.where(lane == sc[1], own, 0.0) - jnp.where(lane == other_expert, other, 0.0)
    mix_hi = mix.astype(BF16)
    mix_lo = (mix - mix_hi.astype(F32)).astype(BF16)
    router = dot(pair[:, 0:D], jnp.concatenate([mix_hi, mix_lo], axis=1), 0, 0)
    router = (router[:, 0:EXPERTS] + router[:, EXPERTS:]).reshape(128, 2, 8, EXPERTS)
    for h in range(2):
        send[:, CH + 128 * h : CH + 128 * (h + 1)] = router[:, h].reshape(SENT, EXPERTS).astype(BF16)
    tail = jnp.zeros((128, 128), F32)
    for c, v in enumerate(pieces(gg)):
        tail = jnp.where(lane == c, v, tail)
    rows = spread(
        scratch,
        [jnp.concatenate([term[:, CH * u : CH * (u + 1)], tail], axis=1) for u in range(8)],
    )
    send[:, 0:CH] = rows[:, 0:CH]
    send[:, 2 * CH :] = rows[:, CH:]


def row_sums(x):
    n, width = x.shape
    acc = x[:, 0:128]
    for c in range(1, width // 128):
        acc = acc + x[:, 128 * c : 128 * (c + 1)]
    return jnp.concatenate(
        [jnp.sum(acc[128 * c : 128 * (c + 1), :].T, axis=0, keepdims=True) for c in range(n // 128)],
        axis=0,
    )


def sums_kernel(
    sc, pair, pair_1, top, bottom, pair_3, grads_0, grads_1, grads_3, gate_w, up_w, down_w, *outs
):
    gate, up, down, down_norms, norms = outs
    distant = jnp.concatenate([top[...], bottom[...]], axis=0)
    both = jnp.concatenate([gate_w[...], up_w[...]], axis=1)
    far_in, far_scaled, _ = hidden_grads(distant, both, down_w[...])
    pairs = (pair, pair_1, distant, pair_3)
    toks = jnp.concatenate([x[:, 0:D] for x in pairs], axis=0)
    cots = jnp.concatenate([x[:, D : 2 * D] for x in pairs], axis=0)
    at = slice(0, 2 * FQ)
    g_in = jnp.concatenate([grads_0[:, at], grads_1[:, at], far_in, grads_3[:, at]], axis=0)
    at = slice(2 * FQ, 3 * FQ)
    scaled = jnp.concatenate([grads_0[:, at], grads_1[:, at], far_scaled, grads_3[:, at]], axis=0)
    in_sums = dot(toks, g_in, 0, 0)
    gate[...] = in_sums[:, 0:FQ].astype(BF16)
    up[...] = in_sums[:, FQ:].astype(BF16)
    squares = in_sums * in_sums
    lines = []
    for x in (squares[:, 0:FQ], squares[:, FQ:]):
        hi, mid, lo = pieces(row_sums(x))
        lines += [hi, mid + lo]
    norms[...] = jnp.concatenate(lines, axis=1).astype(BF16)
    down_sum = dot(scaled, cots, 0, 0)
    down[...] = down_sum.astype(BF16)
    down_norms[...] = row_sums(down_sum * down_sum)


def home_kernel(sc, got, hit0, hit1, norms, out, scratch):
    fill(scratch, got)
    hits = [hit0[...], hit1[...]]
    both = (hits[0].astype(F32) + hits[1].astype(F32)).astype(BF16)
    lines = [gather(scratch, u) for u in range(8)]
    terms = jnp.concatenate([x[:, 0:CH] for x in lines], axis=1)
    summed = dot(both, terms, 0, 0).astype(BF16)
    tail = lines[0][:, 2 * CH :]
    pick = (iota((8, SENT), 0) == iota((8, SENT), 1) % 8).astype(BF16)
    router = dot(pick, got[:, CH : 2 * CH])
    hi, mid, lo = pieces(router)
    lines = [jnp.concatenate([hi, mid + lo], axis=1)]
    flat = []
    for hit in hits:
        flat.append(dot(tail, hit, 0, 0)[0:4, :])
    flat = jnp.concatenate(flat, axis=0)
    lines.append(jnp.concatenate([flat] * 4, axis=1))
    extra = jnp.concatenate(lines, axis=0).astype(BF16)
    for q in range(TP):
        out[q, 0:TOK, :] = summed[:, DQ * q : DQ * (q + 1)]
        out[q, TOK : TOK + 16, :] = extra
        out[q, TOK + 16 :, :] = norms[...]


def last_kernel(
    sc, got, stats, routing, router, grad_tokens, grad_gating, grad_router, norms, in_norms
):
    total = got[0].astype(F32)
    for q in range(1, TP):
        total = total + got[q].astype(F32)
    extra = total[TOK:, :]
    rows = [
        extra[8 + 4 * k : 9 + 4 * k, 0:128]
        + extra[9 + 4 * k : 10 + 4 * k, 0:128]
        + extra[10 + 4 * k : 11 + 4 * k, 0:128]
        for k in range(2)
    ]
    grad_gating[...] = jnp.concatenate(rows, axis=0)
    st = stats[...]
    score_sum = st[2:3, :]
    weighted = st[3:4, :] * rows[0] + st[4:5, :] * rows[1]
    experts = iota((EXPERTS, TOK), 0)
    logits = jnp.zeros((EXPERTS, TOK), F32)
    for k in range(2):
        s = st[k : k + 1, :]
        chosen = (rows[k] - weighted) / score_sum * s * (1.0 - s)
        logits = jnp.where(experts == routing[k : k + 1, :], chosen, logits)
    term = dot(logits.astype(BF16), router[...], 0, 1)
    grad_tokens[...] = (total[0:TOK, :] + term).astype(BF16)
    sums = extra[0:8, 0:256] + extra[0:8, 256:512]
    x = jnp.concatenate([sums[:, 0:128], sums[:, 128:256]], axis=0)
    grad_router[...] = x
    squares = lax.dot_general(
        jnp.ones((8, EXPERTS), F32),
        x * x,
        (((1,), (1,)), ((), ())),
        precision=lax.Precision.HIGHEST,
        preferred_element_type=F32,
    )
    norms[...] = squares[0:1, :]
    for k in range(2):
        sums = extra[16:32, 256 * k : 256 * k + 128] + extra[16:32, 256 * k + 128 : 256 * (k + 1)]
        for c in range(D // 128):
            in_norms[k : k + 1, 128 * c : 128 * (c + 1)] = sums[c : c + 1, :]


def layer(tokens, cotangent, routing, router_weight, gate_weight, up_weight, down_weight):
    tp_index = lax.axis_index("tp")
    ep_index = lax.axis_index(EP)
    sc = jnp.stack([tp_index, ep_index]).astype(jnp.int32)
    routing_t = routing.T
    gate_w = gate_weight[0]
    up_w = up_weight[0]
    down_w = down_weight[0]
    far = functools.partial(pltpu.with_memory_space_constraint, memory_space=pltpu.HBM)

    def shift(x, d):
        return lax.ppermute(x, "tp", [(a, (a + d) % TP) for a in range(TP)])

    gate_1 = shift(gate_w, 1)
    down_3 = shift(down_w, 3)
    up_1 = shift(up_w, 1)
    gate_2 = shift(gate_1, 1)
    up_3 = shift(up_w, 3)
    down_1 = shift(down_w, 1)
    gate_3 = shift(gate_w, 3)
    up_2 = shift(up_1, 1)
    down_2 = shift(down_3, 3)

    send, hit0, hit1, stats = call(
        dispatch_kernel,
        sc,
        (whole(far(tokens)), whole(far(cotangent)), whole(far(routing_t)), whole(far(router_weight))),
        (
            hbm((SENT, 2 * CH + 128), BF16),
            hbm((EXPERTS, TOK), BF16),
            hbm((EXPERTS, TOK), BF16),
            hbm((8, TOK), F32),
        ),
        (pltpu.VMEM((2 * CH // 128 + 1, SENT, 128), F32),),
    )
    got = lax.all_to_all(send.reshape(EXPERTS, 8, 2 * CH + 128), EP, 0, 0, tiled=True)
    (pair,) = call(
        rows_kernel,
        sc,
        (got.reshape(SENT, 2 * CH + 128),),
        (vmem((128, 2 * D + 128), BF16),),
        (pltpu.VMEM((2 * CH // 128 + 1, SENT, 128), F32),),
    )
    pair_1 = shift(pair, 1)
    pair_3 = shift(pair, 3)
    quarter_grads = hbm((128, 3 * FQ), BF16)
    in_place = pl.BlockSpec(memory_space=pltpu.HBM)
    weights = (gate_w, up_w, down_w, gate_3, up_3, down_3, gate_1, up_1, down_1)
    grads_0, back, gg = call(
        three_kernel,
        sc,
        (pair, *((far(x), in_place) for x in weights)),
        (quarter_grads, vmem((128, D), F32), vmem((128, 128), F32)),
        (
            pltpu.VMEM((3, D, 2 * FQ), BF16),
            pltpu.VMEM((3, FQ, D), BF16),
            pltpu.SemaphoreType.DMA((9,)),
        ),
    )
    (send_back,) = call(
        emit_kernel,
        sc,
        (pair, *((far(x), in_place) for x in (gate_2, up_2, down_2)), back, gg),
        (hbm((SENT, 2 * CH + 128), BF16),),
        (
            pltpu.VMEM((CH // 128 + 1, SENT, 128), F32),
            pltpu.VMEM((D, 2 * FQ), BF16),
            pltpu.VMEM((FQ, D), BF16),
            pltpu.SemaphoreType.DMA((3,)),
        ),
    )
    home = lax.all_to_all(send_back.reshape(EXPERTS, 8, 2 * CH + 128), EP, 0, 0, tiled=True)
    home = home.reshape(SENT, 2 * CH + 128)
    top = shift(pair_1[0:64], 1)
    bottom = shift(pair_3[64:], 3)
    own_weights = tuple(whole(far(x)) for x in (gate_w, up_w, down_w))
    grads_1, grads_3 = call(
        redo_kernel,
        sc,
        (*(whole(far(x)) for x in (pair_1, pair_3)), *own_weights),
        (quarter_grads,) * 2,
    )
    grad_gate, grad_up, grad_down, down_norms, norms = call(
        sums_kernel,
        sc,
        (
            *(whole(far(x)) for x in (pair, pair_1, top, bottom, pair_3, grads_0, grads_1, grads_3)),
            *own_weights,
        ),
        (
            sds((D, FQ), BF16),
            sds((D, FQ), BF16),
            sds((FQ, D), BF16),
            sds((1, FQ), F32),
            vmem((16, 4 * 128), BF16),
        ),
    )
    (parts,) = call(
        home_kernel,
        sc,
        (home, whole(hit0), whole(hit1), norms),
        (vmem((TP, TOK + 32, DQ), BF16),),
        (pltpu.VMEM((2 * CH // 128 + 1, SENT, 128), F32),),
    )
    parts = lax.all_to_all(parts, "tp", 0, 0, tiled=True)
    grad_tokens, grad_gating, grad_router, router_norms, in_norms = call(
        last_kernel,
        sc,
        (
            parts,
            whole(stats),
            whole(routing_t),
            (router_weight, pl.BlockSpec((DQ, 128), lambda g, p: (p[0], 0))),
        ),
        (
            sds((TOK, DQ), BF16),
            sds((2, TOK), F32),
            sds((16, EXPERTS), F32),
            sds((1, 16), F32),
            sds((2, D), F32),
        ),
    )
    return (
        grad_tokens,
        grad_gating.T,
        grad_router,
        grad_gate[None],
        grad_up[None],
        grad_down[None],
        in_norms[None],
        down_norms,
        router_norms[0],
    )


def solution(mesh):
    split = Mesh(mesh.devices.reshape(8, 8, 2, TP), ("ep_0", "ep_1", "ep_2", "tp"))
    in_specs = (
        P(EP, None),
        P(EP, None),
        P(EP, None),
        P(),
        P(EP, None, "tp"),
        P(EP, None, "tp"),
        P(EP, "tp", None),
    )
    out_specs = (
        P(EP, "tp"),
        P(EP, None),
        P(EP, None),
        P(EP, None, "tp"),
        P(EP, None, "tp"),
        P(EP, "tp", None),
        P(EP, None, None),
        P(EP, "tp"),
        P(EP),
    )
    return jax.shard_map(layer, mesh=split, in_specs=in_specs, out_specs=out_specs, check_vma=False)
```
